32 devices in a mesh: ep: 8 (over z, x), tp: 4 (over y, core).
Axes of the slice: x: 2, y: 2, z: 4, core: 2. Of those that a mesh axis runs over, the one named last changes fastest.
Arguments:
- mixer_input: bfloat16 [2048, 2048], P('ep'), may hold values from -6 to 6
- mixer_gain: float32 [2048], replicated, may hold values from 0.1 to 8
- query_one: bfloat16 [2048, 512], P(None, 'tp'), may hold values from -0.1875 to 0.1875
- query_two: bfloat16 [2048, 512], P(None, 'tp'), may hold values from -0.1875 to 0.1875
- key_one: bfloat16 [2048, 256], P(None, 'tp'), may hold values from -0.1875 to 0.1875
- key_two: bfloat16 [2048, 256], P(None, 'tp'), may hold values from -0.1875 to 0.1875
- value_weight: bfloat16 [2048, 512], P(None, 'tp'), may hold values from -0.125 to 0.125
- lambdas: float32 [8], P('tp'), may hold values from 0.3 to 0.8
- head_gain: float32 [128], replicated, may hold values from 0.1 to 1.9
- output_weight: bfloat16 [1024, 2048], P('tp'), may hold values from -0.1875 to 0.1875
- expert_input: bfloat16 [4096, 2048], P(('ep', 'tp')), may hold values from -6 to 6
- expert_gain: float32 [2048], replicated, may hold values from 0.1 to 1.9
- routes: int32 [4096, 2], P(('ep', 'tp')), may hold values from 0 to 7, all different within a row; in each aligned block of 128 rows (0 to 127, 128 to 255, ...) at most 40 rows name the same one
- route_weight: float32 [4096, 2], P(('ep', 'tp')), may hold values from 0.2 to 1
- expert_gate: bfloat16 [8, 2048, 1024], P('ep', None, 'tp'), may hold values from -0.125 to 0.125
- expert_up: bfloat16 [8, 2048, 1024], P('ep', None, 'tp'), may hold values from -0.125 to 0.125
- expert_down: bfloat16 [8, 1024, 2048], P('ep', 'tp'), may hold values from -0.1875 to 0.1875
- shared_gate: bfloat16 [2048, 512], P(None, 'tp'), may hold values from -0.125 to 0.125
- shared_up: bfloat16 [2048, 512], P(None, 'tp'), may hold values from -0.125 to 0.125
- shared_down: bfloat16 [512, 2048], P('tp'), may hold values from -0.25 to 0.25
Outputs:
- mixer_output: bfloat16 [2048, 2048], P(('ep', 'tp'))
- expert_output: bfloat16 [4096, 2048], P(('ep', 'tp'))
The draws below stay inside these ranges and needn't reach their ends.
Inputs may be any that keep to these rules, and one draw needn't show every extreme that they name: `routes`: each row names 2 different experts; in the rows of one device no expert is named by more than 40 rows, and some device names some expert exactly 40 times.
All inputs are finite; a program needn't handle non-finite values.
Results may differ from the reference program's by a relative error of at most 0.014.
The reference program's roundings to bfloat16 on the way count: a program that leaves them out, or rounds other values in their place, can miss the bound.
Values may be sent and summed in bfloat16 or wider, within the bound.
A program may use at most 128 MiB of HBM per device.

```python
import math
import jax
import jax.numpy as jnp
import numpy as np
from jax import lax

D = 2048
HEADS = 8
KV_HEADS = 4
HEAD = 64
VDIM = 128
EFF = 1024
SFF = 512
TOP = 2
EXPERTS = 8
ROWS = 128
CAP = 40
SEQ_LEN = 2048
TOKENS = 4096
N_EP = 8
N_TP = 4


def draw_mixer_gain(key, part):
    return jnp.clip(1.0 + 0.18 * jax.random.normal(key, (D,), jnp.float32), 0.1, 1.9)


def shard_levels(stream_key, shape, cuts, least, largest):
    def one(position, blocks):
        draws = jax.random.uniform(jax.random.fold_in(jax.random.fold_in(stream_key, 6), position), (blocks,), jnp.float32, least / len(cuts), largest / len(cuts))
        return jnp.repeat(jnp.exp(draws), shape[position] // blocks).reshape((-1,) + (1,) * (len(shape) - position - 1))

    level = one(*cuts[0])
    for cut in cuts[1:]:
        level = level * one(*cut)
    return level


def deal_out(own_key, own, number, rows, number_of, top, most, slope):
    sequence = jax.random.permutation(own_key, number_of)
    crowded, common = shares(number_of, rows * top, most, slope, True), shares(number_of, rows * top, most, slope, False)
    places = jnp.arange(number_of)

    def named(tallies, offset_by):
        used = int((tallies > 0).sum())
        fixed = max(1, used // 4)
        moved = fixed + (places - fixed + offset_by * (used - fixed)) % max(1, number_of - fixed)
        return jnp.zeros((number_of,), jnp.int32).at[sequence[jnp.where(places < fixed, places, moved)]].set(jnp.asarray(tallies, jnp.int32))

    tallies = jnp.where(number % 4 == 0, named(crowded, number // 4), named(common, number - number // 4 - 1))
    mixed = jax.random.permutation(jax.random.fold_in(own, 3), number_of)
    giver, sink = mixed[0:number_of // 2 * 2:2], mixed[1:number_of // 2 * 2:2]
    slack = jnp.minimum(tallies[giver] - 1, most - tallies[sink]) // 2
    slack = jnp.where((giver == sequence[0]) | (sink == sequence[0]) | (tallies[sink] == 0), 0, jnp.maximum(slack, 0))
    moved = jax.random.randint(jax.random.fold_in(own, 4), (number_of // 2,), 0, 1 << 20) % (slack + 1)
    tallies = tallies.at[giver].add(-moved).at[sink].add(moved)
    items = jnp.searchsorted(jnp.cumsum(tallies), jnp.arange(rows * top), side="right").astype(jnp.int32)
    listing = items.reshape(top, rows).T
    listing = listing[jax.random.permutation(jax.random.fold_in(own, 1), rows)]
    offset_by = jax.random.randint(jax.random.fold_in(own, 2), (rows, 1), 0, top)
    return jnp.take_along_axis(listing, (jnp.arange(top)[None, :] + offset_by) % top, axis=1)


def shares(count, total, reach, slope, full):
    loads = [(1 << 20) // math.isqrt(standing ** slope) + 1 for standing in range(1, count + 1)]
    largest = reach if full else min(reach, max(-(-total // count), total * loads[0] // sum(loads)))
    least = 1 if total - largest >= count - 1 else 0
    given, surplus = [largest] + [least] * (count - 1), total - largest - least * (count - 1)
    while surplus > 0:
        free = [i for i in range(1, count) if given[i] < largest] or [i for i in range(1, count) if given[i] < reach]
        whole, budget = sum([loads[i] for i in free]), surplus
        for i in free:
            extra = min(reach - given[i], max(1, budget * loads[i] // whole), surplus)
            given[i] = given[i] + extra
            surplus = surplus - extra
    return np.array(given)


def centred(rng, dims, width, most, shards=(), kind=jnp.bfloat16):
    drawn = width * jax.random.normal(rng, dims, jnp.float32)
    if shards:
        drawn = drawn * shard_levels(rng, dims, shards, -0.22, 0.18)
    return jnp.clip(drawn, -most, most).astype(kind)


def setup_inputs(seed: int = 0) -> dict:
    arg_keys = jax.random.split(jax.random.key(seed), 21)
    mixer_input = centred(arg_keys[0], (SEQ_LEN, D), 1.0, 6.0, ((0, 8),))
    mixer_gain = draw_mixer_gain(jax.random.fold_in(arg_keys[20], 71), 0)
    query_one = centred(arg_keys[2], (D, HEADS * HEAD), (D // 2) ** -0.5, 0.1875, ((1, 4),))
    query_two = centred(arg_keys[3], (D, HEADS * HEAD), (D // 2) ** -0.5, 0.1875, ((1, 4),))
    key_one = centred(arg_keys[4], (D, KV_HEADS * HEAD), (D // 2) ** -0.5, 0.1875, ((1, 4),))
    key_two = centred(arg_keys[5], (D, KV_HEADS * HEAD), (D // 2) ** -0.5, 0.1875, ((1, 4),))
    value_weight = centred(arg_keys[6], (D, KV_HEADS * VDIM), D ** -0.5, 0.125, ((1, 4),))
    lambdas = jnp.clip(0.3 + 0.5 * jax.random.uniform(arg_keys[7], (HEADS,), jnp.float32) ** shard_levels(arg_keys[7], (HEADS,), ((0, 4),), -0.2, 0.2), 0.3, 0.8)
    head_gain = jnp.clip(1.0 + 0.18 * jax.random.normal(arg_keys[8], (VDIM,), jnp.float32), 0.1, 1.9)
    output_weight = centred(arg_keys[9], (HEADS * VDIM, D), (HEADS * VDIM) ** -0.5, 0.1875, ((0, 4),))
    expert_input = centred(arg_keys[10], (TOKENS, D), 1.0, 6.0, ((0, 32),))
    expert_gain = jnp.clip(1.0 + 0.18 * jax.random.normal(arg_keys[11], (D,), jnp.float32), 0.1, 1.9)
    routes_keys = jax.random.split(jax.random.fold_in(arg_keys[12], 1), TOKENS // ROWS)
    routes_turns = jax.random.permutation(jax.random.fold_in(arg_keys[12], 3), TOKENS // ROWS)
    routes = jax.vmap(lambda own, number: deal_out(jax.random.fold_in(arg_keys[12], 2), own, number, ROWS, EXPERTS, TOP, CAP, 2))(routes_keys, routes_turns).reshape((TOKENS, TOP))
    route_weight = jnp.clip(jnp.exp(math.log(1.0) - 1.609438 * jax.random.uniform(arg_keys[13], (TOKENS, TOP), jnp.float32) ** shard_levels(arg_keys[13], (TOKENS, TOP), ((0, 32),), -0.2, 0.2)), 0.2, 1.0)
    expert_gate = centred(arg_keys[14], (EXPERTS, D, EFF), D ** -0.5, 0.125, ((0, 8), (2, 4)))
    expert_up = centred(arg_keys[15], (EXPERTS, D, EFF), D ** -0.5, 0.125, ((0, 8), (2, 4)))
    expert_down = centred(arg_keys[16], (EXPERTS, EFF, D), EFF ** -0.5, 0.1875, ((0, 8), (1, 4)))
    shared_gate = centred(arg_keys[17], (D, SFF), D ** -0.5, 0.125, ((1, 4),))
    shared_up = centred(arg_keys[18], (D, SFF), D ** -0.5, 0.125, ((1, 4),))
    shared_down = centred(arg_keys[19], (SFF, D), SFF ** -0.5, 0.25, ((0, 4),))
    return dict(mixer_input=mixer_input, mixer_gain=mixer_gain, query_one=query_one, query_two=query_two, key_one=key_one, key_two=key_two, value_weight=value_weight, lambdas=lambdas, head_gain=head_gain, output_weight=output_weight, expert_input=expert_input, expert_gain=expert_gain, routes=routes, route_weight=route_weight, expert_gate=expert_gate, expert_up=expert_up, expert_down=expert_down, shared_gate=shared_gate, shared_up=shared_up, shared_down=shared_down)


EPS = 1e-06
NEG = -1e+30

def normalize(activations, scaling):
    values = activations.astype(jnp.float32)
    factor = lax.rsqrt(lax.optimization_barrier(jnp.mean(values * values, axis=-1, keepdims=True)) + EPS)
    return (values * factor * scaling).astype(jnp.bfloat16)

def swiglu(inputs, gate_weight, up_weight):
    gated = jnp.dot(inputs, gate_weight, preferred_element_type=jnp.float32)
    lifted = jnp.dot(inputs, up_weight, preferred_element_type=jnp.float32)
    return (jax.nn.silu(gated) * lifted).astype(jnp.bfloat16)

def quarter_sum(hidden, down_weight):
    group_width = hidden.shape[1] // N_TP
    running_sum = jnp.zeros((hidden.shape[0], down_weight.shape[1]), jnp.float32)
    for group_index in range(N_TP):
        partial_product = jnp.dot(hidden[:, group_index * group_width:(group_index + 1) * group_width], down_weight[group_index * group_width:(group_index + 1) * group_width], preferred_element_type=jnp.float32)
        rounded = lax.optimization_barrier(partial_product.astype(jnp.bfloat16))
        running_sum = running_sum + rounded.astype(jnp.float32)
    return running_sum

def attention(mixer_input, mixer_gain, query_one, query_two, key_one, key_two, value_weight, lambdas, head_gain, output_weight):
    normed = normalize(mixer_input, mixer_gain)
    tokens = normed.shape[0]
    group_size = HEADS // KV_HEADS

    def project(weight):
        return jnp.dot(normed, weight, preferred_element_type=jnp.float32).astype(jnp.bfloat16)
    query_first = project(query_one).reshape(tokens, KV_HEADS, group_size, HEAD)
    query_second = project(query_two).reshape(tokens, KV_HEADS, group_size, HEAD)
    key_first = project(key_one).reshape(tokens, KV_HEADS, HEAD).astype(jnp.float32)
    key_second = project(key_two).reshape(tokens, KV_HEADS, HEAD).astype(jnp.float32)
    value_rows = project(value_weight).reshape(tokens, KV_HEADS, VDIM).astype(jnp.float32)
    lambda_grid = lambdas.reshape(KV_HEADS, group_size)[:, :, None, None]
    key_pos = jnp.arange(tokens, dtype=jnp.int32)
    span_rows = min(128, tokens)

    def single_map(queries, key_rows, visible):
        scores = jnp.einsum('qkgd,jkd->kgqj', queries.astype(jnp.float32), key_rows) * HEAD ** (-0.5)
        scores = jnp.where(visible, scores, NEG)
        highest = lax.optimization_barrier(jnp.max(scores, axis=-1, keepdims=True))
        weights = jnp.where(visible, jnp.exp(scores - highest), 0.0)
        totals = lax.optimization_barrier(jnp.sum(weights, axis=-1))
        rounded = lax.optimization_barrier(weights.astype(jnp.bfloat16)).astype(jnp.float32)
        mixed = jnp.einsum('kgqj,jkd->kgqd', rounded, value_rows)
        return mixed / totals[..., None]

    def query_block(block_index):
        offset = (block_index * span_rows).astype(jnp.int32)
        query_pos = offset + jnp.arange(span_rows, dtype=jnp.int32)
        visible = key_pos[None, :] <= query_pos[:, None]
        first_part = single_map(lax.dynamic_slice_in_dim(query_first, offset, span_rows, 0), key_first, visible)
        second_part = single_map(lax.dynamic_slice_in_dim(query_second, offset, span_rows, 0), key_second, visible)
        combined = first_part - lambda_grid * second_part
        factor = lax.rsqrt(lax.optimization_barrier(jnp.mean(combined * combined, axis=-1, keepdims=True)) + EPS)
        normed_heads = (combined * factor * head_gain).astype(jnp.bfloat16)
        return normed_heads.transpose(2, 0, 1, 3).reshape(span_rows, HEADS * VDIM)
    head_rows = lax.map(query_block, jnp.arange(tokens // span_rows, dtype=jnp.int32))
    head_rows = head_rows.reshape(tokens, HEADS * VDIM)
    return quarter_sum(head_rows, output_weight).astype(jnp.bfloat16)

def experts_part(expert_input, expert_gain, routes, route_weight, expert_gate, expert_up, expert_down, shared_gate, shared_up, shared_down):
    normed = normalize(expert_input, expert_gain)
    tokens = normed.shape[0]
    shared_result = quarter_sum(swiglu(normed, shared_gate, shared_up), shared_down)
    flat_routes = routes.reshape(-1).astype(jnp.int32)
    copies = flat_routes.shape[0]
    onehot = (flat_routes[:, None] == jnp.arange(EXPERTS, dtype=jnp.int32)[None, :]).astype(jnp.int32)
    slot_place = lax.optimization_barrier(jnp.sum((jnp.cumsum(onehot, axis=0) - onehot) * onehot, axis=1)).astype(jnp.int32)
    owners = (jnp.arange(copies, dtype=jnp.int32) // TOP).astype(jnp.int32)
    table = jnp.zeros((EXPERTS, N_EP * N_TP * CAP), jnp.int32).at[flat_routes, slot_place].set(owners)

    def one_expert(expert_index):
        chosen = normed[table[expert_index]]
        hidden = swiglu(chosen, expert_gate[expert_index], expert_up[expert_index])
        return quarter_sum(hidden, expert_down[expert_index]).astype(jnp.bfloat16)
    results = lax.map(one_expert, jnp.arange(EXPERTS, dtype=jnp.int32))
    picked = results[flat_routes, slot_place].astype(jnp.float32).reshape(tokens, TOP, -1)
    routed = lax.optimization_barrier(jnp.sum(picked * route_weight[:, :, None], axis=1))
    return (routed + shared_result).astype(jnp.bfloat16)

def reference(mixer_input, mixer_gain, query_one, query_two, key_one, key_two, value_weight, lambdas, head_gain, output_weight, expert_input, expert_gain, routes, route_weight, expert_gate, expert_up, expert_down, shared_gate, shared_up, shared_down):
    mixer_output = attention(mixer_input, mixer_gain, query_one, query_two, key_one, key_two, value_weight, lambdas, head_gain, output_weight)
    expert_output = experts_part(expert_input, expert_gain, routes, route_weight, expert_gate, expert_up, expert_down, shared_gate, shared_up, shared_down)
    return (mixer_output, expert_output)
```

```python
import functools
import math

import jax
import jax.numpy as jnp
from jax import lax
from jax.experimental import pallas as pl
from jax.experimental.pallas import tpu as pltpu
from jax.sharding import PartitionSpec as P

HEAD = 64


EPS = 1e-06
NEG = -1e30


def normalize(activations, scaling):
    values = activations.astype(jnp.float32)
    factor = lax.rsqrt(jnp.mean(values * values, axis=-1, keepdims=True) + EPS)
    return (values * factor * scaling).astype(jnp.bfloat16)


def attention_kernel(
    shape, rank_ref, lambdas_ref, queries_ref, keys_ref, gain_ref, out_ref, maxima, totals, weighted
):
    rows, chunk, local_kv, group, value_dim = shape
    rank = rank_ref[0]
    maxima[...] = jnp.full(maxima.shape, NEG, jnp.float32)
    totals[...] = jnp.zeros(totals.shape, jnp.float32)
    weighted[...] = jnp.zeros(weighted.shape, jnp.float32)
    heads = local_kv * group
    key_cols = local_kv * HEAD
    chunks = rows // chunk
    scale = HEAD**-0.5 * math.log2(math.e)

    def block(index, masked):
        start = pl.multiple_of(index * rows, rows)
        for kv in range(local_kv):
            value_start = 2 * key_cols + kv * value_dim
            for part in range(chunks):
                span = (part + 1) * chunk if masked else rows
                values = keys_ref[pl.ds(start, span), value_start : value_start + value_dim]
                for which in range(2):
                    first = which * key_cols + kv * HEAD
                    keys = keys_ref[pl.ds(start, span), first : first + HEAD]
                    for g in range(group):
                        head = kv * group + g
                        col = (which * heads + head) * HEAD
                        queries = queries_ref[part * chunk : (part + 1) * chunk, col : col + HEAD]
                        scores = lax.dot_general(
                            queries,
                            keys,
                            (((1,), (1,)), ((), ())),
                            preferred_element_type=jnp.float32,
                        )
                        if masked:
                            row = part * chunk + lax.broadcasted_iota(jnp.int32, scores.shape, 0)
                            col_pos = lax.broadcasted_iota(jnp.int32, scores.shape, 1)
                            scores = jnp.where(col_pos <= row, scores, NEG)
                        slot = (which * heads + head) * chunks + part
                        earlier = maxima[slot]
                        latest = jnp.maximum(earlier, jnp.max(scores, axis=1, keepdims=True))
                        shrink = jnp.exp2((earlier - latest) * scale)
                        weights = jnp.exp2((scores - latest[:, :1]) * scale)
                        totals[slot] = totals[slot] * shrink + jnp.sum(
                            weights, axis=1, keepdims=True
                        )
                        weighted[slot] = weighted[slot] * shrink[:, :1] + jnp.dot(
                            weights.astype(jnp.bfloat16),
                            values,
                            preferred_element_type=jnp.float32,
                        )
                        maxima[slot] = latest

    def earlier_block(index, carry):
        block(index, False)
        return carry

    lax.fori_loop(0, rank, earlier_block, 0)
    block(rank, True)
    for head in range(heads):
        for part in range(chunks):
            one = head * chunks + part
            two = (heads + head) * chunks + part
            combined = (
                weighted[one] / totals[one][:, :1]
                - lambdas_ref[head] * (weighted[two] / totals[two][:, :1])
            )
            factor = lax.rsqrt(jnp.mean(combined * combined, axis=1, keepdims=True) + EPS)
            out_ref[
                part * chunk : (part + 1) * chunk, head * value_dim : (head + 1) * value_dim
            ] = (combined * factor * gain_ref[...]).astype(jnp.bfloat16)


def attention(queries, keys, rank, lambdas, head_gain, local_kv, group):
    rows = queries.shape[0]
    value_dim = head_gain.shape[0]
    heads = local_kv * group
    chunk = min(128, rows)
    slots = 2 * heads * (rows // chunk)
    vmem = pl.BlockSpec(memory_space=pltpu.VMEM)
    smem = pl.BlockSpec(memory_space=pltpu.SMEM)
    scores = heads * 2 * rows * keys.shape[0]
    return pl.pallas_call(
        functools.partial(attention_kernel, (rows, chunk, local_kv, group, value_dim)),
        out_shape=jax.ShapeDtypeStruct((rows, heads * value_dim), jnp.bfloat16),
        in_specs=[smem, smem, vmem, vmem, vmem],
        out_specs=vmem,
        scratch_shapes=[
            pltpu.VMEM((slots, chunk, 128), jnp.float32),
            pltpu.VMEM((slots, chunk, 128), jnp.float32),
            pltpu.VMEM((slots, chunk, value_dim), jnp.float32),
        ],
        compiler_params=pltpu.CompilerParams(vmem_limit_bytes=48 * 1024 * 1024),
        cost_estimate=pl.CostEstimate(
            flops=8 * scores * HEAD, bytes_accessed=keys.size * 2, transcendentals=scores
        ),
        name="attention",
    )(rank.reshape(1), lambdas, queries, keys, head_gain.reshape(1, value_dim))


def swap(rows, axis, size, distance):
    return lax.ppermute(rows, axis, [(i, i ^ distance) for i in range(size)])


def gather_near(block, axis, size, ahead=None):
    places = {0: block}
    distance = size // 2
    while distance:
        for place in sorted(places):
            moved = swap(places[place], axis, size, distance)
            if ahead is not None:
                moved, ahead = lax.optimization_barrier((moved, ahead))
            places[place ^ distance] = moved
        ahead = None
        distance //= 2
    return [places[place] for place in range(size)]


def scatter_near(partials, axis, size):
    sums = dict(enumerate(partials))
    distance = 1
    while distance < size:
        kept = [place for place in sorted(sums) if not place & distance]
        moved = {
            place: swap(sums[place ^ distance].astype(jnp.bfloat16), axis, size, distance)
            for place in kept
        }
        sums = {
            place: sums[place].astype(jnp.float32) + moved[place].astype(jnp.float32)
            for place in kept
        }
        distance *= 2
    return sums[0]


def general_body(
    mixer_input,
    mixer_gain,
    query_one,
    query_two,
    key_one,
    key_two,
    value_weight,
    lambdas,
    head_gain,
    output_weight,
    expert_input,
    expert_gain,
    routes,
    route_weight,
    expert_gate,
    expert_up,
    expert_down,
    shared_gate,
    shared_up,
    shared_down,
):
    ep_size = lax.axis_size("ep")
    tp_size = lax.axis_size("tp")
    ep_rank = lax.axis_index("ep")
    mixer_rows = mixer_input.shape[0]
    model_width = mixer_input.shape[1]
    query_cols = query_one.shape[1]
    key_cols = key_one.shape[1]
    value_dim = head_gain.shape[0]
    local_kv = key_cols // HEAD
    local_heads = query_cols // HEAD
    group_size = local_heads // local_kv
    normed = normalize(mixer_input, mixer_gain)

    def project(weights):
        return jnp.concatenate(
            [
                jnp.dot(normed, weight, preferred_element_type=jnp.float32).astype(jnp.bfloat16)
                for weight in weights
            ],
            axis=1,
        )

    key_values = project([key_one, key_two, value_weight])
    query_part = project([query_one, query_two])
    arrived = lax.all_gather(key_values, "ep", axis=0, tiled=True)
    head_rows = attention(
        query_part, arrived, ep_rank, lambdas, head_gain, local_kv, group_size
    )
    tp_rank = lax.axis_index("tp")
    own_rows = mixer_rows // tp_size

    def mixer_place(place):
        rows = lax.dynamic_slice_in_dim(head_rows, (tp_rank ^ place) * own_rows, own_rows, 0)
        return jnp.dot(rows, output_weight, preferred_element_type=jnp.float32).astype(
            jnp.bfloat16
        )

    mixer_sum = scatter_near(
        [mixer_place(place) for place in range(tp_size)], "tp", tp_size
    ).astype(jnp.bfloat16)

    token_rows = expert_input.shape[0]
    normed_experts = normalize(expert_input, expert_gain)
    experts_local = expert_gate.shape[0]
    expert_count = experts_local * ep_size
    top_count = routes.shape[1]
    capacity = max(2, 5 * token_rows * top_count // (4 * expert_count))
    slot_count = expert_count * capacity
    flat_routes = routes.reshape(-1)
    onehot = (flat_routes[:, None] == jnp.arange(expert_count, dtype=jnp.int32)[None, :]).astype(
        jnp.int32
    )
    slot_place = jnp.sum((jnp.cumsum(onehot, axis=0) - onehot) * onehot, axis=1)
    slot_ids = (flat_routes * capacity + slot_place).reshape(token_rows, top_count)
    slot_match = jnp.arange(slot_count, dtype=jnp.int32)[:, None, None] == slot_ids[None, :, :]
    select = jnp.any(slot_match, axis=2).astype(jnp.bfloat16)
    outgoing = jnp.dot(select, normed_experts, preferred_element_type=jnp.float32).astype(
        jnp.bfloat16
    )
    pair_rows = experts_local * capacity
    outgoing = outgoing.reshape(ep_size, pair_rows, model_width)
    outgoing, key_values = lax.optimization_barrier((outgoing, key_values))
    received = lax.all_to_all(outgoing, "ep", split_axis=0, concat_axis=0, tiled=True)
    received = received.reshape(ep_size, experts_local, capacity, model_width)
    if experts_local == 1:
        received = received.reshape(ep_size * capacity, model_width)

    def shared_expert(rows):
        gated = jnp.dot(rows, shared_gate, preferred_element_type=jnp.float32)
        lifted = jnp.dot(rows, shared_up, preferred_element_type=jnp.float32)
        hidden = (jax.nn.silu(gated) * lifted).astype(jnp.bfloat16)
        return jnp.dot(hidden, shared_down, preferred_element_type=jnp.float32).astype(
            jnp.bfloat16
        )

    def routed_expert(rows):
        if experts_local == 1:
            gated = jnp.dot(rows, expert_gate[0], preferred_element_type=jnp.float32)
            lifted = jnp.dot(rows, expert_up[0], preferred_element_type=jnp.float32)
            hidden = (jax.nn.silu(gated) * lifted).astype(jnp.bfloat16)
            return jnp.dot(hidden, expert_down[0], preferred_element_type=jnp.float32).astype(
                jnp.bfloat16
            )
        gated = jnp.einsum("secd,edf->secf", rows, expert_gate, preferred_element_type=jnp.float32)
        lifted = jnp.einsum("secd,edf->secf", rows, expert_up, preferred_element_type=jnp.float32)
        hidden = (jax.nn.silu(gated) * lifted).astype(jnp.bfloat16)
        return jnp.einsum(
            "secf,efd->secd", hidden, expert_down, preferred_element_type=jnp.float32
        ).astype(jnp.bfloat16)

    shared_places = gather_near(normed_experts, "tp", tp_size)
    routed_places = gather_near(received, "tp", tp_size, head_rows)
    shared_result = scatter_near([shared_expert(rows) for rows in shared_places], "tp", tp_size)
    routed_result = scatter_near(
        [routed_expert(rows) for rows in routed_places], "tp", tp_size
    ).astype(jnp.bfloat16)
    returned = lax.all_to_all(
        routed_result.reshape(ep_size, pair_rows, model_width),
        "ep",
        split_axis=0,
        concat_axis=0,
        tiled=True,
    )
    returned = returned.reshape(slot_count, model_width)
    spread = jnp.sum(
        jnp.where(
            jnp.arange(slot_count, dtype=jnp.int32)[None, None, :] == slot_ids[:, :, None],
            route_weight[:, :, None],
            0.0,
        ),
        axis=1,
    )
    upper = lax.reduce_precision(spread, 8, 7)
    lower = lax.reduce_precision(spread - upper, 8, 7)
    routed_total = jnp.dot(
        upper.astype(jnp.bfloat16), returned, preferred_element_type=jnp.float32
    ) + jnp.dot(lower.astype(jnp.bfloat16), returned, preferred_element_type=jnp.float32)
    expert_output = (routed_total + shared_result).astype(jnp.bfloat16)
    return (mixer_sum, expert_output)


def chunk_order(half):
    order = [("n", 0)]
    near = [("n", d) for d in range(1, half)]
    far = [("f", d) for d in range(half)]
    while near or far:
        if far:
            order.append(far.pop(0))
        if near and (len(order) > 2 or not far):
            order.append(near.pop(0))
    return order


def padded(rows):
    return -(-rows // 16) * 16


class Sizes:
    def __init__(self, ep, tp, rows, width, tokens, hidden, shared, capacity, value_dim):
        self.ep, self.tp, self.rows, self.width = ep, tp, rows, width
        self.tokens, self.hidden, self.shared = tokens, hidden, shared
        self.cap, self.stride = capacity, padded(capacity)
        self.value_dim = value_dim
        self.half = ep // 2
        self.own = rows // tp
        self.tile = min(512, width)

    def names(self):
        half, ep = self.half, self.ep
        groups = (
            [("XY", 0), ("INFO", 0), ("XC", 0), ("XC", 1)]
            + [("FAR", d) for d in range(half)]
            + [("NEAR", d, a) for d in range(1, half) for a in range(2)]
            + [("FY", d) for d in range(half)]
            + [("NRET", d) for d in range(1, half)]
            + [("FRET", d) for d in range(half)]
            + [("SC", 0), ("SC", 1), ("AY", 0), ("KVF", 0), ("OC", 0), ("OY", 0)]
            + [("KVN", d) for d in range(1, half)]
            + [("KVC", d) for d in range(1, half)]
        )
        table = {name: number for number, name in enumerate(groups)}
        first = len(groups)
        table["RC"], table["PC"], table["QY"] = first, first + ep, first + 2 * ep
        return table, first + 3 * ep

    def scratch(self):
        bf, f32 = jnp.bfloat16, jnp.float32
        ep, half, width, stride = self.ep, self.half, self.width, self.stride
        tokens, rows, hidden, shared = self.tokens, self.rows, self.hidden, self.shared
        vd = self.value_dim
        return dict(
            mx=((rows, width), bf),
            wq=((width, 4 * HEAD), bf),
            wk1=((width, HEAD), bf),
            wk2=((width, HEAD), bf),
            wv=((width, vd), bf),
            wo=((2 * vd, width), bf),
            wg=((width, hidden), bf),
            wu=((width, hidden), bf),
            wd=((hidden, width), bf),
            sg=((width, shared), bf),
            su=((width, shared), bf),
            sd=((shared, width), bf),
            xb=((2, 2, tokens, width), bf),
            other=((8, tokens), f32),
            outf=((half, stride, width), bf),
            outn=((half, 2, stride, width), bf),
            r=((ep, 2, 2, stride, width), bf),
            p=((ep, 2, 2, stride, width), bf),
            pr=((ep, 2, stride, width), bf),
            q=((ep, 2, stride, width), bf),
            qr=((ep, stride, width), bf),
            fb=((ep, stride, width), bf),
            tn=((2, half, stride, width), bf),
            tf=((half, stride, width), bf),
            s=((2, 2, tokens, width), bf),
            sr=((2, tokens, width), bf),
            ao=((tokens, width), bf),
            ar=((tokens, width), bf),
            acc=((tokens, width), f32),
            wown=((2, 2, tokens, half * stride), bf),
            woth=((2, tokens, half * stride), bf),
            nm=((rows, width), bf),
            qs=((2, 2, rows, 2 * HEAD), bf),
            kv=((ep, rows, 2 * HEAD + vd), bf),
            sc=((2, ep, rows, rows), f32),
            stat=((2, rows, 128), f32),
            tot=((2, rows, 128), f32),
            pv=((2, rows, vd), f32),
            hr=((rows, 2 * vd), bf),
            o=((2, 2, self.own, width), bf),
            orx=((2, self.own, width), bf),
            oq=((2, self.own, width), bf),
            oy=((self.own, width), bf),
        )

    def vmem_bytes(self):
        total = 0
        for shape, dtype in self.scratch().values():
            size = jnp.dtype(dtype).itemsize
            for extent in shape[:-1]:
                size *= extent
            total += size * (-(-shape[-1] // 128) * 128)
        return total


class Later:
    def __init__(self, start):
        self.start = start


def fused_kernel(sizes, keys, *refs):
    (lam, info, x, xgain, mgain, hgain) = refs[:6]
    (h_mx, h_q1, h_q2, h_k1, h_k2, h_v, h_wo, h_g, h_u, h_d, h_sg, h_su, h_sd) = refs[6:19]
    mix_out, exp_out = refs[19:21]
    b = dict(zip(keys, refs[21 : 21 + len(keys)]))
    send_sem, recv_sem, load_sem = refs[21 + len(keys) :]
    half, ep, width, stride, cap = sizes.half, sizes.ep, sizes.width, sizes.stride, sizes.cap
    tokens, rows, tile, vd = sizes.tokens, sizes.rows, sizes.tile, sizes.value_dim
    f32, bf = jnp.float32, jnp.bfloat16
    table, _ = sizes.names()
    order = chunk_order(half)
    place = {name: number for number, name in enumerate(order)}

    me = lax.axis_index("ep")
    tp = lax.axis_index("tp")
    side = me // half
    spot = me % half
    row_of = tp // 2
    core = tp % 2
    tiles = width // tile

    near_to = [side * half + (spot + d) % half for d in range(half)]
    near_by = [side * half + (spot + half - d) % half for d in range(half)]
    far_to = [(1 - side) * half + (spot + d) % half for d in range(half)]
    far_by = [(1 - side) * half + (spot + half - d) % half for d in range(half)]

    def near(d):
        return (near_to[d], tp)

    def near_from(d):
        return (near_by[d], tp)

    def far(d):
        return (far_to[d], tp)

    def far_from(d):
        return (far_by[d], tp)

    partner_y = (me, (1 - row_of) * 2 + core)
    partner_c = (me, row_of * 2 + 1 - core)

    def remote(number, source, target, device):
        return pltpu.make_async_remote_copy(
            src_ref=source,
            dst_ref=target,
            send_sem=send_sem.at[number],
            recv_sem=recv_sem.at[number],
            device_id=device,
            device_id_type=pl.DeviceIdType.MESH,
        )

    copies = {}

    def made(name):
        source, target, device = copies[name]
        return remote(table[name], source(), target(), device)

    def copy(name, source, target, device):
        copies[name] = (source, target, device)
        return Later(lambda: made(name).start())

    def dot(left, right):
        return jnp.dot(left, right, preferred_element_type=f32)

    loads = {}
    pairs = dict(
        mx=(h_mx, b["mx"]),
        q1=(h_q1, b["wq"].at[:, : 2 * HEAD]),
        q2=(h_q2, b["wq"].at[:, 2 * HEAD :]),
        k1=(h_k1, b["wk1"]),
        k2=(h_k2, b["wk2"]),
        v=(h_v, b["wv"]),
        sg=(h_sg, b["sg"]),
        su=(h_su, b["su"]),
        sd=(h_sd, b["sd"]),
        wg=(h_g.at[0], b["wg"]),
        wu=(h_u.at[0], b["wu"]),
        wd=(h_d.at[0], b["wd"]),
        wo=(h_wo, b["wo"]),
    )
    for number, (name, (source, target)) in enumerate(pairs.items()):
        loads[name] = pltpu.make_async_copy(source, target, load_sem.at[number])
        loads[name].start()

    barrier = pltpu.get_barrier_semaphore()
    peers = [near(d) for d in range(1, half)] + [far(d) for d in range(half)]
    peers += [partner_y, partner_c]
    for device in peers:
        pl.semaphore_signal(
            barrier, inc=1, device_id=device, device_id_type=pl.DeviceIdType.MESH
        )

    def norm_rows(source, target, count, gain):
        step = min(32, count)

        @pl.loop(0, count // step)
        def _(index):
            at = pl.ds(pl.multiple_of(index * step, step), step)
            values = source[at, :].astype(f32)
            factor = lax.rsqrt(jnp.mean(values * values, axis=-1, keepdims=True) + EPS)
            target[at, :] = (values * factor * gain[...]).astype(bf)

    norm_rows(x, b["xb"].at[0, 0], tokens, xgain)

    earlier = (
        lax.broadcasted_iota(jnp.int32, (tokens, tokens), 0)
        < lax.broadcasted_iota(jnp.int32, (tokens, tokens), 1)
    ).astype(bf)
    padded_ep = -(-ep // 8) * 8
    relative = lax.broadcasted_iota(jnp.int32, (padded_ep, tokens), 0)
    in_far = relative >= half
    turn = jnp.where(in_far, relative - half, relative) + spot
    turn = jnp.where(turn >= half, turn - half, turn)
    names_half = jnp.where(in_far, 1 - side, side)
    expert = (names_half * half + turn).astype(f32)

    def routing(info_ref):
        first = info_ref[0:1, :] == expert
        second = info_ref[1:2, :] == expert
        named = jnp.where(first | second, 1.0, 0.0)
        position = dot(named.astype(bf), earlier)
        position = jnp.where(named > 0.0, position, -1.0)
        weight = jnp.where(first, info_ref[2:3, :], 0.0) + jnp.where(second, info_ref[3:4, :], 0.0)
        return position, weight

    slot = lax.broadcasted_iota(jnp.int32, (stride, tokens), 0).astype(f32)

    def chosen(position, which):
        return slot == position[which : which + 1, :]

    def select(position, which):
        return jnp.concatenate(
            [jnp.where(chosen(position, k), 1.0, 0.0) for k in which], axis=0
        ).astype(bf)

    def spread(position, weight, which):
        stacked = jnp.concatenate(
            [jnp.where(chosen(position, k), weight[k : k + 1, :], 0.0) for k in which], axis=0
        )
        turned = stacked.T
        upper = turned.astype(bf)
        return upper, (turned - upper.astype(f32)).astype(bf)

    own_place, own_weight = routing(info)
    near_set = list(range(half))
    far_set = list(range(half, 2 * half))
    select_near = select(own_place, near_set)
    select_far = select(own_place, far_set)

    pl.semaphore_wait(barrier, len(peers))
    copy(("XY", 0), lambda: b["xb"].at[0, 0], lambda: b["xb"].at[1, 0], partner_y).start()
    copy(("INFO", 0), lambda: info, lambda: b["other"], partner_y).start()
    copy(("XC", 0), lambda: b["xb"].at[0, 0], lambda: b["xb"].at[0, 1], partner_c).start()

    def pick(select_rows, source, store):
        for n in range(tiles):
            cols = slice(n * tile, (n + 1) * tile)
            picked = dot(select_rows, source[:, cols]).astype(bf)
            for d in range(half):
                store(d, cols, picked[d * stride : (d + 1) * stride, :])

    def store_near(a):
        def store(d, cols, value):
            b["outn"][d, a, :, cols] = value

        return store

    def store_far(d, cols, value):
        b["outf"][d, :, cols] = value

    pick(select_near, b["xb"].at[0, 0], store_near(0))

    def start_near(a):
        for d in range(1, half):
            copy(
                ("NEAR", d, a),
                lambda d=d: b["outn"].at[d, a, pl.ds(0, cap)],
                lambda d=d: b["r"].at[place[("n", d)], 0, a, pl.ds(0, cap)],
                near(d),
            ).start()

    start_near(0)
    pick(select_far, b["xb"].at[0, 0], store_far)

    def start_far(d):
        copy(
            ("FAR", d),
            lambda: b["outf"].at[d, pl.ds(0, cap)],
            lambda: b["r"].at[place[("f", d)], 0, 0, pl.ds(0, cap)],
            far(d),
        ).start()

    for d in range(half // 2):
        start_far(d)

    loads["mx"].wait()
    norm_rows(b["mx"], b["nm"], rows, mgain)
    for name in ("q1", "q2", "k1", "k2", "v"):
        loads[name].wait()
    lane = lax.broadcasted_iota(jnp.int32, (rows, 2 * HEAD), 1)
    b["kv"][me, :, 0:HEAD] = dot(b["nm"][...], b["wk1"][...]).astype(bf)
    b["kv"][me, :, HEAD : 2 * HEAD] = dot(b["nm"][...], b["wk2"][...]).astype(bf)
    b["kv"][me, :, 2 * HEAD :] = dot(b["nm"][...], b["wv"][...]).astype(bf)

    copy(("KVF", 0), lambda: b["kv"].at[me], lambda: b["kv"].at[me], far(0))

    @pl.when(side == 0)
    def _():
        made(("KVF", 0)).start()

    for d in range(1, half):
        copy(("KVN", d), lambda: b["kv"].at[me], lambda: b["kv"].at[me], near(d))

        @pl.when(near_to[d] > me)
        def _(d=d):
            made(("KVN", d)).start()

    for d in range(half // 2, half):
        start_far(d)

    for m in range(2):
        queries = dot(b["nm"][...], b["wq"][:, m * 2 * HEAD : (m + 1) * 2 * HEAD])
        turned = pltpu.roll(queries, HEAD, 1)
        keep = (lane < HEAD) if m == 0 else (lane >= HEAD)
        for g in range(2):
            source = queries if g == m else turned
            b["qs"][m, g] = jnp.where(keep, source, 0.0).astype(bf)

    def shared_expert(a):
        both = b["xb"][a].reshape(2 * tokens, width)
        gated = dot(both, b["sg"][...])
        lifted = dot(both, b["su"][...])
        hidden = (jax.nn.silu(gated) * lifted).astype(bf)
        for n in range(tiles):
            cols = slice(n * tile, (n + 1) * tile)
            part = dot(hidden, b["sd"][:, cols]).astype(bf)
            b["s"][a, 0, :, cols] = part[:tokens]
            b["s"][a, 1, :, cols] = part[tokens:]

    for name in ("sg", "su", "sd"):
        loads[name].wait()
    made(("XC", 0)).wait_recv()
    shared_expert(0)
    copy(("SC", 0), lambda: b["s"].at[0, 1], lambda: b["sr"].at[0], partner_c).start()

    made(("XY", 0)).wait_recv()
    made(("INFO", 0)).wait_recv()
    copy(("XC", 1), lambda: b["xb"].at[1, 0], lambda: b["xb"].at[1, 1], partner_c).start()
    other_place, other_weight = routing(b["other"])
    pick(select(other_place, near_set), b["xb"].at[1, 0], store_near(1))
    start_near(1)
    b["r"][0, 0] = b["outn"][0]

    def core_forward(position):
        return remote(
            table["RC"] + position, b["r"].at[position, 0], b["r"].at[position, 1], partner_c
        )

    core_forward(0).start()
    for which, (at, wt, group) in enumerate(
        ((own_place, own_weight, near_set), (own_place, own_weight, far_set))
    ):
        upper, lower = spread(at, wt, group)
        b["wown"][which, 0] = upper
        b["wown"][which, 1] = lower
    upper, lower = spread(other_place, other_weight, near_set)
    b["woth"][0] = upper
    b["woth"][1] = lower
    for d in range(half):
        b["tf"][d, cap:, :] = jnp.zeros((stride - cap, width), bf)
        for a in range(2):
            b["tn"][a, d, cap:, :] = jnp.zeros((stride - cap, width), bf)
    made(("XC", 1)).wait_recv()
    shared_expert(1)
    copy(("SC", 1), lambda: b["s"].at[1, 1], lambda: b["sr"].at[1], partner_c).start()

    for name in ("wg", "wu", "wd"):
        loads[name].wait()

    def arrive_far(d):
        made(("FAR", d)).wait_recv()
        made(("FY", d)).start()

    def crossed(d):
        made(("FY", d)).wait_recv()
        core_forward(place[("f", d)]).start()

    def arrive_near(d):
        for a in range(2):
            made(("NEAR", d, a)).wait_recv()
        core_forward(place[("n", d)]).start()

    def relay_kv():
        @pl.when(side == 1)
        def _():
            slot_of = b["kv"].at[far_by[0]]
            remote(table[("KVF", 0)], slot_of, slot_of, far(0)).wait_recv()

        for d in range(1, half):
            copy(("KVC", d), lambda: b["kv"].at[far_by[0]], lambda: b["kv"].at[far_by[0]], near(d))

            @pl.when(side == 1)
            def _(d=d):
                made(("KVC", d)).start()

    events = {}

    def at_step(step, action):
        events.setdefault(max(step, 0), []).append(action)

    for position, (kind, d) in enumerate(order):
        if kind == "f":
            copies[("FY", d)] = (
                lambda position=position: b["r"].at[position, 0, 0, pl.ds(0, cap)],
                lambda position=position: b["r"].at[position, 0, 1, pl.ds(0, cap)],
                partner_y,
            )
            at_step(position - 2, functools.partial(arrive_far, d))
            at_step(position - 1, functools.partial(crossed, d))
        elif d > 0:
            at_step(position - 1, functools.partial(arrive_near, d))
    at_step(3, relay_kv)

    def is_one(value, choices):
        found = value == choices[0]
        for choice in choices[1:]:
            found = jnp.logical_or(found, value == choice)
        return found

    far_places = [place[("f", d)] for d in range(half)]
    row_count = 4 * stride

    def back_copy(number):
        return remote(
            table["PC"] + number, b["p"].at[number, 1], b["pr"].at[number], partner_c
        )

    def cross_copy(number):
        return remote(
            table["QY"] + number,
            b["q"].at[number, 1, pl.ds(0, cap)],
            b["qr"].at[number, pl.ds(0, cap)],
            partner_y,
        )

    def step_body(step, carry):
        for when, actions in sorted(events.items()):

            @pl.when(step == when)
            def _(actions=actions):
                for action in actions:
                    action()

        @pl.when(step < ep)
        def _():
            core_forward(step).wait_recv()
            arrived = b["r"][step].reshape(row_count, width)
            gated = dot(arrived, b["wg"][...])
            lifted = dot(arrived, b["wu"][...])
            hidden = (jax.nn.silu(gated) * lifted).astype(bf)

            for n in range(tiles):
                cols = slice(n * tile, (n + 1) * tile)
                part = dot(hidden, b["wd"][:, cols]).astype(bf)
                b["p"][step, :, :, :, cols] = part.reshape(2, 2, stride, tile)
            back_copy(step).start()

        last = step - 1

        @pl.when(jnp.logical_and(last >= 0, last < ep))
        def _():
            back_copy(last).wait_recv()
            for a in range(2):
                b["q"][last, a] = (
                    b["p"][last, 0, a].astype(f32) + b["pr"][last, a].astype(f32)
                ).astype(bf)

            @pl.when(last == 0)
            def _():
                for a in range(2):
                    b["tn"][a, 0, 0:cap, :] = b["q"][0, a, 0:cap, :]

            for d in range(1, half):
                at = place[("n", d)]
                copy(
                    ("NRET", d),
                    lambda at=at: b["q"].at[at, :, pl.ds(0, cap)],
                    lambda d=d: b["tn"].at[:, d, pl.ds(0, cap)],
                    near_from(d),
                )

                @pl.when(last == at)
                def _(d=d):
                    made(("NRET", d)).start()

            @pl.when(is_one(last, far_places))
            def _():
                cross_copy(last).start()

        older = step - 2

        @pl.when(jnp.logical_and(older >= 0, is_one(older, far_places)))
        def _():
            cross_copy(older).wait_recv()
            b["fb"][older] = (
                b["q"][older, 0].astype(f32) + b["qr"][older].astype(f32)
            ).astype(bf)
            for d in range(half):
                at = place[("f", d)]
                copy(
                    ("FRET", d),
                    lambda at=at: b["fb"].at[at, pl.ds(0, cap)],
                    lambda d=d: b["tf"].at[d, pl.ds(0, cap)],
                    far_from(d),
                )

                @pl.when(older == at)
                def _(d=d):
                    made(("FRET", d)).start()

        return carry

    lax.fori_loop(0, ep + 2, step_body, 0)

    def kv_arrival(name, source, d):
        block = b["kv"].at[source]
        remote(table[(name, d)], block, block, near(d)).wait_recv()

    for d in range(1, half):

        @pl.when(near_by[d] < me)
        def _(d=d):
            kv_arrival("KVN", near_by[d], d)

        @pl.when(side == 1)
        def _(d=d):
            kv_arrival("KVC", (1 - side) * half + (spot + half - d) % half, d)

    scale = HEAD**-0.5 * math.log2(math.e)
    row_place = me * rows + lax.broadcasted_iota(jnp.int32, (rows, rows), 0)
    col_place = lax.broadcasted_iota(jnp.int32, (rows, rows), 1)
    halves = [slice(c * 128, (c + 1) * 128) for c in range(rows // 128)]

    def head(g):
        b["stat"][...] = jnp.full((2, rows, 128), NEG, f32)
        b["tot"][...] = jnp.zeros((2, rows, 128), f32)
        b["pv"][...] = jnp.zeros((2, rows, vd), f32)

        def score(j, carry):
            keys_j = b["kv"][j, :, 0 : 2 * HEAD]
            for m in range(2):
                scores = lax.dot_general(
                    b["qs"][m, g], keys_j, (((1,), (1,)), ((), ())), preferred_element_type=f32
                )
                scores = jnp.where(j * rows + col_place <= row_place, scores, NEG)
                b["sc"][m, j] = scores
                most = b["stat"][m]
                for cols in halves:
                    most = jnp.maximum(most, scores[:, cols])
                b["stat"][m] = most
            return carry

        lax.fori_loop(0, me + 1, score, 0)
        for m in range(2):
            most = jnp.max(b["stat"][m], axis=1, keepdims=True)
            b["stat"][m] = jnp.broadcast_to(most, (rows, 128))

        def weigh(j, carry):
            values = b["kv"][j, :, 2 * HEAD :]
            for m in range(2):
                most = b["stat"][m]
                total = b["tot"][m]
                parts = []
                for cols in halves:
                    weights = jnp.exp2((b["sc"][m, j, :, cols] - most) * scale)
                    total = total + weights
                    parts.append(weights.astype(bf))
                b["tot"][m] = total
                b["pv"][m] += dot(jnp.concatenate(parts, axis=1), values)
            return carry

        lax.fori_loop(0, me + 1, weigh, 0)
        sums = [jnp.sum(b["tot"][m], axis=1, keepdims=True) for m in range(2)]
        combined = b["pv"][0] / sums[0] - lam[g] * (b["pv"][1] / sums[1])
        factor = lax.rsqrt(jnp.mean(combined * combined, axis=1, keepdims=True) + EPS)
        b["hr"][:, g * vd : (g + 1) * vd] = (combined * factor * hgain[...]).astype(bf)

    for g in range(2):
        head(g)

    loads["wo"].wait()
    own = sizes.own
    for n in range(tiles):
        cols = slice(n * tile, (n + 1) * tile)
        part = dot(b["hr"][...], b["wo"][:, cols]).astype(bf)
        b["o"][:, :, :, cols] = part.reshape(2, 2, own, tile)
    copy(("OC", 0), lambda: b["o"].at[:, 1 - core], lambda: b["orx"], partner_c).start()

    for d in range(1, half):
        made(("NRET", d)).wait_recv()
    for a in range(2):
        made(("SC", a)).wait_recv()
    for n in range(tiles):
        cols = slice(n * tile, (n + 1) * tile)
        back = b["tn"][1, :, :, cols].reshape(half * stride, tile)
        total = dot(b["woth"][0], back) + dot(b["woth"][1], back)
        total = total + b["s"][1, 0, :, cols].astype(f32) + b["sr"][1, :, cols].astype(f32)
        b["ao"][:, cols] = total.astype(bf)
    copy(("AY", 0), lambda: b["ao"], lambda: b["ar"], partner_y).start()

    made(("OC", 0)).wait_recv()
    for a in range(2):
        b["oq"][a] = (b["o"][a, core].astype(f32) + b["orx"][a].astype(f32)).astype(bf)
    copy(("OY", 0), lambda: b["oq"].at[1 - row_of], lambda: b["oy"], partner_y).start()

    for n in range(tiles):
        cols = slice(n * tile, (n + 1) * tile)
        back = b["tn"][0, :, :, cols].reshape(half * stride, tile)
        total = dot(b["wown"][0, 0], back) + dot(b["wown"][0, 1], back)
        b["acc"][:, cols] = (
            total + b["s"][0, 0, :, cols].astype(f32) + b["sr"][0, :, cols].astype(f32)
        )
    made(("OY", 0)).wait_recv()
    mix_out[...] = (b["oq"][row_of].astype(f32) + b["oy"][...].astype(f32)).astype(bf)

    for d in range(half):
        made(("FRET", d)).wait_recv()
    made(("AY", 0)).wait_recv()
    for n in range(tiles):
        cols = slice(n * tile, (n + 1) * tile)
        back = b["tf"][:, :, cols].reshape(half * stride, tile)
        total = dot(b["wown"][1, 0], back) + dot(b["wown"][1, 1], back)
        total = total + b["acc"][:, cols] + b["ar"][:, cols].astype(f32)
        exp_out[:, cols] = total.astype(bf)

    conditional = {("KVF", 0): side == 0}
    for d in range(1, half):
        conditional[("KVN", d)] = near_to[d] > me
        conditional[("KVC", d)] = side == 1
    for name in copies:
        if name in conditional:

            @pl.when(conditional[name])
            def _(name=name):
                made(name).wait_send()

        else:
            made(name).wait_send()
    for position in range(ep):
        core_forward(position).wait_send()
        back_copy(position).wait_send()
        if position in far_places:
            cross_copy(position).wait_send()


def fused(sizes, args):
    scratch = sizes.scratch()
    keys = list(scratch)
    _, count = sizes.names()
    vmem = pl.BlockSpec(memory_space=pltpu.VMEM)
    smem = pl.BlockSpec(memory_space=pltpu.SMEM)
    hbm = pl.BlockSpec(memory_space=pltpu.HBM)
    return pl.pallas_call(
        functools.partial(fused_kernel, sizes, keys),
        out_shape=(
            jax.ShapeDtypeStruct((sizes.own, sizes.width), jnp.bfloat16),
            jax.ShapeDtypeStruct((sizes.tokens, sizes.width), jnp.bfloat16),
        ),
        in_specs=[smem] + [vmem] * 5 + [hbm] * 13,
        out_specs=(vmem, vmem),
        scratch_shapes=[pltpu.VMEM(shape, dtype) for shape, dtype in scratch.values()]
        + [
            pltpu.SemaphoreType.DMA((count,)),
            pltpu.SemaphoreType.DMA((count,)),
            pltpu.SemaphoreType.DMA((13,)),
        ],
        compiler_params=pltpu.CompilerParams(
            collective_id=0, has_side_effects=True, vmem_limit_bytes=VMEM_LIMIT
        ),
        name="layer",
    )(*args)


VMEM_LIMIT = 67043328


def fused_body(sizes, *arrays):
    (
        mixer_input,
        mixer_gain,
        query_one,
        query_two,
        key_one,
        key_two,
        value_weight,
        lambdas,
        head_gain,
        output_weight,
        expert_input,
        expert_gain,
        routes,
        route_weight,
        expert_gate,
        expert_up,
        expert_down,
        shared_gate,
        shared_up,
        shared_down,
    ) = arrays
    info = jnp.concatenate(
        [
            routes.T.astype(jnp.float32),
            route_weight.T,
            jnp.zeros((4, sizes.tokens), jnp.float32),
        ],
        axis=0,
    )
    return fused(
        sizes,
        (
            lambdas,
            info,
            expert_input,
            expert_gain.reshape(1, -1),
            mixer_gain.reshape(1, -1),
            head_gain.reshape(1, -1),
            mixer_input,
            query_one,
            query_two,
            key_one,
            key_two,
            value_weight,
            output_weight,
            expert_gate,
            expert_up,
            expert_down,
            shared_gate,
            shared_up,
            shared_down,
        ),
    )


def body(*arrays):
    ep_size, tp_size = lax.axis_size("ep"), lax.axis_size("tp")
    mixer_input, query_one, key_one = arrays[0], arrays[2], arrays[4]
    head_gain, expert_input, routes = arrays[8], arrays[10], arrays[12]
    expert_gate, shared_gate = arrays[14], arrays[17]
    rows, width = mixer_input.shape
    tokens, top_count = routes.shape
    local_experts = expert_gate.shape[0]
    capacity = max(2, 5 * tokens * top_count // (4 * local_experts * ep_size))
    fits = (
        tp_size == 4
        and ep_size % 2 == 0
        and ep_size >= 4
        and local_experts == 1
        and top_count == 2
        and key_one.shape[1] == HEAD
        and query_one.shape[1] == 2 * HEAD
        and head_gain.shape[0] == 128
        and tokens == 128
        and rows % (16 * tp_size) == 0
        and rows % 128 == 0
        and width % 512 == 0
        and expert_input.shape[1] == width
        and capacity % 8 == 0
    )
    if fits:
        sizes = Sizes(
            ep_size,
            tp_size,
            rows,
            width,
            tokens,
            expert_gate.shape[2],
            shared_gate.shape[1],
            capacity,
            head_gain.shape[0],
        )
        if sizes.vmem_bytes() + 8 * 2**20 <= VMEM_LIMIT:
            return fused_body(sizes, *arrays)
    return general_body(*arrays)


def solution(mesh):
    in_specs = (
        P("ep", None),
        P(),
        P(None, "tp"),
        P(None, "tp"),
        P(None, "tp"),
        P(None, "tp"),
        P(None, "tp"),
        P("tp"),
        P(),
        P("tp", None),
        P(("ep", "tp"), None),
        P(),
        P(("ep", "tp"), None),
        P(("ep", "tp"), None),
        P("ep", None, "tp"),
        P("ep", None, "tp"),
        P("ep", "tp", None),
        P(None, "tp"),
        P(None, "tp"),
        P("tp", None),
    )
    out_specs = (P(("ep", "tp"), None), P(("ep", "tp"), None))
    return jax.shard_map(body, mesh=mesh, in_specs=in_specs, out_specs=out_specs, check_vma=False)
```

```python
import functools
import math

import jax
import jax.numpy as jnp
from jax import lax
from jax.experimental import pallas as pl
from jax.experimental.pallas import tpu as pltpu
from jax.sharding import PartitionSpec as P

HEAD = 64


EPS = 1e-06
NEG = -1e30


def normalize(activations, scaling):
    values = activations.astype(jnp.float32)
    factor = lax.rsqrt(jnp.mean(values * values, axis=-1, keepdims=True) + EPS)
    return (values * factor * scaling).astype(jnp.bfloat16)


def attention_kernel(
    shape, rank_ref, lambdas_ref, queries_ref, keys_ref, gain_ref, out_ref, maxima, totals, weighted
):
    rows, chunk, local_kv, group, value_dim = shape
    rank = rank_ref[0]
    maxima[...] = jnp.full(maxima.shape, NEG, jnp.float32)
    totals[...] = jnp.zeros(totals.shape, jnp.float32)
    weighted[...] = jnp.zeros(weighted.shape, jnp.float32)
    heads = local_kv * group
    key_cols = local_kv * HEAD
    chunks = rows // chunk
    scale = HEAD**-0.5 * math.log2(math.e)

    def block(index, masked):
        start = pl.multiple_of(index * rows, rows)
        for kv in range(local_kv):
            value_start = 2 * key_cols + kv * value_dim
            for part in range(chunks):
                span = (part + 1) * chunk if masked else rows
                values = keys_ref[pl.ds(start, span), value_start : value_start + value_dim]
                for which in range(2):
                    first = which * key_cols + kv * HEAD
                    keys = keys_ref[pl.ds(start, span), first : first + HEAD]
                    for g in range(group):
                        head = kv * group + g
                        col = (which * heads + head) * HEAD
                        queries = queries_ref[part * chunk : (part + 1) * chunk, col : col + HEAD]
                        scores = lax.dot_general(
                            queries,
                            keys,
                            (((1,), (1,)), ((), ())),
                            preferred_element_type=jnp.float32,
                        )
                        if masked:
                            row = part * chunk + lax.broadcasted_iota(jnp.int32, scores.shape, 0)
                            col_pos = lax.broadcasted_iota(jnp.int32, scores.shape, 1)
                            scores = jnp.where(col_pos <= row, scores, NEG)
                        slot = (which * heads + head) * chunks + part
                        earlier = maxima[slot]
                        latest = jnp.maximum(earlier, jnp.max(scores, axis=1, keepdims=True))
                        shrink = jnp.exp2((earlier - latest) * scale)
                        weights = jnp.exp2((scores - latest[:, :1]) * scale)
                        totals[slot] = totals[slot] * shrink + jnp.sum(
                            weights, axis=1, keepdims=True
                        )
                        weighted[slot] = weighted[slot] * shrink[:, :1] + jnp.dot(
                            weights.astype(jnp.bfloat16),
                            values,
                            preferred_element_type=jnp.float32,
                        )
                        maxima[slot] = latest

    def earlier_block(index, carry):
        block(index, False)
        return carry

    lax.fori_loop(0, rank, earlier_block, 0)
    block(rank, True)
    for head in range(heads):
        for part in range(chunks):
            one = head * chunks + part
            two = (heads + head) * chunks + part
            combined = (
                weighted[one] / totals[one][:, :1]
                - lambdas_ref[head] * (weighted[two] / totals[two][:, :1])
            )
            factor = lax.rsqrt(jnp.mean(combined * combined, axis=1, keepdims=True) + EPS)
            out_ref[
                part * chunk : (part + 1) * chunk, head * value_dim : (head + 1) * value_dim
            ] = (combined * factor * gain_ref[...]).astype(jnp.bfloat16)


def attention(queries, keys, rank, lambdas, head_gain, local_kv, group):
    rows = queries.shape[0]
    value_dim = head_gain.shape[0]
    heads = local_kv * group
    chunk = min(128, rows)
    slots = 2 * heads * (rows // chunk)
    vmem = pl.BlockSpec(memory_space=pltpu.VMEM)
    smem = pl.BlockSpec(memory_space=pltpu.SMEM)
    scores = heads * 2 * rows * keys.shape[0]
    return pl.pallas_call(
        functools.partial(attention_kernel, (rows, chunk, local_kv, group, value_dim)),
        out_shape=jax.ShapeDtypeStruct((rows, heads * value_dim), jnp.bfloat16),
        in_specs=[smem, smem, vmem, vmem, vmem],
        out_specs=vmem,
        scratch_shapes=[
            pltpu.VMEM((slots, chunk, 128), jnp.float32),
            pltpu.VMEM((slots, chunk, 128), jnp.float32),
            pltpu.VMEM((slots, chunk, value_dim), jnp.float32),
        ],
        compiler_params=pltpu.CompilerParams(vmem_limit_bytes=48 * 1024 * 1024),
        cost_estimate=pl.CostEstimate(
            flops=8 * scores * HEAD, bytes_accessed=keys.size * 2, transcendentals=scores
        ),
        name="attention",
    )(rank.reshape(1), lambdas, queries, keys, head_gain.reshape(1, value_dim))


def swap(rows, axis, size, distance):
    return lax.ppermute(rows, axis, [(i, i ^ distance) for i in range(size)])


def gather_near(block, axis, size, ahead=None):
    places = {0: block}
    distance = size // 2
    while distance:
        for place in sorted(places):
            moved = swap(places[place], axis, size, distance)
            if ahead is not None:
                moved, ahead = lax.optimization_barrier((moved, ahead))
            places[place ^ distance] = moved
        ahead = None
        distance //= 2
    return [places[place] for place in range(size)]


def scatter_near(partials, axis, size):
    sums = dict(enumerate(partials))
    distance = 1
    while distance < size:
        kept = [place for place in sorted(sums) if not place & distance]
        moved = {
            place: swap(sums[place ^ distance].astype(jnp.bfloat16), axis, size, distance)
            for place in kept
        }
        sums = {
            place: sums[place].astype(jnp.float32) + moved[place].astype(jnp.float32)
            for place in kept
        }
        distance *= 2
    return sums[0]


def general_body(
    mixer_input,
    mixer_gain,
    query_one,
    query_two,
    key_one,
    key_two,
    value_weight,
    lambdas,
    head_gain,
    output_weight,
    expert_input,
    expert_gain,
    routes,
    route_weight,
    expert_gate,
    expert_up,
    expert_down,
    shared_gate,
    shared_up,
    shared_down,
):
    ep_size = lax.axis_size("ep")
    tp_size = lax.axis_size("tp")
    ep_rank = lax.axis_index("ep")
    mixer_rows = mixer_input.shape[0]
    model_width = mixer_input.shape[1]
    query_cols = query_one.shape[1]
    key_cols = key_one.shape[1]
    value_dim = head_gain.shape[0]
    local_kv = key_cols // HEAD
    local_heads = query_cols // HEAD
    group_size = local_heads // local_kv
    normed = normalize(mixer_input, mixer_gain)

    def project(weights):
        return jnp.concatenate(
            [
                jnp.dot(normed, weight, preferred_element_type=jnp.float32).astype(jnp.bfloat16)
                for weight in weights
            ],
            axis=1,
        )

    key_values = project([key_one, key_two, value_weight])
    query_part = project([query_one, query_two])
    arrived = lax.all_gather(key_values, "ep", axis=0, tiled=True)
    head_rows = attention(
        query_part, arrived, ep_rank, lambdas, head_gain, local_kv, group_size
    )
    tp_rank = lax.axis_index("tp")
    own_rows = mixer_rows // tp_size

    def mixer_place(place):
        rows = lax.dynamic_slice_in_dim(head_rows, (tp_rank ^ place) * own_rows, own_rows, 0)
        return jnp.dot(rows, output_weight, preferred_element_type=jnp.float32).astype(
            jnp.bfloat16
        )

    mixer_sum = scatter_near(
        [mixer_place(place) for place in range(tp_size)], "tp", tp_size
    ).astype(jnp.bfloat16)

    token_rows = expert_input.shape[0]
    normed_experts = normalize(expert_input, expert_gain)
    experts_local = expert_gate.shape[0]
    expert_count = experts_local * ep_size
    top_count = routes.shape[1]
    capacity = max(2, 5 * token_rows * top_count // (4 * expert_count))
    slot_count = expert_count * capacity
    flat_routes = routes.reshape(-1)
    onehot = (flat_routes[:, None] == jnp.arange(expert_count, dtype=jnp.int32)[None, :]).astype(
        jnp.int32
    )
    slot_place = jnp.sum((jnp.cumsum(onehot, axis=0) - onehot) * onehot, axis=1)
    slot_ids = (flat_routes * capacity + slot_place).reshape(token_rows, top_count)
    slot_match = jnp.arange(slot_count, dtype=jnp.int32)[:, None, None] == slot_ids[None, :, :]
    select = jnp.any(slot_match, axis=2).astype(jnp.bfloat16)
    outgoing = jnp.dot(select, normed_experts, preferred_element_type=jnp.float32).astype(
        jnp.bfloat16
    )
    pair_rows = experts_local * capacity
    outgoing = outgoing.reshape(ep_size, pair_rows, model_width)
    outgoing, key_values = lax.optimization_barrier((outgoing, key_values))
    received = lax.all_to_all(outgoing, "ep", split_axis=0, concat_axis=0, tiled=True)
    received = received.reshape(ep_size, experts_local, capacity, model_width)
    if experts_local == 1:
        received = received.reshape(ep_size * capacity, model_width)

    def shared_expert(rows):
        gated = jnp.dot(rows, shared_gate, preferred_element_type=jnp.float32)
        lifted = jnp.dot(rows, shared_up, preferred_element_type=jnp.float32)
        hidden = (jax.nn.silu(gated) * lifted).astype(jnp.bfloat16)
        return jnp.dot(hidden, shared_down, preferred_element_type=jnp.float32).astype(
            jnp.bfloat16
        )

    def routed_expert(rows):
        if experts_local == 1:
            gated = jnp.dot(rows, expert_gate[0], preferred_element_type=jnp.float32)
            lifted = jnp.dot(rows, expert_up[0], preferred_element_type=jnp.float32)
            hidden = (jax.nn.silu(gated) * lifted).astype(jnp.bfloat16)
            return jnp.dot(hidden, expert_down[0], preferred_element_type=jnp.float32).astype(
                jnp.bfloat16
            )
        gated = jnp.einsum("secd,edf->secf", rows, expert_gate, preferred_element_type=jnp.float32)
        lifted = jnp.einsum("secd,edf->secf", rows, expert_up, preferred_element_type=jnp.float32)
        hidden = (jax.nn.silu(gated) * lifted).astype(jnp.bfloat16)
        return jnp.einsum(
            "secf,efd->secd", hidden, expert_down, preferred_element_type=jnp.float32
        ).astype(jnp.bfloat16)

    shared_places = gather_near(normed_experts, "tp", tp_size)
    routed_places = gather_near(received, "tp", tp_size, head_rows)
    shared_result = scatter_near([shared_expert(rows) for rows in shared_places], "tp", tp_size)
    routed_result = scatter_near(
        [routed_expert(rows) for rows in routed_places], "tp", tp_size
    ).astype(jnp.bfloat16)
    returned = lax.all_to_all(
        routed_result.reshape(ep_size, pair_rows, model_width),
        "ep",
        split_axis=0,
        concat_axis=0,
        tiled=True,
    )
    returned = returned.reshape(slot_count, model_width)
    spread = jnp.sum(
        jnp.where(
            jnp.arange(slot_count, dtype=jnp.int32)[None, None, :] == slot_ids[:, :, None],
            route_weight[:, :, None],
            0.0,
        ),
        axis=1,
    )
    upper = lax.reduce_precision(spread, 8, 7)
    lower = lax.reduce_precision(spread - upper, 8, 7)
    routed_total = jnp.dot(
        upper.astype(jnp.bfloat16), returned, preferred_element_type=jnp.float32
    ) + jnp.dot(lower.astype(jnp.bfloat16), returned, preferred_element_type=jnp.float32)
    expert_output = (routed_total + shared_result).astype(jnp.bfloat16)
    return (mixer_sum, expert_output)


def chunk_order(half):
    near = [("n", d) for d in range(half)]
    far = [("f", d) for d in range(half)]
    early = half // 2
    return near[:1] + far[:early] + near[1:] + far[early:]


def padded(rows):
    return -(-rows // 16) * 16


class Sizes:
    def __init__(self, ep, tp, rows, width, tokens, hidden, shared, capacity, value_dim):
        self.ep, self.tp, self.rows, self.width = ep, tp, rows, width
        self.tokens, self.hidden, self.shared = tokens, hidden, shared
        self.cap, self.stride = capacity, padded(capacity)
        self.value_dim = value_dim
        self.half = ep // 2
        self.own = rows // tp
        self.tile = min(512, width)

    def names(self):
        half, ep = self.half, self.ep
        groups = (
            [("XY", 0), ("INFO", 0), ("XC", 0), ("XC", 1)]
            + [("FAR", d) for d in range(half)]
            + [("NEAR", d, a) for d in range(1, half) for a in range(2)]
            + [("FY", d) for d in range(half)]
            + [("NRET", d) for d in range(1, half)]
            + [("FRET", d) for d in range(half)]
            + [("SC", 0), ("SC", 1), ("AY", 0), ("KVF", 0), ("OC", 0), ("OY", 0)]
            + [("KVN", d) for d in range(1, half)]
            + [("KVC", d) for d in range(1, half)]
        )
        table = {name: number for number, name in enumerate(groups)}
        first = len(groups)
        table["RC"], table["PC"], table["QY"] = first, first + ep, first + 2 * ep
        return table, first + 3 * ep

    def scratch(self):
        bf, f32 = jnp.bfloat16, jnp.float32
        ep, half, width, stride = self.ep, self.half, self.width, self.stride
        tokens, rows, hidden, shared = self.tokens, self.rows, self.hidden, self.shared
        vd = self.value_dim
        return dict(
            mx=((rows, width), bf),
            wq=((width, 4 * HEAD), bf),
            wk=((2 * HEAD, width), bf),
            x=((tokens, width), bf),
            info=((8, tokens), f32),
            ids=((2, tokens), jnp.int32),
            gates=((2, tokens), f32),
            wv=((width, vd), bf),
            wo=((2 * vd, width), bf),
            wg=((width, hidden), bf),
            wu=((width, hidden), bf),
            wd=((hidden, width), bf),
            sg=((width, shared), bf),
            su=((width, shared), bf),
            sd=((shared, width), bf),
            xb=((2, 2, tokens, width), bf),
            other=((8, tokens), f32),
            outf=((half, stride, width), bf),
            outn=((half, 2, stride, width), bf),
            r=((ep, 2, 2, stride, width), bf),
            p=((ep, 2, 2, stride, width), bf),
            pr=((ep, 2, stride, width), bf),
            q=((ep, 2, stride, width), bf),
            qr=((ep, stride, width), bf),
            fb=((ep, stride, width), bf),
            tn=((2, half, stride, width), bf),
            tf=((half, stride, width), bf),
            s=((2, 2, tokens, width), bf),
            sr=((2, tokens, width), bf),
            ao=((tokens, width), bf),
            ar=((tokens, width), bf),
            acc=((tokens, width), f32),
            wown=((2, 2, tokens, half * stride), bf),
            woth=((2, tokens, half * stride), bf),
            nm=((rows, width), bf),
            qs=((2, 2, rows, 2 * HEAD), bf),
            kv=((ep, rows, 2 * HEAD + vd), bf),
            sc=((2, ep, rows, rows), f32),
            stat=((2, rows, 128), f32),
            tot=((2, rows, 128), f32),
            pv=((2, rows, vd), f32),
            hr=((rows, 2 * vd), bf),
            o=((2, 2, self.own, width), bf),
            orx=((2, self.own, width), bf),
            oq=((2, self.own, width), bf),
            oy=((self.own, width), bf),
        )

    def vmem_bytes(self):
        total = 0
        for shape, dtype in self.scratch().values():
            size = jnp.dtype(dtype).itemsize
            for extent in shape[:-1]:
                size *= extent
            total += size * (-(-shape[-1] // 128) * 128)
        return total


def step_plan(half):
    early = half // 2
    plan = {0: []}
    late = half - 1
    for d in range(early):
        plan[1 + d] = [("crossed", d), ("core_sum", "n", 0) if d == 0 else ("core_sum", "f", d - 1)]
    first = 1 + early
    for d in range(1, half):
        actions = [("arrive_near", d)]
        if d == 1:
            actions += [("core_sum", "f", early - 1), ("relay_kv",)]
        else:
            actions += [("core_sum", "n", d - 1)]
            if d - 2 < early:
                actions += [("side_sum", d - 2)]
        plan[first + d - 1] = actions
    for d in range(early, half):
        actions = [("arrive_far", d)]
        if d == early:
            actions += [("core_sum", "n", half - 1)]
            actions += [("side_sum", e) for e in range(max(half - 2, 0), early)]
            actions += [("kv_arrivals",), ("head", 0), ("head", 1)]
        else:
            actions += [("core_sum", "f", d - 1)]
        if d == late:
            actions += [("project_out",)]
        actions += [("crossed", d)]
        plan[first + late + d - early] = actions
    last = 2 * half
    plan[last] = [("core_sum", "f", half - 1)]
    plan[last] += [("side_sum", d) for d in range(early, half - 1)]
    plan[last] += [("mix_sum",), ("other_rows",), ("side_sum", half - 1), ("own_rows",)]
    return plan


class Later:
    def __init__(self, start):
        self.start = start


def fused_kernel(sizes, keys, *refs):
    lam, xgain, mgain, hgain = refs[:4]
    (h_x, h_ids, h_gates, h_mx, h_q1, h_q2, h_k1, h_k2, h_v) = refs[4:13]
    (h_wo, h_g, h_u, h_d, h_sg, h_su, h_sd) = refs[13:20]
    mix_out, exp_out = refs[20:22]
    b = dict(zip(keys, refs[22 : 22 + len(keys)]))
    send_sem, recv_sem, load_sem = refs[22 + len(keys) :]
    x, info = b["x"], b["info"]
    half, ep, width, stride, cap = sizes.half, sizes.ep, sizes.width, sizes.stride, sizes.cap
    tokens, rows, tile, vd = sizes.tokens, sizes.rows, sizes.tile, sizes.value_dim
    f32, bf = jnp.float32, jnp.bfloat16
    table, _ = sizes.names()
    order = chunk_order(half)
    place = {name: number for number, name in enumerate(order)}

    me = lax.axis_index("ep")
    tp = lax.axis_index("tp")
    side = me // half
    spot = me % half
    row_of = tp // 2
    core = tp % 2
    tiles = width // tile

    near_to = [side * half + (spot + d) % half for d in range(half)]
    near_by = [side * half + (spot + half - d) % half for d in range(half)]
    far_to = [(1 - side) * half + (spot + d) % half for d in range(half)]
    far_by = [(1 - side) * half + (spot + half - d) % half for d in range(half)]
    early = half // 2

    def near(d):
        return (near_to[d], tp)

    def near_from(d):
        return (near_by[d], tp)

    def far(d):
        return (far_to[d], tp)

    def far_from(d):
        return (far_by[d], tp)

    partner_y = (me, (1 - row_of) * 2 + core)
    partner_c = (me, row_of * 2 + 1 - core)

    def remote(number, source, target, device):
        return pltpu.make_async_remote_copy(
            src_ref=source,
            dst_ref=target,
            send_sem=send_sem.at[number],
            recv_sem=recv_sem.at[number],
            device_id=device,
            device_id_type=pl.DeviceIdType.MESH,
        )

    copies = {}

    def made(name):
        source, target, device = copies[name]
        return remote(table[name], source(), target(), device)

    def copy(name, source, target, device):
        copies[name] = (source, target, device)
        return Later(lambda: made(name).start())

    def dot(left, right):
        return jnp.dot(left, right, preferred_element_type=f32)

    for d in range(half):
        position = place[("f", d)]
        copies[("FY", d)] = (
            lambda position=position: b["r"].at[position, 0, 0, pl.ds(0, cap)],
            lambda position=position: b["r"].at[position, 0, 1, pl.ds(0, cap)],
            partner_y,
        )
        copies[("FRET", d)] = (
            lambda position=position: b["fb"].at[position, pl.ds(0, cap)],
            lambda d=d: b["tf"].at[d, pl.ds(0, cap)],
            far_from(d),
        )
    for d in range(1, half):
        position = place[("n", d)]
        copies[("NRET", d)] = (
            lambda position=position: b["q"].at[position, :, pl.ds(0, cap)],
            lambda d=d: b["tn"].at[:, d, pl.ds(0, cap)],
            near_from(d),
        )

    loads = {}
    pairs = dict(
        x=(h_x, b["x"]),
        ids=(h_ids, b["ids"]),
        gates=(h_gates, b["gates"]),
        mx=(h_mx, b["mx"]),
        q1=(h_q1, b["wq"].at[:, : 2 * HEAD]),
        q2=(h_q2, b["wq"].at[:, 2 * HEAD :]),
        k1=(h_k1, b["wk"].at[:HEAD]),
        k2=(h_k2, b["wk"].at[HEAD:]),
        v=(h_v, b["wv"]),
        sg=(h_sg, b["sg"]),
        su=(h_su, b["su"]),
        sd=(h_sd, b["sd"]),
        wg=(h_g.at[0], b["wg"]),
        wu=(h_u.at[0], b["wu"]),
        wd=(h_d.at[0], b["wd"]),
        wo=(h_wo, b["wo"]),
    )
    for number, (name, (source, target)) in enumerate(pairs.items()):
        loads[name] = pltpu.make_async_copy(source, target, load_sem.at[number])
        loads[name].start()

    barrier = pltpu.get_barrier_semaphore()
    peers = [near(d) for d in range(1, half)] + [far(d) for d in range(half)]
    peers += [partner_y, partner_c]
    for device in peers:
        pl.semaphore_signal(
            barrier, inc=1, device_id=device, device_id_type=pl.DeviceIdType.MESH
        )

    def norm_rows(source, target, count, gain):
        step = min(32, count)

        @pl.loop(0, count // step)
        def _(index):
            at = pl.ds(pl.multiple_of(index * step, step), step)
            values = source[at, :].astype(f32)
            factor = lax.rsqrt(jnp.mean(values * values, axis=-1, keepdims=True) + EPS)
            target[at, :] = (values * factor * gain[...]).astype(bf)

    loads["x"].wait()
    norm_rows(x, b["xb"].at[0, 0], tokens, xgain)
    loads["ids"].wait()
    loads["gates"].wait()
    info[...] = jnp.zeros((8, tokens), f32)
    info[0:2, :] = b["ids"][...].astype(f32)
    info[2:4, :] = b["gates"][...]

    earlier = (
        lax.broadcasted_iota(jnp.int32, (tokens, tokens), 0)
        < lax.broadcasted_iota(jnp.int32, (tokens, tokens), 1)
    ).astype(bf)
    padded_ep = -(-ep // 8) * 8
    relative = lax.broadcasted_iota(jnp.int32, (padded_ep, tokens), 0)
    in_far = relative >= half
    turn = jnp.where(in_far, relative - half, relative) + spot
    turn = jnp.where(turn >= half, turn - half, turn)
    names_half = jnp.where(in_far, 1 - side, side)
    expert = (names_half * half + turn).astype(f32)

    def routing(info_ref):
        first = info_ref[0:1, :] == expert
        second = info_ref[1:2, :] == expert
        named = jnp.where(first | second, 1.0, 0.0)
        position = dot(named.astype(bf), earlier)
        position = jnp.where(named > 0.0, position, -1.0)
        weight = jnp.where(first, info_ref[2:3, :], 0.0) + jnp.where(second, info_ref[3:4, :], 0.0)
        return position, weight

    slot = lax.broadcasted_iota(jnp.int32, (stride, tokens), 0).astype(f32)

    def chosen(position, which):
        return slot == position[which : which + 1, :]

    def select(position, which):
        return jnp.concatenate(
            [jnp.where(chosen(position, k), 1.0, 0.0) for k in which], axis=0
        ).astype(bf)

    def spread(position, weight, which):
        stacked = jnp.concatenate(
            [jnp.where(chosen(position, k), weight[k : k + 1, :], 0.0) for k in which], axis=0
        )
        turned = stacked.T
        upper = turned.astype(bf)
        return upper, (turned - upper.astype(f32)).astype(bf)

    own_place, own_weight = routing(info)
    near_set = list(range(half))
    far_set = list(range(half, 2 * half))
    select_near = select(own_place, near_set)
    select_far = select(own_place, far_set)

    pl.semaphore_wait(barrier, len(peers))
    copy(("XY", 0), lambda: b["xb"].at[0, 0], lambda: b["xb"].at[1, 0], partner_y).start()
    copy(("INFO", 0), lambda: info, lambda: b["other"], partner_y).start()
    copy(("XC", 0), lambda: b["xb"].at[0, 0], lambda: b["xb"].at[0, 1], partner_c).start()

    def pick(select_rows, source, store):
        for n in range(tiles):
            cols = slice(n * tile, (n + 1) * tile)
            picked = dot(select_rows, source[:, cols]).astype(bf)
            for d in range(half):
                store(d, cols, picked[d * stride : (d + 1) * stride, :])

    def store_near(a):
        def store(d, cols, value):
            b["outn"][d, a, :, cols] = value

        return store

    def store_far(d, cols, value):
        b["outf"][d, :, cols] = value

    pick(select_near, b["xb"].at[0, 0], store_near(0))

    def start_near(a):
        for d in range(1, half):
            copy(
                ("NEAR", d, a),
                lambda d=d: b["outn"].at[d, a, pl.ds(0, cap)],
                lambda d=d: b["r"].at[place[("n", d)], 0, a, pl.ds(0, cap)],
                near(d),
            ).start()

    start_near(0)
    pick(select_far, b["xb"].at[0, 0], store_far)

    def start_far(d):
        copy(
            ("FAR", d),
            lambda: b["outf"].at[d, pl.ds(0, cap)],
            lambda: b["r"].at[place[("f", d)], 0, 0, pl.ds(0, cap)],
            far(d),
        ).start()

    for d in range(early):
        start_far(d)

    loads["mx"].wait()
    norm_rows(b["mx"], b["nm"], rows, mgain)
    for name in ("q1", "q2", "k1", "k2", "v"):
        loads[name].wait()
    lane = lax.broadcasted_iota(jnp.int32, (rows, 2 * HEAD), 1)
    b["kv"][me, :, : 2 * HEAD] = lax.dot_general(
        b["nm"][...], b["wk"][...], (((1,), (1,)), ((), ())), preferred_element_type=f32
    ).astype(bf)
    b["kv"][me, :, 2 * HEAD :] = dot(b["nm"][...], b["wv"][...]).astype(bf)

    copy(("KVF", 0), lambda: b["kv"].at[me], lambda: b["kv"].at[me], far(0))

    @pl.when(side == 0)
    def _():
        made(("KVF", 0)).start()

    for d in range(1, half):
        copy(("KVN", d), lambda: b["kv"].at[me], lambda: b["kv"].at[me], near(d))

        @pl.when(near_to[d] > me)
        def _(d=d):
            made(("KVN", d)).start()

    for m in range(2):
        queries = dot(b["nm"][...], b["wq"][:, m * 2 * HEAD : (m + 1) * 2 * HEAD])
        turned = pltpu.roll(queries, HEAD, 1)
        keep = (lane < HEAD) if m == 0 else (lane >= HEAD)
        for g in range(2):
            source = queries if g == m else turned
            b["qs"][m, g] = jnp.where(keep, source, 0.0).astype(bf)

    def shared_expert(a):
        both = b["xb"][a].reshape(2 * tokens, width)
        gated = dot(both, b["sg"][...])
        lifted = dot(both, b["su"][...])
        hidden = (jax.nn.silu(gated) * lifted).astype(bf)
        for n in range(tiles):
            cols = slice(n * tile, (n + 1) * tile)
            part = dot(hidden, b["sd"][:, cols]).astype(bf)
            b["s"][a, 0, :, cols] = part[:tokens]
            b["s"][a, 1, :, cols] = part[tokens:]

    for name in ("sg", "su", "sd"):
        loads[name].wait()
    made(("XC", 0)).wait_recv()
    shared_expert(0)
    copy(("SC", 0), lambda: b["s"].at[0, 1], lambda: b["sr"].at[0], partner_c).start()

    made(("XY", 0)).wait_recv()
    made(("INFO", 0)).wait_recv()
    copy(("XC", 1), lambda: b["xb"].at[1, 0], lambda: b["xb"].at[1, 1], partner_c).start()
    other_place, other_weight = routing(b["other"])
    pick(select(other_place, near_set), b["xb"].at[1, 0], store_near(1))
    start_near(1)
    for d in range(early, half):
        start_far(d)
    b["r"][0, 0] = b["outn"][0]

    def core_forward(position):
        return remote(
            table["RC"] + position, b["r"].at[position, 0], b["r"].at[position, 1], partner_c
        )

    core_forward(0).start()
    for d in range(early):
        made(("FAR", d)).wait_recv()
        made(("FY", d)).start()
    for which, (at, wt, group) in enumerate(
        ((own_place, own_weight, near_set), (own_place, own_weight, far_set))
    ):
        upper, lower = spread(at, wt, group)
        b["wown"][which, 0] = upper
        b["wown"][which, 1] = lower
    upper, lower = spread(other_place, other_weight, near_set)
    b["woth"][0] = upper
    b["woth"][1] = lower
    for d in range(half):
        b["tf"][d, cap:, :] = jnp.zeros((stride - cap, width), bf)
        for a in range(2):
            b["tn"][a, d, cap:, :] = jnp.zeros((stride - cap, width), bf)
    made(("XC", 1)).wait_recv()
    shared_expert(1)
    copy(("SC", 1), lambda: b["s"].at[1, 1], lambda: b["sr"].at[1], partner_c).start()

    for name in ("wg", "wu", "wd"):
        loads[name].wait()

    def arrive_far(d):
        made(("FAR", d)).wait_recv()
        made(("FY", d)).start()

    def crossed(d):
        made(("FY", d)).wait_recv()
        core_forward(place[("f", d)]).start()

    def arrive_near(d):
        for a in range(2):
            made(("NEAR", d, a)).wait_recv()
        core_forward(place[("n", d)]).start()

    def relay_kv():
        @pl.when(side == 1)
        def _():
            slot_of = b["kv"].at[far_by[0]]
            remote(table[("KVF", 0)], slot_of, slot_of, far(0)).wait_recv()

        for d in range(1, half):
            copy(("KVC", d), lambda: b["kv"].at[far_by[0]], lambda: b["kv"].at[far_by[0]], near(d))

            @pl.when(side == 1)
            def _(d=d):
                made(("KVC", d)).start()

    far_places = [place[("f", d)] for d in range(half)]
    row_count = 4 * stride

    def back_copy(number):
        return remote(
            table["PC"] + number, b["p"].at[number, 1], b["pr"].at[number], partner_c
        )

    def cross_copy(number):
        return remote(
            table["QY"] + number,
            b["q"].at[number, 1, pl.ds(0, cap)],
            b["qr"].at[number, pl.ds(0, cap)],
            partner_y,
        )

    def core_sum(kind, d):
        position = place[(kind, d)]
        back_copy(position).wait_recv()
        for a in range(2):
            b["q"][position, a] = (
                b["p"][position, 0, a].astype(f32) + b["pr"][position, a].astype(f32)
            ).astype(bf)
        if kind == "f":
            cross_copy(position).start()
        elif d > 0:
            made(("NRET", d)).start()
        else:
            for a in range(2):
                b["tn"][a, 0, 0:cap, :] = b["q"][position, a, 0:cap, :]

    def side_sum(d):
        position = place[("f", d)]
        cross_copy(position).wait_recv()
        b["fb"][position] = (
            b["q"][position, 0].astype(f32) + b["qr"][position].astype(f32)
        ).astype(bf)
        made(("FRET", d)).start()

    def kv_arrival(name, source, d):
        block = b["kv"].at[source]
        remote(table[(name, d)], block, block, near(d)).wait_recv()

    def kv_arrivals():
        for d in range(1, half):

            @pl.when(near_by[d] < me)
            def _(d=d):
                kv_arrival("KVN", near_by[d], d)

            @pl.when(side == 1)
            def _(d=d):
                kv_arrival("KVC", (1 - side) * half + (spot + half - d) % half, d)

    scale = HEAD**-0.5 * math.log2(math.e)
    row_place = me * rows + lax.broadcasted_iota(jnp.int32, (rows, rows), 0)
    col_place = lax.broadcasted_iota(jnp.int32, (rows, rows), 1)
    halves = [slice(c * 128, (c + 1) * 128) for c in range(rows // 128)]

    def head(g):
        b["stat"][...] = jnp.full((2, rows, 128), NEG, f32)
        b["tot"][...] = jnp.zeros((2, rows, 128), f32)
        b["pv"][...] = jnp.zeros((2, rows, vd), f32)

        def score(j, carry):
            keys_j = b["kv"][j, :, 0 : 2 * HEAD]
            for m in range(2):
                scores = lax.dot_general(
                    b["qs"][m, g], keys_j, (((1,), (1,)), ((), ())), preferred_element_type=f32
                )
                scores = jnp.where(j * rows + col_place <= row_place, scores, NEG)
                b["sc"][m, j] = scores
                most = b["stat"][m]
                for cols in halves:
                    most = jnp.maximum(most, scores[:, cols])
                b["stat"][m] = most
            return carry

        lax.fori_loop(0, me + 1, score, 0)
        for m in range(2):
            most = jnp.max(b["stat"][m], axis=1, keepdims=True)
            b["stat"][m] = jnp.broadcast_to(most, (rows, 128))

        def weigh(j, carry):
            values = b["kv"][j, :, 2 * HEAD :]
            for m in range(2):
                most = b["stat"][m]
                total = b["tot"][m]
                parts = []
                for cols in halves:
                    weights = jnp.exp2((b["sc"][m, j, :, cols] - most) * scale)
                    total = total + weights
                    parts.append(weights.astype(bf))
                b["tot"][m] = total
                b["pv"][m] += dot(jnp.concatenate(parts, axis=1), values)
            return carry

        lax.fori_loop(0, me + 1, weigh, 0)
        sums = [jnp.sum(b["tot"][m], axis=1, keepdims=True) for m in range(2)]
        combined = b["pv"][0] / sums[0] - lam[g] * (b["pv"][1] / sums[1])
        factor = lax.rsqrt(jnp.mean(combined * combined, axis=1, keepdims=True) + EPS)
        b["hr"][:, g * vd : (g + 1) * vd] = (combined * factor * hgain[...]).astype(bf)

    def project_out():
        loads["wo"].wait()
        own = sizes.own
        for n in range(tiles):
            cols = slice(n * tile, (n + 1) * tile)
            part = dot(b["hr"][...], b["wo"][:, cols]).astype(bf)
            b["o"][:, :, :, cols] = part.reshape(2, 2, own, tile)
        made(("OC", 0)).start()

    def other_rows():
        for d in range(1, half):
            made(("NRET", d)).wait_recv()
        for a in range(2):
            made(("SC", a)).wait_recv()
        for n in range(tiles):
            cols = slice(n * tile, (n + 1) * tile)
            back = b["tn"][1, :, :, cols].reshape(half * stride, tile)
            total = dot(b["woth"][0], back) + dot(b["woth"][1], back)
            total = total + b["s"][1, 0, :, cols].astype(f32) + b["sr"][1, :, cols].astype(f32)
            b["ao"][:, cols] = total.astype(bf)
        made(("AY", 0)).start()

    def mix_sum():
        made(("OC", 0)).wait_recv()
        for a in range(2):
            b["oq"][a] = (b["o"][a, core].astype(f32) + b["orx"][a].astype(f32)).astype(bf)
        made(("OY", 0)).start()

    def own_rows():
        for n in range(tiles):
            cols = slice(n * tile, (n + 1) * tile)
            back = b["tn"][0, :, :, cols].reshape(half * stride, tile)
            total = dot(b["wown"][0, 0], back) + dot(b["wown"][0, 1], back)
            b["acc"][:, cols] = (
                total + b["s"][0, 0, :, cols].astype(f32) + b["sr"][0, :, cols].astype(f32)
            )

    copies[("OC", 0)] = (lambda: b["o"].at[:, 1 - core], lambda: b["orx"], partner_c)
    copies[("AY", 0)] = (lambda: b["ao"], lambda: b["ar"], partner_y)
    copies[("OY", 0)] = (lambda: b["oq"].at[1 - row_of], lambda: b["oy"], partner_y)
    schedule = step_plan(half)
    actions = dict(
        arrive_far=arrive_far,
        crossed=crossed,
        arrive_near=arrive_near,
        core_sum=core_sum,
        side_sum=side_sum,
        relay_kv=relay_kv,
        kv_arrivals=kv_arrivals,
        head=head,
        project_out=project_out,
        mix_sum=mix_sum,
        other_rows=other_rows,
        own_rows=own_rows,
    )

    def step_body(step, carry):
        for when in sorted(schedule):

            @pl.when(step == when)
            def _(when=when):
                for name, *values in schedule[when]:
                    actions[name](*values)

        @pl.when(step < ep)
        def _():
            core_forward(step).wait_recv()
            arrived = b["r"][step].reshape(row_count, width)
            gated = dot(arrived, b["wg"][...])
            lifted = dot(arrived, b["wu"][...])
            hidden = (jax.nn.silu(gated) * lifted).astype(bf)
            for n in range(tiles):
                cols = slice(n * tile, (n + 1) * tile)
                part = dot(hidden, b["wd"][:, cols]).astype(bf)
                b["p"][step, :, :, :, cols] = part.reshape(2, 2, stride, tile)
            back_copy(step).start()

        return carry

    lax.fori_loop(0, max(schedule) + 1, step_body, 0)

    made(("OY", 0)).wait_recv()
    mix_out[...] = (b["oq"][row_of].astype(f32) + b["oy"][...].astype(f32)).astype(bf)

    for d in range(half):
        made(("FRET", d)).wait_recv()
    made(("AY", 0)).wait_recv()
    for n in range(tiles):
        cols = slice(n * tile, (n + 1) * tile)
        back = b["tf"][:, :, cols].reshape(half * stride, tile)
        total = dot(b["wown"][1, 0], back) + dot(b["wown"][1, 1], back)
        total = total + b["acc"][:, cols] + b["ar"][:, cols].astype(f32)
        exp_out[:, cols] = total.astype(bf)

    conditional = {("KVF", 0): side == 0}
    for d in range(1, half):
        conditional[("KVN", d)] = near_to[d] > me
        conditional[("KVC", d)] = side == 1
    for name in copies:
        if name in conditional:

            @pl.when(conditional[name])
            def _(name=name):
                made(name).wait_send()

        else:
            made(name).wait_send()
    for position in range(ep):
        core_forward(position).wait_send()
        back_copy(position).wait_send()
        if position in far_places:
            cross_copy(position).wait_send()


def fused(sizes, args):
    scratch = sizes.scratch()
    keys = list(scratch)
    _, count = sizes.names()
    vmem = pl.BlockSpec(memory_space=pltpu.VMEM)
    smem = pl.BlockSpec(memory_space=pltpu.SMEM)
    hbm = pl.BlockSpec(memory_space=pltpu.HBM)
    return pl.pallas_call(
        functools.partial(fused_kernel, sizes, keys),
        out_shape=(
            jax.ShapeDtypeStruct((sizes.own, sizes.width), jnp.bfloat16),
            jax.ShapeDtypeStruct((sizes.tokens, sizes.width), jnp.bfloat16),
        ),
        in_specs=[smem] + [vmem] * 3 + [hbm] * 16,
        out_specs=(vmem, vmem),
        scratch_shapes=[pltpu.VMEM(shape, dtype) for shape, dtype in scratch.values()]
        + [
            pltpu.SemaphoreType.DMA((count,)),
            pltpu.SemaphoreType.DMA((count,)),
            pltpu.SemaphoreType.DMA((16,)),
        ],
        compiler_params=pltpu.CompilerParams(
            collective_id=0, has_side_effects=True, vmem_limit_bytes=VMEM_LIMIT
        ),
        name="layer",
    )(*args)


VMEM_LIMIT = 67043328


def fused_body(sizes, *arrays):
    (
        mixer_input,
        mixer_gain,
        query_one,
        query_two,
        key_one,
        key_two,
        value_weight,
        lambdas,
        head_gain,
        output_weight,
        expert_input,
        expert_gain,
        routes,
        route_weight,
        expert_gate,
        expert_up,
        expert_down,
        shared_gate,
        shared_up,
        shared_down,
    ) = arrays
    return fused(
        sizes,
        (
            lambdas,
            expert_gain.reshape(1, -1),
            mixer_gain.reshape(1, -1),
            head_gain.reshape(1, -1),
            expert_input,
            routes.T,
            route_weight.T,
            mixer_input,
            query_one,
            query_two,
            key_one.T,
            key_two.T,
            value_weight,
            output_weight,
            expert_gate,
            expert_up,
            expert_down,
            shared_gate,
            shared_up,
            shared_down,
        ),
    )


def body(*arrays):
    ep_size, tp_size = lax.axis_size("ep"), lax.axis_size("tp")
    mixer_input, query_one, key_one = arrays[0], arrays[2], arrays[4]
    head_gain, expert_input, routes = arrays[8], arrays[10], arrays[12]
    expert_gate, shared_gate = arrays[14], arrays[17]
    rows, width = mixer_input.shape
    tokens, top_count = routes.shape
    local_experts = expert_gate.shape[0]
    capacity = max(2, 5 * tokens * top_count // (4 * local_experts * ep_size))
    fits = (
        tp_size == 4
        and ep_size % 2 == 0
        and ep_size >= 4
        and local_experts == 1
        and top_count == 2
        and key_one.shape[1] == HEAD
        and query_one.shape[1] == 2 * HEAD
        and head_gain.shape[0] == 128
        and tokens == 128
        and rows % (16 * tp_size) == 0
        and rows % 128 == 0
        and width % 512 == 0
        and expert_input.shape[1] == width
        and capacity % 8 == 0
    )
    if fits:
        sizes = Sizes(
            ep_size,
            tp_size,
            rows,
            width,
            tokens,
            expert_gate.shape[2],
            shared_gate.shape[1],
            capacity,
            head_gain.shape[0],
        )
        if sizes.vmem_bytes() + 8 * 2**20 <= VMEM_LIMIT:
            return fused_body(sizes, *arrays)
    return general_body(*arrays)


def solution(mesh):
    in_specs = (
        P("ep", None),
        P(),
        P(None, "tp"),
        P(None, "tp"),
        P(None, "tp"),
        P(None, "tp"),
        P(None, "tp"),
        P("tp"),
        P(),
        P("tp", None),
        P(("ep", "tp"), None),
        P(),
        P(("ep", "tp"), None),
        P(("ep", "tp"), None),
        P("ep", None, "tp"),
        P("ep", None, "tp"),
        P("ep", "tp", None),
        P(None, "tp"),
        P(None, "tp"),
        P("tp", None),
    )
    out_specs = (P(("ep", "tp"), None), P(("ep", "tp"), None))
    return jax.shard_map(body, mesh=mesh, in_specs=in_specs, out_specs=out_specs, check_vma=False)
```

```python
import functools
import math

import jax
import jax.numpy as jnp
from jax import lax
from jax.experimental import pallas as pl
from jax.experimental.pallas import tpu as pltpu
from jax.sharding import PartitionSpec as P

HEAD = 64


EPS = 1e-06
NEG = -1e30


def normalize(activations, scaling):
    values = activations.astype(jnp.float32)
    factor = lax.rsqrt(jnp.mean(values * values, axis=-1, keepdims=True) + EPS)
    return (values * factor * scaling).astype(jnp.bfloat16)


def attention_kernel(
    shape, rank_ref, lambdas_ref, queries_ref, keys_ref, gain_ref, out_ref, maxima, totals, weighted
):
    rows, chunk, local_kv, group, value_dim = shape
    rank = rank_ref[0]
    maxima[...] = jnp.full(maxima.shape, NEG, jnp.float32)
    totals[...] = jnp.zeros(totals.shape, jnp.float32)
    weighted[...] = jnp.zeros(weighted.shape, jnp.float32)
    heads = local_kv * group
    key_cols = local_kv * HEAD
    chunks = rows // chunk
    scale = HEAD**-0.5 * math.log2(math.e)

    def block(index, masked):
        start = pl.multiple_of(index * rows, rows)
        for kv in range(local_kv):
            value_start = 2 * key_cols + kv * value_dim
            for part in range(chunks):
                span = (part + 1) * chunk if masked else rows
                values = keys_ref[pl.ds(start, span), value_start : value_start + value_dim]
                for which in range(2):
                    first = which * key_cols + kv * HEAD
                    keys = keys_ref[pl.ds(start, span), first : first + HEAD]
                    for g in range(group):
                        head = kv * group + g
                        col = (which * heads + head) * HEAD
                        queries = queries_ref[part * chunk : (part + 1) * chunk, col : col + HEAD]
                        scores = lax.dot_general(
                            queries,
                            keys,
                            (((1,), (1,)), ((), ())),
                            preferred_element_type=jnp.float32,
                        )
                        if masked:
                            row = part * chunk + lax.broadcasted_iota(jnp.int32, scores.shape, 0)
                            col_pos = lax.broadcasted_iota(jnp.int32, scores.shape, 1)
                            scores = jnp.where(col_pos <= row, scores, NEG)
                        slot = (which * heads + head) * chunks + part
                        earlier = maxima[slot]
                        latest = jnp.maximum(earlier, jnp.max(scores, axis=1, keepdims=True))
                        shrink = jnp.exp2((earlier - latest) * scale)
                        weights = jnp.exp2((scores - latest[:, :1]) * scale)
                        totals[slot] = totals[slot] * shrink + jnp.sum(
                            weights, axis=1, keepdims=True
                        )
                        weighted[slot] = weighted[slot] * shrink[:, :1] + jnp.dot(
                            weights.astype(jnp.bfloat16),
                            values,
                            preferred_element_type=jnp.float32,
                        )
                        maxima[slot] = latest

    def earlier_block(index, carry):
        block(index, False)
        return carry

    lax.fori_loop(0, rank, earlier_block, 0)
    block(rank, True)
    for head in range(heads):
        for part in range(chunks):
            one = head * chunks + part
            two = (heads + head) * chunks + part
            combined = (
                weighted[one] / totals[one][:, :1]
                - lambdas_ref[head] * (weighted[two] / totals[two][:, :1])
            )
            factor = lax.rsqrt(jnp.mean(combined * combined, axis=1, keepdims=True) + EPS)
            out_ref[
                part * chunk : (part + 1) * chunk, head * value_dim : (head + 1) * value_dim
            ] = (combined * factor * gain_ref[...]).astype(jnp.bfloat16)


def attention(queries, keys, rank, lambdas, head_gain, local_kv, group):
    rows = queries.shape[0]
    value_dim = head_gain.shape[0]
    heads = local_kv * group
    chunk = min(128, rows)
    slots = 2 * heads * (rows // chunk)
    vmem = pl.BlockSpec(memory_space=pltpu.VMEM)
    smem = pl.BlockSpec(memory_space=pltpu.SMEM)
    scores = heads * 2 * rows * keys.shape[0]
    return pl.pallas_call(
        functools.partial(attention_kernel, (rows, chunk, local_kv, group, value_dim)),
        out_shape=jax.ShapeDtypeStruct((rows, heads * value_dim), jnp.bfloat16),
        in_specs=[smem, smem, vmem, vmem, vmem],
        out_specs=vmem,
        scratch_shapes=[
            pltpu.VMEM((slots, chunk, 128), jnp.float32),
            pltpu.VMEM((slots, chunk, 128), jnp.float32),
            pltpu.VMEM((slots, chunk, value_dim), jnp.float32),
        ],
        compiler_params=pltpu.CompilerParams(vmem_limit_bytes=48 * 1024 * 1024),
        cost_estimate=pl.CostEstimate(
            flops=8 * scores * HEAD, bytes_accessed=keys.size * 2, transcendentals=scores
        ),
        name="attention",
    )(rank.reshape(1), lambdas, queries, keys, head_gain.reshape(1, value_dim))


def swap(rows, axis, size, distance):
    return lax.ppermute(rows, axis, [(i, i ^ distance) for i in range(size)])


def gather_near(block, axis, size, ahead=None):
    places = {0: block}
    distance = size // 2
    while distance:
        for place in sorted(places):
            moved = swap(places[place], axis, size, distance)
            if ahead is not None:
                moved, ahead = lax.optimization_barrier((moved, ahead))
            places[place ^ distance] = moved
        ahead = None
        distance //= 2
    return [places[place] for place in range(size)]


def scatter_near(partials, axis, size):
    sums = dict(enumerate(partials))
    distance = 1
    while distance < size:
        kept = [place for place in sorted(sums) if not place & distance]
        moved = {
            place: swap(sums[place ^ distance].astype(jnp.bfloat16), axis, size, distance)
            for place in kept
        }
        sums = {
            place: sums[place].astype(jnp.float32) + moved[place].astype(jnp.float32)
            for place in kept
        }
        distance *= 2
    return sums[0]


def general_body(
    mixer_input,
    mixer_gain,
    query_one,
    query_two,
    key_one,
    key_two,
    value_weight,
    lambdas,
    head_gain,
    output_weight,
    expert_input,
    expert_gain,
    routes,
    route_weight,
    expert_gate,
    expert_up,
    expert_down,
    shared_gate,
    shared_up,
    shared_down,
):
    ep_size = lax.axis_size("ep")
    tp_size = lax.axis_size("tp")
    ep_rank = lax.axis_index("ep")
    mixer_rows = mixer_input.shape[0]
    model_width = mixer_input.shape[1]
    query_cols = query_one.shape[1]
    key_cols = key_one.shape[1]
    value_dim = head_gain.shape[0]
    local_kv = key_cols // HEAD
    local_heads = query_cols // HEAD
    group_size = local_heads // local_kv
    normed = normalize(mixer_input, mixer_gain)

    def project(weights):
        return jnp.concatenate(
            [
                jnp.dot(normed, weight, preferred_element_type=jnp.float32).astype(jnp.bfloat16)
                for weight in weights
            ],
            axis=1,
        )

    key_values = project([key_one, key_two, value_weight])
    query_part = project([query_one, query_two])
    arrived = lax.all_gather(key_values, "ep", axis=0, tiled=True)
    head_rows = attention(
        query_part, arrived, ep_rank, lambdas, head_gain, local_kv, group_size
    )
    tp_rank = lax.axis_index("tp")
    own_rows = mixer_rows // tp_size

    def mixer_place(place):
        rows = lax.dynamic_slice_in_dim(head_rows, (tp_rank ^ place) * own_rows, own_rows, 0)
        return jnp.dot(rows, output_weight, preferred_element_type=jnp.float32).astype(
            jnp.bfloat16
        )

    mixer_sum = scatter_near(
        [mixer_place(place) for place in range(tp_size)], "tp", tp_size
    ).astype(jnp.bfloat16)

    token_rows = expert_input.shape[0]
    normed_experts = normalize(expert_input, expert_gain)
    experts_local = expert_gate.shape[0]
    expert_count = experts_local * ep_size
    top_count = routes.shape[1]
    capacity = max(2, 5 * token_rows * top_count // (4 * expert_count))
    slot_count = expert_count * capacity
    flat_routes = routes.reshape(-1)
    onehot = (flat_routes[:, None] == jnp.arange(expert_count, dtype=jnp.int32)[None, :]).astype(
        jnp.int32
    )
    slot_place = jnp.sum((jnp.cumsum(onehot, axis=0) - onehot) * onehot, axis=1)
    slot_ids = (flat_routes * capacity + slot_place).reshape(token_rows, top_count)
    slot_match = jnp.arange(slot_count, dtype=jnp.int32)[:, None, None] == slot_ids[None, :, :]
    select = jnp.any(slot_match, axis=2).astype(jnp.bfloat16)
    outgoing = jnp.dot(select, normed_experts, preferred_element_type=jnp.float32).astype(
        jnp.bfloat16
    )
    pair_rows = experts_local * capacity
    outgoing = outgoing.reshape(ep_size, pair_rows, model_width)
    outgoing, key_values = lax.optimization_barrier((outgoing, key_values))
    received = lax.all_to_all(outgoing, "ep", split_axis=0, concat_axis=0, tiled=True)
    received = received.reshape(ep_size, experts_local, capacity, model_width)
    if experts_local == 1:
        received = received.reshape(ep_size * capacity, model_width)

    def shared_expert(rows):
        gated = jnp.dot(rows, shared_gate, preferred_element_type=jnp.float32)
        lifted = jnp.dot(rows, shared_up, preferred_element_type=jnp.float32)
        hidden = (jax.nn.silu(gated) * lifted).astype(jnp.bfloat16)
        return jnp.dot(hidden, shared_down, preferred_element_type=jnp.float32).astype(
            jnp.bfloat16
        )

    def routed_expert(rows):
        if experts_local == 1:
            gated = jnp.dot(rows, expert_gate[0], preferred_element_type=jnp.float32)
            lifted = jnp.dot(rows, expert_up[0], preferred_element_type=jnp.float32)
            hidden = (jax.nn.silu(gated) * lifted).astype(jnp.bfloat16)
            return jnp.dot(hidden, expert_down[0], preferred_element_type=jnp.float32).astype(
                jnp.bfloat16
            )
        gated = jnp.einsum("secd,edf->secf", rows, expert_gate, preferred_element_type=jnp.float32)
        lifted = jnp.einsum("secd,edf->secf", rows, expert_up, preferred_element_type=jnp.float32)
        hidden = (jax.nn.silu(gated) * lifted).astype(jnp.bfloat16)
        return jnp.einsum(
            "secf,efd->secd", hidden, expert_down, preferred_element_type=jnp.float32
        ).astype(jnp.bfloat16)

    shared_places = gather_near(normed_experts, "tp", tp_size)
    routed_places = gather_near(received, "tp", tp_size, head_rows)
    shared_result = scatter_near([shared_expert(rows) for rows in shared_places], "tp", tp_size)
    routed_result = scatter_near(
        [routed_expert(rows) for rows in routed_places], "tp", tp_size
    ).astype(jnp.bfloat16)
    returned = lax.all_to_all(
        routed_result.reshape(ep_size, pair_rows, model_width),
        "ep",
        split_axis=0,
        concat_axis=0,
        tiled=True,
    )
    returned = returned.reshape(slot_count, model_width)
    spread = jnp.sum(
        jnp.where(
            jnp.arange(slot_count, dtype=jnp.int32)[None, None, :] == slot_ids[:, :, None],
            route_weight[:, :, None],
            0.0,
        ),
        axis=1,
    )
    upper = lax.reduce_precision(spread, 8, 7)
    lower = lax.reduce_precision(spread - upper, 8, 7)
    routed_total = jnp.dot(
        upper.astype(jnp.bfloat16), returned, preferred_element_type=jnp.float32
    ) + jnp.dot(lower.astype(jnp.bfloat16), returned, preferred_element_type=jnp.float32)
    expert_output = (routed_total + shared_result).astype(jnp.bfloat16)
    return (mixer_sum, expert_output)


def chunk_order(half):
    order = [("n", 0)] + [("n", 2)] * (half > 2) + [("n", 1)]
    order += [("n", d) for d in range(3, half)]
    return order + [("f", d) for d in range(half)]


def padded(rows):
    return -(-rows // 16) * 16


class Sizes:
    def __init__(self, ep, tp, rows, width, tokens, hidden, shared, capacity, value_dim):
        self.ep, self.tp, self.rows, self.width = ep, tp, rows, width
        self.tokens, self.hidden, self.shared = tokens, hidden, shared
        self.cap, self.stride = capacity, padded(capacity)
        self.value_dim = value_dim
        self.half = ep // 2
        self.own = rows // tp
        self.tile = min(512, width)

    def names(self):
        half, ep = self.half, self.ep
        crossing = [("n", d) for d in range(2, half)] + [("f", d) for d in range(half)]
        groups = (
            [("XY", 0), ("INFO", 0), ("XC", 0), ("XC", 1)]
            + [("FAR", d) for d in range(half)]
            + [("NEAR", d, 0) for d in range(1, half)]
            + [("NEAR", 1, 1)]
            + [("FY",) + name for name in crossing]
            + [("RET", d) for d in range(half)]
            + [("NRET", d, c) for d in range(1, half) for c in range(2)]
            + [("SC", 0), ("SC", 1), ("AY", 0), ("AY", 1), ("KVF", 0), ("OC", 0), ("OY", 0)]
            + [("KVN", d) for d in range(1, half)]
            + [("KVC", d) for d in range(1, half)]
        )
        table = {name: number for number, name in enumerate(groups)}
        first = len(groups)
        table["RC"], table["PC"], table["QY"] = first, first + ep, first + 2 * ep
        return table, first + 3 * ep

    def scratch(self):
        bf, f32 = jnp.bfloat16, jnp.float32
        ep, half, width, stride = self.ep, self.half, self.width, self.stride
        tokens, rows, hidden, shared = self.tokens, self.rows, self.hidden, self.shared
        vd = self.value_dim
        return dict(
            mx=((rows, width), bf),
            wq=((width, 4 * HEAD), bf),
            wk=((2 * HEAD, width), bf),
            x=((tokens, width), bf),
            info=((8, tokens), f32),
            ids=((2, tokens), jnp.int32),
            gates=((2, tokens), f32),
            wv=((width, vd), bf),
            wo=((2 * vd, width), bf),
            wg=((width, hidden), bf),
            wu=((width, hidden), bf),
            wd=((hidden, width), bf),
            sg=((width, shared), bf),
            su=((width, shared), bf),
            sd=((shared, width), bf),
            xb=((2, 2, tokens, width), bf),
            other=((8, tokens), f32),
            outf=((half, stride, width), bf),
            outn=((half, 2, stride, width), bf),
            r=((ep, 2, 2, stride, width), bf),
            p=((ep, 2, 2, stride, width), bf),
            pr=((ep, 2, stride, width), bf),
            q=((ep, 2, stride, width), bf),
            qr=((ep, stride, width), bf),
            fb=((ep, stride, width), bf),
            tn=((2, half, stride, width), bf),
            tf=((half, stride, width), bf),
            s=((2, 2, tokens, width), bf),
            sr=((2, tokens, width), bf),
            ao=((tokens, width), bf),
            ar=((tokens, width), bf),
            acc=((tokens, width), f32),
            wown=((2, tokens, half * stride), bf),
            wfar=((2, tokens, half * stride), bf),
            woth=((2, tokens, half * stride), bf),
            nm=((rows, width), bf),
            qs=((2, 2, rows, 2 * HEAD), bf),
            kv=((ep, rows, 2 * HEAD + vd), bf),
            sc=((2, ep, rows, rows), f32),
            stat=((2, rows, 128), f32),
            tot=((2, rows, 128), f32),
            pv=((2, rows, vd), f32),
            hr=((rows, 2 * vd), bf),
            o=((2, 2, self.own, width), bf),
            orx=((2, self.own, width), bf),
            oq=((2, self.own, width), bf),
            oy=((self.own, width), bf),
        )

    def vmem_bytes(self):
        total = 0
        for shape, dtype in self.scratch().values():
            size = jnp.dtype(dtype).itemsize
            for extent in shape[:-1]:
                size *= extent
            total += size * (-(-shape[-1] // 128) * 128)
        return total


def step_plan(half):
    order = chunk_order(half)
    place = {name: number for number, name in enumerate(order)}
    plan = {number: [] for number in range(2 * half + 1)}
    early = half // 2
    plan[place[("n", 1)]] += [("core_sum", "n", 0), ("arrive_near",)]
    for d in range(2, half):
        plan[place[("n", d)]] += [("crossed", "n", d)]
    for d in range(early):
        plan[place[("f", d)] - 1] += [("crossed", "f", d)]
    for d in range(1, half):
        plan[place[("n", d)] + 2] += [("core_sum", "n", d)]
    for d in range(early):
        plan[place[("f", d)] + 2] += [("core_sum", "f", d)]
    for d in range(early, half):
        plan[place[("f", d)] - 1] += [("arrive_cross", "f", d)]
    first = plan[place[("f", early)]]
    first += [("kv_arrivals",), ("head", 0), ("crossed", "f", early)]
    for d in range(early + 1, half):
        now = plan[place[("f", d)]]
        now += [("side_sum", d - early - 1)]
        if d == early + 1:
            now += [("head", 1), ("project_out",)]
        now += [("crossed", "f", d)]
    last = plan[2 * half]
    last += [("core_sum", "f", d) for d in range(early, half - 1)]
    last += [("side_sum", d) for d in range(half - early - 1, early)]
    last += [("core_sum", "f", half - 1), ("mix_sum",)]
    last += [("side_sum", d) for d in range(early, half)]
    last += [("other_rows", 0), ("other_rows", 1), ("own_rows",)]
    return plan


class Later:
    def __init__(self, start):
        self.start = start


def fused_kernel(sizes, keys, *refs):
    lam, xgain, mgain, hgain = refs[:4]
    (h_x, h_ids, h_gates, h_mx, h_q1, h_q2, h_k1, h_k2, h_v) = refs[4:13]
    (h_wo, h_g, h_u, h_d, h_sg, h_su, h_sd) = refs[13:20]
    mix_out, exp_out = refs[20:22]
    b = dict(zip(keys, refs[22 : 22 + len(keys)]))
    send_sem, recv_sem, load_sem = refs[22 + len(keys) :]
    x, info = b["x"], b["info"]
    half, ep, width, stride, cap = sizes.half, sizes.ep, sizes.width, sizes.stride, sizes.cap
    tokens, rows, tile, vd = sizes.tokens, sizes.rows, sizes.tile, sizes.value_dim
    f32, bf = jnp.float32, jnp.bfloat16
    table, _ = sizes.names()
    order = chunk_order(half)
    place = {name: number for number, name in enumerate(order)}

    me = lax.axis_index("ep")
    tp = lax.axis_index("tp")
    side = me // half
    spot = me % half
    row_of = tp // 2
    core = tp % 2
    tiles = width // tile

    lines = half // 2
    line, lane_x = spot // 2, spot % 2

    def shifted(which, d, turn):
        moved = (line + lines + turn * (d // 2)) % lines
        return which * half + moved * 2 + (lane_x + d % 2) % 2

    near_to = [shifted(side, d, 1) for d in range(half)]
    near_by = [shifted(side, d, -1) for d in range(half)]
    far_to = [shifted(1 - side, d, 1) for d in range(half)]
    far_by = [shifted(1 - side, d, -1) for d in range(half)]
    early = half // 2

    def near(d):
        return (near_to[d], tp)

    def near_from(d):
        return (near_by[d], tp)

    def far(d):
        return (far_to[d], tp)

    def far_from(d):
        return (far_by[d], tp)

    partner_y = (me, (1 - row_of) * 2 + core)
    partner_c = (me, row_of * 2 + 1 - core)

    def remote(number, source, target, device):
        return pltpu.make_async_remote_copy(
            src_ref=source,
            dst_ref=target,
            send_sem=send_sem.at[number],
            recv_sem=recv_sem.at[number],
            device_id=device,
            device_id_type=pl.DeviceIdType.MESH,
        )

    copies = {}

    def made(name):
        source, target, device = copies[name]
        return remote(table[name], source(), target(), device)

    def copy(name, source, target, device):
        copies[name] = (source, target, device)
        return Later(lambda: made(name).start())

    def dot(left, right):
        return jnp.dot(left, right, preferred_element_type=f32)

    crossing = [("n", d) for d in range(2, half)] + [("f", d) for d in range(half)]
    for kind, d in crossing:
        position = place[(kind, d)]
        copies[("FY", kind, d)] = (
            lambda position=position: b["r"].at[position, 0, 0, pl.ds(0, cap)],
            lambda position=position: b["r"].at[position, 0, 1, pl.ds(0, cap)],
            partner_y,
        )
    for d in range(half):
        copies[("RET", d)] = (
            lambda d=d: b["fb"].at[place[("f", d)], pl.ds(0, cap)],
            lambda d=d: b["tf"].at[d, pl.ds(0, cap)],
            far_from(d),
        )
    for d in range(1, half):
        for c in range(2):
            cols = pl.ds(c * width // 2, width // 2)
            copies[("NRET", d, c)] = (
                lambda d=d, cols=cols: b["q"].at[place[("n", d)], :, pl.ds(0, cap), cols],
                lambda d=d, cols=cols: b["tn"].at[:, d, pl.ds(0, cap), cols],
                near_from(d),
            )

    loads = {}
    pairs = dict(
        x=(h_x, b["x"]),
        ids=(h_ids, b["ids"]),
        gates=(h_gates, b["gates"]),
        mx=(h_mx, b["mx"]),
        q1=(h_q1, b["wq"].at[:, : 2 * HEAD]),
        q2=(h_q2, b["wq"].at[:, 2 * HEAD :]),
        k1=(h_k1, b["wk"].at[:HEAD]),
        k2=(h_k2, b["wk"].at[HEAD:]),
        v=(h_v, b["wv"]),
        sg=(h_sg, b["sg"]),
        su=(h_su, b["su"]),
        sd=(h_sd, b["sd"]),
        wg=(h_g.at[0], b["wg"]),
        wu=(h_u.at[0], b["wu"]),
        wd=(h_d.at[0], b["wd"]),
        wo=(h_wo, b["wo"]),
    )
    for number, (name, (source, target)) in enumerate(pairs.items()):
        loads[name] = pltpu.make_async_copy(source, target, load_sem.at[number])
        loads[name].start()

    barrier = pltpu.get_barrier_semaphore()
    peers = [near(d) for d in range(1, half)] + [far(d) for d in range(half)]
    peers += [partner_y, partner_c]
    for device in peers:
        pl.semaphore_signal(
            barrier, inc=1, device_id=device, device_id_type=pl.DeviceIdType.MESH
        )

    def norm_rows(source, target, count, gain):
        step = min(32, count)

        @pl.loop(0, count // step)
        def _(index):
            at = pl.ds(pl.multiple_of(index * step, step), step)
            values = source[at, :].astype(f32)
            factor = lax.rsqrt(jnp.mean(values * values, axis=-1, keepdims=True) + EPS)
            target[at, :] = (values * factor * gain[...]).astype(bf)

    loads["x"].wait()
    norm_rows(x, b["xb"].at[0, 0], tokens, xgain)
    loads["ids"].wait()
    loads["gates"].wait()
    info[...] = jnp.zeros((8, tokens), f32)
    info[0:2, :] = b["ids"][...].astype(f32)
    info[2:4, :] = b["gates"][...]

    earlier = (
        lax.broadcasted_iota(jnp.int32, (tokens, tokens), 0)
        < lax.broadcasted_iota(jnp.int32, (tokens, tokens), 1)
    ).astype(bf)
    padded_ep = -(-ep // 8) * 8
    relative = lax.broadcasted_iota(jnp.int32, (padded_ep, tokens), 0)
    expert = jnp.zeros((padded_ep, tokens), f32) - 1.0
    for k, target in enumerate(near_to + far_to):
        expert = jnp.where(relative == k, target.astype(f32), expert)

    def routing(info_ref):
        first = info_ref[0:1, :] == expert
        second = info_ref[1:2, :] == expert
        named = jnp.where(first | second, 1.0, 0.0)
        position = dot(named.astype(bf), earlier)
        position = jnp.where(named > 0.0, position, -1.0)
        weight = jnp.where(first, info_ref[2:3, :], 0.0) + jnp.where(second, info_ref[3:4, :], 0.0)
        return position, weight

    slot = lax.broadcasted_iota(jnp.int32, (stride, tokens), 0).astype(f32)

    def chosen(position, which):
        return slot == position[which : which + 1, :]

    def select(position, which):
        return jnp.concatenate(
            [jnp.where(chosen(position, k), 1.0, 0.0) for k in which], axis=0
        ).astype(bf)

    def spread(position, weight, which):
        stacked = jnp.concatenate(
            [jnp.where(chosen(position, k), weight[k : k + 1, :], 0.0) for k in which], axis=0
        )
        turned = stacked.T
        upper = turned.astype(bf)
        return upper, (turned - upper.astype(f32)).astype(bf)

    own_place, own_weight = routing(info)
    near_set = list(range(half))
    far_set = list(range(half, 2 * half))
    direct_set = [0, 1]
    select_near = select(own_place, near_set)
    select_far = select(own_place, far_set)

    pl.semaphore_wait(barrier, len(peers))
    copy(("XY", 0), lambda: b["xb"].at[0, 0], lambda: b["xb"].at[1, 0], partner_y).start()
    copy(("INFO", 0), lambda: info, lambda: b["other"], partner_y).start()
    copy(("XC", 0), lambda: b["xb"].at[0, 0], lambda: b["xb"].at[0, 1], partner_c).start()

    def pick(select_rows, source, store):
        for n in range(tiles):
            cols = slice(n * tile, (n + 1) * tile)
            picked = dot(select_rows, source[:, cols]).astype(bf)
            for d in range(select_rows.shape[0] // stride):
                store(d, cols, picked[d * stride : (d + 1) * stride, :])

    def store_near(a):
        def store(d, cols, value):
            b["outn"][d, a, :, cols] = value

        return store

    def store_far(d, cols, value):
        b["outf"][d, :, cols] = value

    pick(select_near, b["xb"].at[0, 0], store_near(0))

    def core_forward(position):
        return remote(
            table["RC"] + position, b["r"].at[position, 0], b["r"].at[position, 1], partner_c
        )

    def arrive_cross(kind, d):
        made(("FAR", d) if kind == "f" else ("NEAR", d, 0)).wait_recv()
        made(("FY", kind, d)).start()

    def crossed(kind, d):
        made(("FY", kind, d)).wait_recv()
        core_forward(place[(kind, d)]).start()

    def arrive_near():
        for a in range(2):
            made(("NEAR", 1, a)).wait_recv()
        core_forward(place[("n", 1)]).start()

    def relay_kv():
        @pl.when(side == 1)
        def _():
            slot_of = b["kv"].at[far_by[0]]
            remote(table[("KVF", 0)], slot_of, slot_of, far(0)).wait_recv()

        for d in range(1, half):
            copy(("KVC", d), lambda: b["kv"].at[far_by[0]], lambda: b["kv"].at[far_by[0]], near(d))

            @pl.when(side == 1)
            def _(d=d):
                made(("KVC", d)).start()

    def other_spread():
        upper, lower = spread(other_place, other_weight, near_set)
        b["woth"][0] = upper
        b["woth"][1] = lower

    def start_near(a):
        for d in (range(1, half) if a == 0 else (1,)):
            copy(
                ("NEAR", d, a),
                lambda d=d: b["outn"].at[d, a, pl.ds(0, cap)],
                lambda d=d: b["r"].at[place[("n", d)], 0, a, pl.ds(0, cap)],
                near(d),
            ).start()

    start_near(0)
    pick(select_far, b["xb"].at[0, 0], store_far)

    def start_far(d):
        copy(
            ("FAR", d),
            lambda: b["outf"].at[d, pl.ds(0, cap)],
            lambda: b["r"].at[place[("f", d)], 0, 0, pl.ds(0, cap)],
            far(d),
        ).start()

    start_far(0)

    loads["mx"].wait()
    norm_rows(b["mx"], b["nm"], rows, mgain)
    for name in ("q1", "q2", "k1", "k2", "v"):
        loads[name].wait()
    lane = lax.broadcasted_iota(jnp.int32, (rows, 2 * HEAD), 1)
    b["kv"][me, :, : 2 * HEAD] = lax.dot_general(
        b["nm"][...], b["wk"][...], (((1,), (1,)), ((), ())), preferred_element_type=f32
    ).astype(bf)
    b["kv"][me, :, 2 * HEAD :] = dot(b["nm"][...], b["wv"][...]).astype(bf)

    copy(("KVF", 0), lambda: b["kv"].at[me], lambda: b["kv"].at[me], far(0))

    @pl.when(side == 0)
    def _():
        made(("KVF", 0)).start()

    for d in range(1, half):
        copy(("KVN", d), lambda: b["kv"].at[me], lambda: b["kv"].at[me], near(d))

        @pl.when(near_to[d] > me)
        def _(d=d):
            made(("KVN", d)).start()

    for d in range(1, early):
        start_far(d)

    for m in range(2):
        queries = dot(b["nm"][...], b["wq"][:, m * 2 * HEAD : (m + 1) * 2 * HEAD])
        turned = pltpu.roll(queries, HEAD, 1)
        keep = (lane < HEAD) if m == 0 else (lane >= HEAD)
        for g in range(2):
            source = queries if g == m else turned
            b["qs"][m, g] = jnp.where(keep, source, 0.0).astype(bf)

    def shared_expert(a):
        both = b["xb"][a].reshape(2 * tokens, width)
        gated = dot(both, b["sg"][...])
        lifted = dot(both, b["su"][...])
        hidden = (jax.nn.silu(gated) * lifted).astype(bf)
        for n in range(tiles):
            cols = slice(n * tile, (n + 1) * tile)
            part = dot(hidden, b["sd"][:, cols]).astype(bf)
            b["s"][a, 0, :, cols] = part[:tokens]
            b["s"][a, 1, :, cols] = part[tokens:]

    for name in ("sg", "su", "sd"):
        loads[name].wait()
    made(("XC", 0)).wait_recv()
    shared_expert(0)
    copy(("SC", 0), lambda: b["s"].at[0, 1], lambda: b["sr"].at[0], partner_c).start()

    for name, group in (("wown", near_set), ("wfar", far_set)):
        upper, lower = spread(own_place, own_weight, group)
        b[name][0] = upper
        b[name][1] = lower
    for d in range(half):
        b["tf"][d, cap:, :] = jnp.zeros((stride - cap, width), bf)
        for a in range(2):
            b["tn"][a, d, cap:, :] = jnp.zeros((stride - cap, width), bf)
    made(("XY", 0)).wait_recv()
    made(("INFO", 0)).wait_recv()
    copy(("XC", 1), lambda: b["xb"].at[1, 0], lambda: b["xb"].at[1, 1], partner_c).start()
    for d in range(2, half):
        arrive_cross("n", d)
    other_place, other_weight = routing(b["other"])
    pick(select(other_place, direct_set), b["xb"].at[1, 0], store_near(1))
    relay_kv()
    start_near(1)
    for d in range(early, half):
        start_far(d)
    b["r"][0, 0] = b["outn"][0]

    core_forward(0).start()
    arrive_cross("f", 0)
    made(("XC", 1)).wait_recv()
    shared_expert(1)
    copy(("SC", 1), lambda: b["s"].at[1, 1], lambda: b["sr"].at[1], partner_c).start()
    other_spread()
    for d in range(1, early):
        arrive_cross("f", d)

    for name in ("wg", "wu", "wd"):
        loads[name].wait()

    far_places = [place[("f", d)] for d in range(half)]
    row_count = 4 * stride

    def back_copy(number):
        return remote(
            table["PC"] + number, b["p"].at[number, 1], b["pr"].at[number], partner_c
        )

    def cross_copy(number):
        return remote(
            table["QY"] + number,
            b["q"].at[number, 1, pl.ds(0, cap)],
            b["qr"].at[number, pl.ds(0, cap)],
            partner_y,
        )

    def core_sum(kind, d):
        position = place[(kind, d)]
        back_copy(position).wait_recv()
        for a in range(2):
            b["q"][position, a] = (
                b["p"][position, 0, a].astype(f32) + b["pr"][position, a].astype(f32)
            ).astype(bf)
        if kind == "f":
            cross_copy(position).start()
        elif d > 0:
            for c in range(2):
                made(("NRET", d, c)).start()
        else:
            for a in range(2):
                b["tn"][a, 0, 0:cap, :] = b["q"][position, a, 0:cap, :]

    def side_sum(d):
        position = place[("f", d)]
        cross_copy(position).wait_recv()
        b["fb"][position] = (
            b["q"][position, 0].astype(f32) + b["qr"][position].astype(f32)
        ).astype(bf)
        made(("RET", d)).start()

    def kv_arrival(name, source, d):
        block = b["kv"].at[source]
        remote(table[(name, d)], block, block, near(d)).wait_recv()

    def kv_arrivals():
        for d in range(1, half):

            @pl.when(near_by[d] < me)
            def _(d=d):
                kv_arrival("KVN", near_by[d], d)

            @pl.when(side == 1)
            def _(d=d):
                kv_arrival("KVC", far_by[d], d)

    scale = HEAD**-0.5 * math.log2(math.e)
    row_place = me * rows + lax.broadcasted_iota(jnp.int32, (rows, rows), 0)
    col_place = lax.broadcasted_iota(jnp.int32, (rows, rows), 1)
    halves = [slice(c * 128, (c + 1) * 128) for c in range(rows // 128)]

    def head(g):
        b["stat"][...] = jnp.full((2, rows, 128), NEG, f32)
        b["tot"][...] = jnp.zeros((2, rows, 128), f32)
        b["pv"][...] = jnp.zeros((2, rows, vd), f32)

        def score(j, carry):
            keys_j = b["kv"][j, :, 0 : 2 * HEAD]
            for m in range(2):
                scores = lax.dot_general(
                    b["qs"][m, g], keys_j, (((1,), (1,)), ((), ())), preferred_element_type=f32
                )
                scores = jnp.where(j * rows + col_place <= row_place, scores, NEG)
                b["sc"][m, j] = scores
                most = b["stat"][m]
                for cols in halves:
                    most = jnp.maximum(most, scores[:, cols])
                b["stat"][m] = most
            return carry

        lax.fori_loop(0, me + 1, score, 0)
        for m in range(2):
            most = jnp.max(b["stat"][m], axis=1, keepdims=True)
            b["stat"][m] = jnp.broadcast_to(most, (rows, 128))

        def weigh(j, carry):
            values = b["kv"][j, :, 2 * HEAD :]
            for m in range(2):
                most = b["stat"][m]
                total = b["tot"][m]
                parts = []
                for cols in halves:
                    weights = jnp.exp2((b["sc"][m, j, :, cols] - most) * scale)
                    total = total + weights
                    parts.append(weights.astype(bf))
                b["tot"][m] = total
                b["pv"][m] += dot(jnp.concatenate(parts, axis=1), values)
            return carry

        lax.fori_loop(0, me + 1, weigh, 0)
        sums = [jnp.sum(b["tot"][m], axis=1, keepdims=True) for m in range(2)]
        combined = b["pv"][0] / sums[0] - lam[g] * (b["pv"][1] / sums[1])
        factor = lax.rsqrt(jnp.mean(combined * combined, axis=1, keepdims=True) + EPS)
        b["hr"][:, g * vd : (g + 1) * vd] = (combined * factor * hgain[...]).astype(bf)

    def project_out():
        loads["wo"].wait()
        own = sizes.own
        for n in range(tiles):
            cols = slice(n * tile, (n + 1) * tile)
            part = dot(b["hr"][...], b["wo"][:, cols]).astype(bf)
            b["o"][:, :, :, cols] = part.reshape(2, 2, own, tile)
        made(("OC", 0)).start()

    def other_rows(c):
        for d in range(1, half):
            made(("NRET", d, c)).wait_recv()
        if c == 0:
            for a in range(2):
                made(("SC", a)).wait_recv()
        for n in range(c * tiles // 2, (c + 1) * tiles // 2):
            cols = slice(n * tile, (n + 1) * tile)
            back = b["tn"][1, :, :, cols].reshape(half * stride, tile)
            total = dot(b["woth"][0], back) + dot(b["woth"][1], back)
            total = total + b["s"][1, 0, :, cols].astype(f32) + b["sr"][1, :, cols].astype(f32)
            b["ao"][:, cols] = total.astype(bf)
        made(("AY", c)).start()

    def mix_sum():
        made(("OC", 0)).wait_recv()
        for a in range(2):
            b["oq"][a] = (b["o"][a, core].astype(f32) + b["orx"][a].astype(f32)).astype(bf)
        made(("OY", 0)).start()

    def own_rows():
        for n in range(tiles):
            cols = slice(n * tile, (n + 1) * tile)
            back = b["tn"][0, :, :, cols].reshape(half * stride, tile)
            total = dot(b["wown"][0], back) + dot(b["wown"][1], back)
            b["acc"][:, cols] = (
                total + b["s"][0, 0, :, cols].astype(f32) + b["sr"][0, :, cols].astype(f32)
            )

    copies[("OC", 0)] = (lambda: b["o"].at[:, 1 - core], lambda: b["orx"], partner_c)
    for c in range(2):
        cols = pl.ds(c * width // 2, width // 2)
        copies[("AY", c)] = (
            lambda cols=cols: b["ao"].at[:, cols],
            lambda cols=cols: b["ar"].at[:, cols],
            partner_y,
        )
    copies[("OY", 0)] = (lambda: b["oq"].at[1 - row_of], lambda: b["oy"], partner_y)
    schedule = step_plan(half)
    actions = dict(
        arrive_cross=arrive_cross,
        crossed=crossed,
        arrive_near=arrive_near,
        core_sum=core_sum,
        side_sum=side_sum,
        kv_arrivals=kv_arrivals,
        head=head,
        project_out=project_out,
        mix_sum=mix_sum,
        other_rows=other_rows,
        own_rows=own_rows,
    )

    def step_body(step, carry):
        for when in sorted(schedule):

            @pl.when(step == when)
            def _(when=when):
                for name, *values in schedule[when]:
                    actions[name](*values)

        @pl.when(step < ep)
        def _():
            core_forward(step).wait_recv()
            arrived = b["r"][step].reshape(row_count, width)
            gated = dot(arrived, b["wg"][...])
            lifted = dot(arrived, b["wu"][...])
            hidden = (jax.nn.silu(gated) * lifted).astype(bf)
            for n in range(tiles):
                cols = slice(n * tile, (n + 1) * tile)
                part = dot(hidden, b["wd"][:, cols]).astype(bf)
                b["p"][step, :, :, :, cols] = part.reshape(2, 2, stride, tile)
            back_copy(step).start()

        return carry

    lax.fori_loop(0, max(schedule) + 1, step_body, 0)

    made(("OY", 0)).wait_recv()
    mix_out[...] = (b["oq"][row_of].astype(f32) + b["oy"][...].astype(f32)).astype(bf)

    for d in range(half):
        made(("RET", d)).wait_recv()
    for c in range(2):
        made(("AY", c)).wait_recv()
    for n in range(tiles):
        cols = slice(n * tile, (n + 1) * tile)
        back = b["tf"][:, :, cols].reshape(half * stride, tile)
        total = dot(b["wfar"][0], back) + dot(b["wfar"][1], back)
        total = total + b["acc"][:, cols] + b["ar"][:, cols].astype(f32)
        exp_out[:, cols] = total.astype(bf)

    conditional = {("KVF", 0): side == 0}
    for d in range(1, half):
        conditional[("KVN", d)] = near_to[d] > me
        conditional[("KVC", d)] = side == 1
    for name in copies:
        if name in conditional:

            @pl.when(conditional[name])
            def _(name=name):
                made(name).wait_send()

        else:
            made(name).wait_send()
    for position in range(ep):
        core_forward(position).wait_send()
        back_copy(position).wait_send()
        if position in far_places:
            cross_copy(position).wait_send()


def fused(sizes, args):
    scratch = sizes.scratch()
    keys = list(scratch)
    _, count = sizes.names()
    vmem = pl.BlockSpec(memory_space=pltpu.VMEM)
    smem = pl.BlockSpec(memory_space=pltpu.SMEM)
    hbm = pl.BlockSpec(memory_space=pltpu.HBM)
    return pl.pallas_call(
        functools.partial(fused_kernel, sizes, keys),
        out_shape=(
            jax.ShapeDtypeStruct((sizes.own, sizes.width), jnp.bfloat16),
            jax.ShapeDtypeStruct((sizes.tokens, sizes.width), jnp.bfloat16),
        ),
        in_specs=[smem] + [vmem] * 3 + [hbm] * 16,
        out_specs=(vmem, vmem),
        scratch_shapes=[pltpu.VMEM(shape, dtype) for shape, dtype in scratch.values()]
        + [
            pltpu.SemaphoreType.DMA((count,)),
            pltpu.SemaphoreType.DMA((count,)),
            pltpu.SemaphoreType.DMA((16,)),
        ],
        compiler_params=pltpu.CompilerParams(
            collective_id=0, has_side_effects=True, vmem_limit_bytes=VMEM_LIMIT
        ),
        name="layer",
    )(*args)


VMEM_LIMIT = 67043328


def fused_body(sizes, *arrays):
    (
        mixer_input,
        mixer_gain,
        query_one,
        query_two,
        key_one,
        key_two,
        value_weight,
        lambdas,
        head_gain,
        output_weight,
        expert_input,
        expert_gain,
        routes,
        route_weight,
        expert_gate,
        expert_up,
        expert_down,
        shared_gate,
        shared_up,
        shared_down,
    ) = arrays
    return fused(
        sizes,
        (
            lambdas,
            expert_gain.reshape(1, -1),
            mixer_gain.reshape(1, -1),
            head_gain.reshape(1, -1),
            expert_input,
            routes.T,
            route_weight.T,
            mixer_input,
            query_one,
            query_two,
            key_one.T,
            key_two.T,
            value_weight,
            output_weight,
            expert_gate,
            expert_up,
            expert_down,
            shared_gate,
            shared_up,
            shared_down,
        ),
    )


def body(*arrays):
    ep_size, tp_size = lax.axis_size("ep"), lax.axis_size("tp")
    mixer_input, query_one, key_one = arrays[0], arrays[2], arrays[4]
    head_gain, expert_input, routes = arrays[8], arrays[10], arrays[12]
    expert_gate, shared_gate = arrays[14], arrays[17]
    rows, width = mixer_input.shape
    tokens, top_count = routes.shape
    local_experts = expert_gate.shape[0]
    capacity = max(2, 5 * tokens * top_count // (4 * local_experts * ep_size))
    fits = (
        tp_size == 4
        and ep_size % 2 == 0
        and ep_size >= 4
        and local_experts == 1
        and top_count == 2
        and key_one.shape[1] == HEAD
        and query_one.shape[1] == 2 * HEAD
        and head_gain.shape[0] == 128
        and tokens == 128
        and rows % (16 * tp_size) == 0
        and rows % 128 == 0
        and width % 512 == 0
        and expert_input.shape[1] == width
        and capacity % 8 == 0
    )
    if fits:
        sizes = Sizes(
            ep_size,
            tp_size,
            rows,
            width,
            tokens,
            expert_gate.shape[2],
            shared_gate.shape[1],
            capacity,
            head_gain.shape[0],
        )
        if sizes.vmem_bytes() + 8 * 2**20 <= VMEM_LIMIT:
            return fused_body(sizes, *arrays)
    return general_body(*arrays)


def solution(mesh):
    in_specs = (
        P("ep", None),
        P(),
        P(None, "tp"),
        P(None, "tp"),
        P(None, "tp"),
        P(None, "tp"),
        P(None, "tp"),
        P("tp"),
        P(),
        P("tp", None),
        P(("ep", "tp"), None),
        P(),
        P(("ep", "tp"), None),
        P(("ep", "tp"), None),
        P("ep", None, "tp"),
        P("ep", None, "tp"),
        P("ep", "tp", None),
        P(None, "tp"),
        P(None, "tp"),
        P("tp", None),
    )
    out_specs = (P(("ep", "tp"), None), P(("ep", "tp"), None))
    return jax.shard_map(body, mesh=mesh, in_specs=in_specs, out_specs=out_specs, check_vma=False)
```

```python
import functools
import math

import jax
import jax.numpy as jnp
from jax import lax
from jax.experimental import pallas as pl
from jax.experimental.pallas import tpu as pltpu
from jax.sharding import PartitionSpec as P

HEAD = 64


EPS = 1e-06
NEG = -1e30


def normalize(activations, scaling):
    values = activations.astype(jnp.float32)
    factor = lax.rsqrt(jnp.mean(values * values, axis=-1, keepdims=True) + EPS)
    return (values * factor * scaling).astype(jnp.bfloat16)


def attention_kernel(
    shape, rank_ref, lambdas_ref, queries_ref, keys_ref, gain_ref, out_ref, maxima, totals, weighted
):
    rows, chunk, local_kv, group, value_dim = shape
    rank = rank_ref[0]
    maxima[...] = jnp.full(maxima.shape, NEG, jnp.float32)
    totals[...] = jnp.zeros(totals.shape, jnp.float32)
    weighted[...] = jnp.zeros(weighted.shape, jnp.float32)
    heads = local_kv * group
    key_cols = local_kv * HEAD
    chunks = rows // chunk
    scale = HEAD**-0.5 * math.log2(math.e)

    def block(index, masked):
        start = pl.multiple_of(index * rows, rows)
        for kv in range(local_kv):
            value_start = 2 * key_cols + kv * value_dim
            for part in range(chunks):
                span = (part + 1) * chunk if masked else rows
                values = keys_ref[pl.ds(start, span), value_start : value_start + value_dim]
                for which in range(2):
                    first = which * key_cols + kv * HEAD
                    keys = keys_ref[pl.ds(start, span), first : first + HEAD]
                    for g in range(group):
                        head = kv * group + g
                        col = (which * heads + head) * HEAD
                        queries = queries_ref[part * chunk : (part + 1) * chunk, col : col + HEAD]
                        scores = lax.dot_general(
                            queries,
                            keys,
                            (((1,), (1,)), ((), ())),
                            preferred_element_type=jnp.float32,
                        )
                        if masked:
                            row = part * chunk + lax.broadcasted_iota(jnp.int32, scores.shape, 0)
                            col_pos = lax.broadcasted_iota(jnp.int32, scores.shape, 1)
                            scores = jnp.where(col_pos <= row, scores, NEG)
                        slot = (which * heads + head) * chunks + part
                        earlier = maxima[slot]
                        latest = jnp.maximum(earlier, jnp.max(scores, axis=1, keepdims=True))
                        shrink = jnp.exp2((earlier - latest) * scale)
                        weights = jnp.exp2((scores - latest[:, :1]) * scale)
                        totals[slot] = totals[slot] * shrink + jnp.sum(
                            weights, axis=1, keepdims=True
                        )
                        weighted[slot] = weighted[slot] * shrink[:, :1] + jnp.dot(
                            weights.astype(jnp.bfloat16),
                            values,
                            preferred_element_type=jnp.float32,
                        )
                        maxima[slot] = latest

    def earlier_block(index, carry):
        block(index, False)
        return carry

    lax.fori_loop(0, rank, earlier_block, 0)
    block(rank, True)
    for head in range(heads):
        for part in range(chunks):
            one = head * chunks + part
            two = (heads + head) * chunks + part
            combined = (
                weighted[one] / totals[one][:, :1]
                - lambdas_ref[head] * (weighted[two] / totals[two][:, :1])
            )
            factor = lax.rsqrt(jnp.mean(combined * combined, axis=1, keepdims=True) + EPS)
            out_ref[
                part * chunk : (part + 1) * chunk, head * value_dim : (head + 1) * value_dim
            ] = (combined * factor * gain_ref[...]).astype(jnp.bfloat16)


def attention(queries, keys, rank, lambdas, head_gain, local_kv, group):
    rows = queries.shape[0]
    value_dim = head_gain.shape[0]
    heads = local_kv * group
    chunk = min(128, rows)
    slots = 2 * heads * (rows // chunk)
    vmem = pl.BlockSpec(memory_space=pltpu.VMEM)
    smem = pl.BlockSpec(memory_space=pltpu.SMEM)
    scores = heads * 2 * rows * keys.shape[0]
    return pl.pallas_call(
        functools.partial(attention_kernel, (rows, chunk, local_kv, group, value_dim)),
        out_shape=jax.ShapeDtypeStruct((rows, heads * value_dim), jnp.bfloat16),
        in_specs=[smem, smem, vmem, vmem, vmem],
        out_specs=vmem,
        scratch_shapes=[
            pltpu.VMEM((slots, chunk, 128), jnp.float32),
            pltpu.VMEM((slots, chunk, 128), jnp.float32),
            pltpu.VMEM((slots, chunk, value_dim), jnp.float32),
        ],
        compiler_params=pltpu.CompilerParams(vmem_limit_bytes=48 * 1024 * 1024),
        cost_estimate=pl.CostEstimate(
            flops=8 * scores * HEAD, bytes_accessed=keys.size * 2, transcendentals=scores
        ),
        name="attention",
    )(rank.reshape(1), lambdas, queries, keys, head_gain.reshape(1, value_dim))


def swap(rows, axis, size, distance):
    return lax.ppermute(rows, axis, [(i, i ^ distance) for i in range(size)])


def gather_near(block, axis, size, ahead=None):
    places = {0: block}
    distance = size // 2
    while distance:
        for place in sorted(places):
            moved = swap(places[place], axis, size, distance)
            if ahead is not None:
                moved, ahead = lax.optimization_barrier((moved, ahead))
            places[place ^ distance] = moved
        ahead = None
        distance //= 2
    return [places[place] for place in range(size)]


def scatter_near(partials, axis, size):
    sums = dict(enumerate(partials))
    distance = 1
    while distance < size:
        kept = [place for place in sorted(sums) if not place & distance]
        moved = {
            place: swap(sums[place ^ distance].astype(jnp.bfloat16), axis, size, distance)
            for place in kept
        }
        sums = {
            place: sums[place].astype(jnp.float32) + moved[place].astype(jnp.float32)
            for place in kept
        }
        distance *= 2
    return sums[0]


def general_body(
    mixer_input,
    mixer_gain,
    query_one,
    query_two,
    key_one,
    key_two,
    value_weight,
    lambdas,
    head_gain,
    output_weight,
    expert_input,
    expert_gain,
    routes,
    route_weight,
    expert_gate,
    expert_up,
    expert_down,
    shared_gate,
    shared_up,
    shared_down,
):
    ep_size = lax.axis_size("ep")
    tp_size = lax.axis_size("tp")
    ep_rank = lax.axis_index("ep")
    mixer_rows = mixer_input.shape[0]
    model_width = mixer_input.shape[1]
    query_cols = query_one.shape[1]
    key_cols = key_one.shape[1]
    value_dim = head_gain.shape[0]
    local_kv = key_cols // HEAD
    local_heads = query_cols // HEAD
    group_size = local_heads // local_kv
    normed = normalize(mixer_input, mixer_gain)

    def project(weights):
        return jnp.concatenate(
            [
                jnp.dot(normed, weight, preferred_element_type=jnp.float32).astype(jnp.bfloat16)
                for weight in weights
            ],
            axis=1,
        )

    key_values = project([key_one, key_two, value_weight])
    query_part = project([query_one, query_two])
    arrived = lax.all_gather(key_values, "ep", axis=0, tiled=True)
    head_rows = attention(
        query_part, arrived, ep_rank, lambdas, head_gain, local_kv, group_size
    )
    tp_rank = lax.axis_index("tp")
    own_rows = mixer_rows // tp_size

    def mixer_place(place):
        rows = lax.dynamic_slice_in_dim(head_rows, (tp_rank ^ place) * own_rows, own_rows, 0)
        return jnp.dot(rows, output_weight, preferred_element_type=jnp.float32).astype(
            jnp.bfloat16
        )

    mixer_sum = scatter_near(
        [mixer_place(place) for place in range(tp_size)], "tp", tp_size
    ).astype(jnp.bfloat16)

    token_rows = expert_input.shape[0]
    normed_experts = normalize(expert_input, expert_gain)
    experts_local = expert_gate.shape[0]
    expert_count = experts_local * ep_size
    top_count = routes.shape[1]
    capacity = max(2, 5 * token_rows * top_count // (4 * expert_count))
    slot_count = expert_count * capacity
    flat_routes = routes.reshape(-1)
    onehot = (flat_routes[:, None] == jnp.arange(expert_count, dtype=jnp.int32)[None, :]).astype(
        jnp.int32
    )
    slot_place = jnp.sum((jnp.cumsum(onehot, axis=0) - onehot) * onehot, axis=1)
    slot_ids = (flat_routes * capacity + slot_place).reshape(token_rows, top_count)
    slot_match = jnp.arange(slot_count, dtype=jnp.int32)[:, None, None] == slot_ids[None, :, :]
    select = jnp.any(slot_match, axis=2).astype(jnp.bfloat16)
    outgoing = jnp.dot(select, normed_experts, preferred_element_type=jnp.float32).astype(
        jnp.bfloat16
    )
    pair_rows = experts_local * capacity
    outgoing = outgoing.reshape(ep_size, pair_rows, model_width)
    outgoing, key_values = lax.optimization_barrier((outgoing, key_values))
    received = lax.all_to_all(outgoing, "ep", split_axis=0, concat_axis=0, tiled=True)
    received = received.reshape(ep_size, experts_local, capacity, model_width)
    if experts_local == 1:
        received = received.reshape(ep_size * capacity, model_width)

    def shared_expert(rows):
        gated = jnp.dot(rows, shared_gate, preferred_element_type=jnp.float32)
        lifted = jnp.dot(rows, shared_up, preferred_element_type=jnp.float32)
        hidden = (jax.nn.silu(gated) * lifted).astype(jnp.bfloat16)
        return jnp.dot(hidden, shared_down, preferred_element_type=jnp.float32).astype(
            jnp.bfloat16
        )

    def routed_expert(rows):
        if experts_local == 1:
            gated = jnp.dot(rows, expert_gate[0], preferred_element_type=jnp.float32)
            lifted = jnp.dot(rows, expert_up[0], preferred_element_type=jnp.float32)
            hidden = (jax.nn.silu(gated) * lifted).astype(jnp.bfloat16)
            return jnp.dot(hidden, expert_down[0], preferred_element_type=jnp.float32).astype(
                jnp.bfloat16
            )
        gated = jnp.einsum("secd,edf->secf", rows, expert_gate, preferred_element_type=jnp.float32)
        lifted = jnp.einsum("secd,edf->secf", rows, expert_up, preferred_element_type=jnp.float32)
        hidden = (jax.nn.silu(gated) * lifted).astype(jnp.bfloat16)
        return jnp.einsum(
            "secf,efd->secd", hidden, expert_down, preferred_element_type=jnp.float32
        ).astype(jnp.bfloat16)

    shared_places = gather_near(normed_experts, "tp", tp_size)
    routed_places = gather_near(received, "tp", tp_size, head_rows)
    shared_result = scatter_near([shared_expert(rows) for rows in shared_places], "tp", tp_size)
    routed_result = scatter_near(
        [routed_expert(rows) for rows in routed_places], "tp", tp_size
    ).astype(jnp.bfloat16)
    returned = lax.all_to_all(
        routed_result.reshape(ep_size, pair_rows, model_width),
        "ep",
        split_axis=0,
        concat_axis=0,
        tiled=True,
    )
    returned = returned.reshape(slot_count, model_width)
    spread = jnp.sum(
        jnp.where(
            jnp.arange(slot_count, dtype=jnp.int32)[None, None, :] == slot_ids[:, :, None],
            route_weight[:, :, None],
            0.0,
        ),
        axis=1,
    )
    upper = lax.reduce_precision(spread, 8, 7)
    lower = lax.reduce_precision(spread - upper, 8, 7)
    routed_total = jnp.dot(
        upper.astype(jnp.bfloat16), returned, preferred_element_type=jnp.float32
    ) + jnp.dot(lower.astype(jnp.bfloat16), returned, preferred_element_type=jnp.float32)
    expert_output = (routed_total + shared_result).astype(jnp.bfloat16)
    return (mixer_sum, expert_output)


def chunk_order(half):
    early = half // 2
    order = [("n", 0)] + [("f", d) for d in range(early)]
    order += [("n", d) for d in range(1, half)]
    return order + [("f", d) for d in range(early, half)]


def padded(rows):
    return -(-rows // 16) * 16


class Sizes:
    def __init__(self, ep, tp, rows, width, tokens, hidden, shared, capacity, value_dim):
        self.ep, self.tp, self.rows, self.width = ep, tp, rows, width
        self.tokens, self.hidden, self.shared = tokens, hidden, shared
        self.cap, self.stride = capacity, padded(capacity)
        self.value_dim = value_dim
        self.half = ep // 2
        self.own = rows // tp
        self.tile = min(512, width)

    def names(self):
        half, ep = self.half, self.ep
        crossing = [("n", d) for d in range(2, half)] + [("f", d) for d in range(half)]
        groups = (
            [("XY", 0), ("INFO", 0), ("XC", 0), ("XC", 1)]
            + [("FAR", d) for d in range(half)]
            + [("NEAR", d, 0) for d in range(1, half)]
            + [("NEAR", 1, 1)]
            + [("FY",) + name for name in crossing]
            + [("RET", d) for d in range(half)]
            + [("NRET", d, c) for d in range(1, half) for c in range(2)]
            + [("SC", 0), ("SC", 1), ("AY", 0), ("AY", 1), ("KVF", 0), ("OC", 0), ("OY", 0)]
            + [("KVN", d) for d in range(1, half)]
            + [("KVC", d) for d in range(1, half)]
        )
        table = {name: number for number, name in enumerate(groups)}
        first = len(groups)
        table["RC"], table["PC"], table["QY"] = first, first + ep, first + 2 * ep
        return table, first + 3 * ep

    def scratch(self):
        bf, f32 = jnp.bfloat16, jnp.float32
        ep, half, width, stride = self.ep, self.half, self.width, self.stride
        tokens, rows, hidden, shared = self.tokens, self.rows, self.hidden, self.shared
        vd = self.value_dim
        return dict(
            mx=((rows, width), bf),
            wq=((width, 4 * HEAD), bf),
            wk=((2 * HEAD, width), bf),
            x=((tokens, width), bf),
            info=((8, tokens), f32),
            ids=((2, tokens), jnp.int32),
            gates=((2, tokens), f32),
            wv=((width, vd), bf),
            wo=((2 * vd, width), bf),
            wg=((width, hidden), bf),
            wu=((width, hidden), bf),
            wd=((hidden, width), bf),
            sg=((width, shared), bf),
            su=((width, shared), bf),
            sd=((shared, width), bf),
            xb=((2, 2, tokens, width), bf),
            other=((8, tokens), f32),
            outf=((half, stride, width), bf),
            outn=((half, 2, stride, width), bf),
            r=((ep, 2, 2, stride, width), bf),
            p=((ep, 2, 2, stride, width), bf),
            pr=((ep, 2, stride, width), bf),
            q=((ep, 2, stride, width), bf),
            qr=((ep, stride, width), bf),
            fb=((ep, stride, width), bf),
            tn=((2, half, stride, width), bf),
            tf=((half, stride, width), bf),
            s=((2, 2, tokens, width), bf),
            sr=((2, tokens, width), bf),
            ao=((tokens, width), bf),
            ar=((tokens, width), bf),
            acc=((tokens, width), f32),
            wown=((2, tokens, half * stride), bf),
            wfar=((half, 2, tokens, stride), bf),
            woth=((2, tokens, half * stride), bf),
            nm=((rows, width), bf),
            qs=((2, 2, rows, 2 * HEAD), bf),
            kv=((ep, rows, 2 * HEAD + vd), bf),
            sc=((2, ep, rows, rows), f32),
            stat=((2, rows, 128), f32),
            tot=((2, rows, 128), f32),
            pv=((2, rows, vd), f32),
            hr=((rows, 2 * vd), bf),
            o=((2, 2, self.own, width), bf),
            orx=((2, self.own, width), bf),
            oq=((2, self.own, width), bf),
            oy=((self.own, width), bf),
        )

    def vmem_bytes(self):
        total = 0
        for shape, dtype in self.scratch().values():
            size = jnp.dtype(dtype).itemsize
            for extent in shape[:-1]:
                size *= extent
            total += size * (-(-shape[-1] // 128) * 128)
        return total


def step_plan(half):
    order = chunk_order(half)
    place = {name: number for number, name in enumerate(order)}
    plan = {number: [] for number in range(2 * half + 1)}
    early = half // 2
    for d in range(early):
        plan[place[("f", d)]] += [("crossed", "f", d)]
    plan[early] += [("core_sum", "n", 0), ("relay_kv",)]
    first = place[("n", 1)]
    plan[first] += [("crossed", "n", 2)] * (half > 2) + [("arrive_near",)]
    for d in range(3, half):
        plan[place[("n", d)] - 1] += [("crossed", "n", d)]
    for d in range(early):
        plan[first + d] += [("core_sum", "f", d)]
    for d in range(1, half):
        plan[place[("n", d)] + 2] += [("core_sum", "n", d)]
    for d in range(early, half):
        plan[place[("f", d)] - 1] += [("arrive_cross", "f", d)]
    for d in range(early):
        plan[first + d + 2] += [("side_sum", d)]
    for d in range(early, half):
        at = plan[place[("f", d)]]
        if d == half - 1:
            at += [("kv_arrivals",), ("head", 0)]
        if d > early:
            at += [("core_sum", "f", d - 1)]
        at += [("crossed", "f", d)]
    last = plan[2 * half]
    last += [("core_sum", "f", half - 1), ("side_sum", early), ("head", 1), ("project_out",)]
    last += [("side_sum", d) for d in range(early + 1, half)] + [("mix_sum",)]
    last += [("other_rows", 0), ("other_rows", 1), ("own_rows",)]
    return plan


class Later:
    def __init__(self, start):
        self.start = start


def fused_kernel(sizes, keys, *refs):
    lam, xgain, mgain, hgain = refs[:4]
    (h_x, h_ids, h_gates, h_mx, h_q1, h_q2, h_k1, h_k2, h_v) = refs[4:13]
    (h_wo, h_g, h_u, h_d, h_sg, h_su, h_sd) = refs[13:20]
    mix_out, exp_out = refs[20:22]
    b = dict(zip(keys, refs[22 : 22 + len(keys)]))
    send_sem, recv_sem, load_sem = refs[22 + len(keys) :]
    x, info = b["x"], b["info"]
    half, ep, width, stride, cap = sizes.half, sizes.ep, sizes.width, sizes.stride, sizes.cap
    tokens, rows, tile, vd = sizes.tokens, sizes.rows, sizes.tile, sizes.value_dim
    f32, bf = jnp.float32, jnp.bfloat16
    table, _ = sizes.names()
    order = chunk_order(half)
    place = {name: number for number, name in enumerate(order)}

    me = lax.axis_index("ep")
    tp = lax.axis_index("tp")
    side = me // half
    spot = me % half
    row_of = tp // 2
    core = tp % 2
    tiles = width // tile

    lines = half // 2
    line, lane_x = spot // 2, spot % 2

    def shifted(which, d, turn):
        moved = (line + lines + turn * (d // 2)) % lines
        return which * half + moved * 2 + (lane_x + d % 2) % 2

    near_to = [shifted(side, d, 1) for d in range(half)]
    near_by = [shifted(side, d, -1) for d in range(half)]
    far_to = [shifted(1 - side, d, 1) for d in range(half)]
    far_by = [shifted(1 - side, d, -1) for d in range(half)]
    early = half // 2

    def near(d):
        return (near_to[d], tp)

    def near_from(d):
        return (near_by[d], tp)

    def far(d):
        return (far_to[d], tp)

    def far_from(d):
        return (far_by[d], tp)

    partner_y = (me, (1 - row_of) * 2 + core)
    partner_c = (me, row_of * 2 + 1 - core)

    def remote(number, source, target, device):
        return pltpu.make_async_remote_copy(
            src_ref=source,
            dst_ref=target,
            send_sem=send_sem.at[number],
            recv_sem=recv_sem.at[number],
            device_id=device,
            device_id_type=pl.DeviceIdType.MESH,
        )

    copies = {}

    def made(name):
        source, target, device = copies[name]
        return remote(table[name], source(), target(), device)

    def copy(name, source, target, device):
        copies[name] = (source, target, device)
        return Later(lambda: made(name).start())

    def dot(left, right):
        return jnp.dot(left, right, preferred_element_type=f32)

    crossing = [("n", d) for d in range(2, half)] + [("f", d) for d in range(half)]
    for kind, d in crossing:
        position = place[(kind, d)]
        copies[("FY", kind, d)] = (
            lambda position=position: b["r"].at[position, 0, 0, pl.ds(0, cap)],
            lambda position=position: b["r"].at[position, 0, 1, pl.ds(0, cap)],
            partner_y,
        )
    for d in range(half):
        copies[("RET", d)] = (
            lambda d=d: b["fb"].at[place[("f", d)], pl.ds(0, cap)],
            lambda d=d: b["tf"].at[d, pl.ds(0, cap)],
            far_from(d),
        )
    for d in range(1, half):
        for c in range(2):
            cols = pl.ds(c * width // 2, width // 2)
            copies[("NRET", d, c)] = (
                lambda d=d, cols=cols: b["q"].at[place[("n", d)], :, pl.ds(0, cap), cols],
                lambda d=d, cols=cols: b["tn"].at[:, d, pl.ds(0, cap), cols],
                near_from(d),
            )

    loads = {}
    pairs = dict(
        x=(h_x, b["x"]),
        ids=(h_ids, b["ids"]),
        gates=(h_gates, b["gates"]),
        mx=(h_mx, b["mx"]),
        q1=(h_q1, b["wq"].at[:, : 2 * HEAD]),
        q2=(h_q2, b["wq"].at[:, 2 * HEAD :]),
        k1=(h_k1, b["wk"].at[:HEAD]),
        k2=(h_k2, b["wk"].at[HEAD:]),
        v=(h_v, b["wv"]),
        sg=(h_sg, b["sg"]),
        su=(h_su, b["su"]),
        sd=(h_sd, b["sd"]),
        wg=(h_g.at[0], b["wg"]),
        wu=(h_u.at[0], b["wu"]),
        wd=(h_d.at[0], b["wd"]),
        wo=(h_wo, b["wo"]),
    )
    for number, (name, (source, target)) in enumerate(pairs.items()):
        loads[name] = pltpu.make_async_copy(source, target, load_sem.at[number])
        loads[name].start()

    barrier = pltpu.get_barrier_semaphore()
    peers = [near(d) for d in range(1, half)] + [far(d) for d in range(half)]
    peers += [partner_y, partner_c]
    for device in peers:
        pl.semaphore_signal(
            barrier, inc=1, device_id=device, device_id_type=pl.DeviceIdType.MESH
        )

    def norm_rows(source, target, count, gain):
        step = min(32, count)

        @pl.loop(0, count // step)
        def _(index):
            at = pl.ds(pl.multiple_of(index * step, step), step)
            values = source[at, :].astype(f32)
            factor = lax.rsqrt(jnp.mean(values * values, axis=-1, keepdims=True) + EPS)
            target[at, :] = (values * factor * gain[...]).astype(bf)

    loads["x"].wait()
    norm_rows(x, b["xb"].at[0, 0], tokens, xgain)
    loads["ids"].wait()
    loads["gates"].wait()
    info[...] = jnp.zeros((8, tokens), f32)
    info[0:2, :] = b["ids"][...].astype(f32)
    info[2:4, :] = b["gates"][...]

    earlier = (
        lax.broadcasted_iota(jnp.int32, (tokens, tokens), 0)
        < lax.broadcasted_iota(jnp.int32, (tokens, tokens), 1)
    ).astype(bf)
    padded_ep = -(-ep // 8) * 8
    relative = lax.broadcasted_iota(jnp.int32, (padded_ep, tokens), 0)
    expert = jnp.zeros((padded_ep, tokens), f32) - 1.0
    for k, target in enumerate(near_to + far_to):
        expert = jnp.where(relative == k, target.astype(f32), expert)

    def routing(info_ref):
        first = info_ref[0:1, :] == expert
        second = info_ref[1:2, :] == expert
        named = jnp.where(first | second, 1.0, 0.0)
        position = dot(named.astype(bf), earlier)
        position = jnp.where(named > 0.0, position, -1.0)
        weight = jnp.where(first, info_ref[2:3, :], 0.0) + jnp.where(second, info_ref[3:4, :], 0.0)
        return position, weight

    slot = lax.broadcasted_iota(jnp.int32, (stride, tokens), 0).astype(f32)

    def chosen(position, which):
        return slot == position[which : which + 1, :]

    def select(position, which):
        return jnp.concatenate(
            [jnp.where(chosen(position, k), 1.0, 0.0) for k in which], axis=0
        ).astype(bf)

    def spread(position, weight, which):
        stacked = jnp.concatenate(
            [jnp.where(chosen(position, k), weight[k : k + 1, :], 0.0) for k in which], axis=0
        )
        turned = stacked.T
        upper = turned.astype(bf)
        return upper, (turned - upper.astype(f32)).astype(bf)

    own_place, own_weight = routing(info)
    near_set = list(range(half))
    far_set = list(range(half, 2 * half))
    direct_set = [0, 1]
    select_near = select(own_place, near_set)
    select_far = select(own_place, far_set)

    pl.semaphore_wait(barrier, len(peers))
    copy(("XY", 0), lambda: b["xb"].at[0, 0], lambda: b["xb"].at[1, 0], partner_y).start()
    copy(("INFO", 0), lambda: info, lambda: b["other"], partner_y).start()
    copy(("XC", 0), lambda: b["xb"].at[0, 0], lambda: b["xb"].at[0, 1], partner_c).start()

    def pick(select_rows, source, store):
        for n in range(tiles):
            cols = slice(n * tile, (n + 1) * tile)
            picked = dot(select_rows, source[:, cols]).astype(bf)
            for d in range(select_rows.shape[0] // stride):
                store(d, cols, picked[d * stride : (d + 1) * stride, :])

    def store_near(a):
        def store(d, cols, value):
            b["outn"][d, a, :, cols] = value

        return store

    def store_far(d, cols, value):
        b["outf"][d, :, cols] = value

    pick(select_near, b["xb"].at[0, 0], store_near(0))

    def core_forward(position):
        return remote(
            table["RC"] + position, b["r"].at[position, 0], b["r"].at[position, 1], partner_c
        )

    def arrive_cross(kind, d):
        made(("FAR", d) if kind == "f" else ("NEAR", d, 0)).wait_recv()
        made(("FY", kind, d)).start()

    def crossed(kind, d):
        made(("FY", kind, d)).wait_recv()
        core_forward(place[(kind, d)]).start()

    def arrive_near():
        for a in range(2):
            made(("NEAR", 1, a)).wait_recv()
        core_forward(place[("n", 1)]).start()

    def relay_kv():
        @pl.when(side == 1)
        def _():
            slot_of = b["kv"].at[far_by[0]]
            remote(table[("KVF", 0)], slot_of, slot_of, far(0)).wait_recv()

        for d in range(1, half):
            copy(("KVC", d), lambda: b["kv"].at[far_by[0]], lambda: b["kv"].at[far_by[0]], near(d))

            @pl.when(side == 1)
            def _(d=d):
                made(("KVC", d)).start()

    def other_spread():
        upper, lower = spread(other_place, other_weight, near_set)
        b["woth"][0] = upper
        b["woth"][1] = lower

    def start_near(a):
        for d in (range(1, half) if a == 0 else (1,)):
            copy(
                ("NEAR", d, a),
                lambda d=d: b["outn"].at[d, a, pl.ds(0, cap)],
                lambda d=d: b["r"].at[place[("n", d)], 0, a, pl.ds(0, cap)],
                near(d),
            ).start()

    start_near(0)
    pick(select_far, b["xb"].at[0, 0], store_far)

    def start_far(d):
        copy(
            ("FAR", d),
            lambda: b["outf"].at[d, pl.ds(0, cap)],
            lambda: b["r"].at[place[("f", d)], 0, 0, pl.ds(0, cap)],
            far(d),
        ).start()

    for d in range(early):
        start_far(d)

    loads["mx"].wait()
    norm_rows(b["mx"], b["nm"], rows, mgain)
    for name in ("q1", "q2", "k1", "k2", "v"):
        loads[name].wait()
    lane = lax.broadcasted_iota(jnp.int32, (rows, 2 * HEAD), 1)
    b["kv"][me, :, : 2 * HEAD] = lax.dot_general(
        b["nm"][...], b["wk"][...], (((1,), (1,)), ((), ())), preferred_element_type=f32
    ).astype(bf)
    b["kv"][me, :, 2 * HEAD :] = dot(b["nm"][...], b["wv"][...]).astype(bf)

    copy(("KVF", 0), lambda: b["kv"].at[me], lambda: b["kv"].at[me], far(0))

    @pl.when(side == 0)
    def _():
        made(("KVF", 0)).start()

    for d in range(1, half):
        copy(("KVN", d), lambda: b["kv"].at[me], lambda: b["kv"].at[me], near(d))

        @pl.when(near_to[d] > me)
        def _(d=d):
            made(("KVN", d)).start()

    for m in range(2):
        queries = dot(b["nm"][...], b["wq"][:, m * 2 * HEAD : (m + 1) * 2 * HEAD])
        turned = pltpu.roll(queries, HEAD, 1)
        keep = (lane < HEAD) if m == 0 else (lane >= HEAD)
        for g in range(2):
            source = queries if g == m else turned
            b["qs"][m, g] = jnp.where(keep, source, 0.0).astype(bf)

    def shared_expert(a):
        both = b["xb"][a].reshape(2 * tokens, width)
        gated = dot(both, b["sg"][...])
        lifted = dot(both, b["su"][...])
        hidden = (jax.nn.silu(gated) * lifted).astype(bf)
        for n in range(tiles):
            cols = slice(n * tile, (n + 1) * tile)
            part = dot(hidden, b["sd"][:, cols]).astype(bf)
            b["s"][a, 0, :, cols] = part[:tokens]
            b["s"][a, 1, :, cols] = part[tokens:]

    for name in ("sg", "su", "sd"):
        loads[name].wait()
    made(("XC", 0)).wait_recv()
    shared_expert(0)
    copy(("SC", 0), lambda: b["s"].at[0, 1], lambda: b["sr"].at[0], partner_c).start()

    upper, lower = spread(own_place, own_weight, near_set)
    b["wown"][0] = upper
    b["wown"][1] = lower
    for d in range(half):
        upper, lower = spread(own_place, own_weight, [half + d])
        b["wfar"][d, 0] = upper
        b["wfar"][d, 1] = lower
    for d in range(half):
        b["tf"][d, cap:, :] = jnp.zeros((stride - cap, width), bf)
        for a in range(2):
            b["tn"][a, d, cap:, :] = jnp.zeros((stride - cap, width), bf)
    made(("XY", 0)).wait_recv()
    made(("INFO", 0)).wait_recv()
    copy(("XC", 1), lambda: b["xb"].at[1, 0], lambda: b["xb"].at[1, 1], partner_c).start()
    arrive_cross("f", 0)
    other_place, other_weight = routing(b["other"])
    pick(select(other_place, direct_set), b["xb"].at[1, 0], store_near(1))
    start_near(1)
    for d in range(early, half):
        start_far(d)
    b["r"][0, 0] = b["outn"][0]

    core_forward(0).start()
    made(("XC", 1)).wait_recv()
    shared_expert(1)
    copy(("SC", 1), lambda: b["s"].at[1, 1], lambda: b["sr"].at[1], partner_c).start()
    other_spread()
    for d in range(1, early):
        arrive_cross("f", d)
    for d in range(2, half):
        arrive_cross("n", d)

    for name in ("wg", "wu", "wd"):
        loads[name].wait()

    far_places = [place[("f", d)] for d in range(half)]
    row_count = 4 * stride

    def back_copy(number):
        return remote(
            table["PC"] + number, b["p"].at[number, 1], b["pr"].at[number], partner_c
        )

    def cross_copy(number):
        return remote(
            table["QY"] + number,
            b["q"].at[number, 1, pl.ds(0, cap)],
            b["qr"].at[number, pl.ds(0, cap)],
            partner_y,
        )

    def core_sum(kind, d):
        position = place[(kind, d)]
        back_copy(position).wait_recv()
        for a in range(2):
            b["q"][position, a] = (
                b["p"][position, 0, a].astype(f32) + b["pr"][position, a].astype(f32)
            ).astype(bf)
        if kind == "f":
            cross_copy(position).start()
        elif d > 0:
            for c in range(2):
                made(("NRET", d, c)).start()
        else:
            for a in range(2):
                b["tn"][a, 0, 0:cap, :] = b["q"][position, a, 0:cap, :]

    def side_sum(d):
        position = place[("f", d)]
        cross_copy(position).wait_recv()
        b["fb"][position] = (
            b["q"][position, 0].astype(f32) + b["qr"][position].astype(f32)
        ).astype(bf)
        made(("RET", d)).start()

    def kv_arrival(name, source, d):
        block = b["kv"].at[source]
        remote(table[(name, d)], block, block, near(d)).wait_recv()

    def kv_arrivals():
        for d in range(1, half):

            @pl.when(near_by[d] < me)
            def _(d=d):
                kv_arrival("KVN", near_by[d], d)

            @pl.when(side == 1)
            def _(d=d):
                kv_arrival("KVC", far_by[d], d)

    scale = HEAD**-0.5 * math.log2(math.e)
    row_place = me * rows + lax.broadcasted_iota(jnp.int32, (rows, rows), 0)
    col_place = lax.broadcasted_iota(jnp.int32, (rows, rows), 1)
    halves = [slice(c * 128, (c + 1) * 128) for c in range(rows // 128)]

    def head(g):
        b["stat"][...] = jnp.full((2, rows, 128), NEG, f32)
        b["tot"][...] = jnp.zeros((2, rows, 128), f32)
        b["pv"][...] = jnp.zeros((2, rows, vd), f32)

        def score(j, carry):
            keys_j = b["kv"][j, :, 0 : 2 * HEAD]
            for m in range(2):
                scores = lax.dot_general(
                    b["qs"][m, g], keys_j, (((1,), (1,)), ((), ())), preferred_element_type=f32
                )
                scores = jnp.where(j * rows + col_place <= row_place, scores, NEG)
                b["sc"][m, j] = scores
                most = b["stat"][m]
                for cols in halves:
                    most = jnp.maximum(most, scores[:, cols])
                b["stat"][m] = most
            return carry

        lax.fori_loop(0, me + 1, score, 0)
        for m in range(2):
            most = jnp.max(b["stat"][m], axis=1, keepdims=True)
            b["stat"][m] = jnp.broadcast_to(most, (rows, 128))

        def weigh(j, carry):
            values = b["kv"][j, :, 2 * HEAD :]
            for m in range(2):
                most = b["stat"][m]
                total = b["tot"][m]
                parts = []
                for cols in halves:
                    weights = jnp.exp2((b["sc"][m, j, :, cols] - most) * scale)
                    total = total + weights
                    parts.append(weights.astype(bf))
                b["tot"][m] = total
                b["pv"][m] += dot(jnp.concatenate(parts, axis=1), values)
            return carry

        lax.fori_loop(0, me + 1, weigh, 0)
        sums = [jnp.sum(b["tot"][m], axis=1, keepdims=True) for m in range(2)]
        combined = b["pv"][0] / sums[0] - lam[g] * (b["pv"][1] / sums[1])
        factor = lax.rsqrt(jnp.mean(combined * combined, axis=1, keepdims=True) + EPS)
        b["hr"][:, g * vd : (g + 1) * vd] = (combined * factor * hgain[...]).astype(bf)

    def project_out():
        loads["wo"].wait()
        own = sizes.own
        for n in range(tiles):
            cols = slice(n * tile, (n + 1) * tile)
            part = dot(b["hr"][...], b["wo"][:, cols]).astype(bf)
            b["o"][:, :, :, cols] = part.reshape(2, 2, own, tile)
        made(("OC", 0)).start()

    def other_rows(c):
        for d in range(1, half):
            made(("NRET", d, c)).wait_recv()
        if c == 0:
            for a in range(2):
                made(("SC", a)).wait_recv()
        for n in range(c * tiles // 2, (c + 1) * tiles // 2):
            cols = slice(n * tile, (n + 1) * tile)
            back = b["tn"][1, :, :, cols].reshape(half * stride, tile)
            total = dot(b["woth"][0], back) + dot(b["woth"][1], back)
            total = total + b["s"][1, 0, :, cols].astype(f32) + b["sr"][1, :, cols].astype(f32)
            b["ao"][:, cols] = total.astype(bf)
        made(("AY", c)).start()

    def mix_sum():
        made(("OC", 0)).wait_recv()
        for a in range(2):
            b["oq"][a] = (b["o"][a, core].astype(f32) + b["orx"][a].astype(f32)).astype(bf)
        made(("OY", 0)).start()

    def own_rows():
        for n in range(tiles):
            cols = slice(n * tile, (n + 1) * tile)
            back = b["tn"][0, :, :, cols].reshape(half * stride, tile)
            total = dot(b["wown"][0], back) + dot(b["wown"][1], back)
            b["acc"][:, cols] = (
                total + b["s"][0, 0, :, cols].astype(f32) + b["sr"][0, :, cols].astype(f32)
            )

    copies[("OC", 0)] = (lambda: b["o"].at[:, 1 - core], lambda: b["orx"], partner_c)
    for c in range(2):
        cols = pl.ds(c * width // 2, width // 2)
        copies[("AY", c)] = (
            lambda cols=cols: b["ao"].at[:, cols],
            lambda cols=cols: b["ar"].at[:, cols],
            partner_y,
        )
    copies[("OY", 0)] = (lambda: b["oq"].at[1 - row_of], lambda: b["oy"], partner_y)
    schedule = step_plan(half)
    actions = dict(
        arrive_cross=arrive_cross,
        crossed=crossed,
        arrive_near=arrive_near,
        core_sum=core_sum,
        side_sum=side_sum,
        kv_arrivals=kv_arrivals,
        head=head,
        relay_kv=relay_kv,
        project_out=project_out,
        mix_sum=mix_sum,
        other_rows=other_rows,
        own_rows=own_rows,
    )

    def step_body(step, carry):
        for when in sorted(schedule):

            @pl.when(step == when)
            def _(when=when):
                for name, *values in schedule[when]:
                    actions[name](*values)

        @pl.when(step < ep)
        def _():
            core_forward(step).wait_recv()
            arrived = b["r"][step].reshape(row_count, width)
            gated = dot(arrived, b["wg"][...])
            lifted = dot(arrived, b["wu"][...])
            hidden = (jax.nn.silu(gated) * lifted).astype(bf)
            for n in range(tiles):
                cols = slice(n * tile, (n + 1) * tile)
                part = dot(hidden, b["wd"][:, cols]).astype(bf)
                b["p"][step, :, :, :, cols] = part.reshape(2, 2, stride, tile)
            back_copy(step).start()

        return carry

    lax.fori_loop(0, max(schedule) + 1, step_body, 0)

    made(("OY", 0)).wait_recv()
    mix_out[...] = (b["oq"][row_of].astype(f32) + b["oy"][...].astype(f32)).astype(bf)

    for d in range(half):
        made(("RET", d)).wait_recv()
        for n in range(tiles):
            cols = slice(n * tile, (n + 1) * tile)
            back = b["tf"][d, :, cols]
            b["acc"][:, cols] += dot(b["wfar"][d, 0], back) + dot(b["wfar"][d, 1], back)
    for c in range(2):
        made(("AY", c)).wait_recv()
        cols = slice(c * width // 2, (c + 1) * width // 2)
        exp_out[:, cols] = (b["acc"][:, cols] + b["ar"][:, cols].astype(f32)).astype(bf)

    conditional = {("KVF", 0): side == 0}
    for d in range(1, half):
        conditional[("KVN", d)] = near_to[d] > me
        conditional[("KVC", d)] = side == 1
    for name in copies:
        if name in conditional:

            @pl.when(conditional[name])
            def _(name=name):
                made(name).wait_send()

        else:
            made(name).wait_send()
    for position in range(ep):
        core_forward(position).wait_send()
        back_copy(position).wait_send()
        if position in far_places:
            cross_copy(position).wait_send()


def fused(sizes, args):
    scratch = sizes.scratch()
    keys = list(scratch)
    _, count = sizes.names()
    vmem = pl.BlockSpec(memory_space=pltpu.VMEM)
    smem = pl.BlockSpec(memory_space=pltpu.SMEM)
    hbm = pl.BlockSpec(memory_space=pltpu.HBM)
    return pl.pallas_call(
        functools.partial(fused_kernel, sizes, keys),
        out_shape=(
            jax.ShapeDtypeStruct((sizes.own, sizes.width), jnp.bfloat16),
            jax.ShapeDtypeStruct((sizes.tokens, sizes.width), jnp.bfloat16),
        ),
        in_specs=[smem] + [vmem] * 3 + [hbm] * 16,
        out_specs=(vmem, vmem),
        scratch_shapes=[pltpu.VMEM(shape, dtype) for shape, dtype in scratch.values()]
        + [
            pltpu.SemaphoreType.DMA((count,)),
            pltpu.SemaphoreType.DMA((count,)),
            pltpu.SemaphoreType.DMA((16,)),
        ],
        compiler_params=pltpu.CompilerParams(
            collective_id=0, has_side_effects=True, vmem_limit_bytes=VMEM_LIMIT
        ),
        name="layer",
    )(*args)


VMEM_LIMIT = 67043328


def fused_body(sizes, *arrays):
    (
        mixer_input,
        mixer_gain,
        query_one,
        query_two,
        key_one,
        key_two,
        value_weight,
        lambdas,
        head_gain,
        output_weight,
        expert_input,
        expert_gain,
        routes,
        route_weight,
        expert_gate,
        expert_up,
        expert_down,
        shared_gate,
        shared_up,
        shared_down,
    ) = arrays
    return fused(
        sizes,
        (
            lambdas,
            expert_gain.reshape(1, -1),
            mixer_gain.reshape(1, -1),
            head_gain.reshape(1, -1),
            expert_input,
            routes.T,
            route_weight.T,
            mixer_input,
            query_one,
            query_two,
            key_one.T,
            key_two.T,
            value_weight,
            output_weight,
            expert_gate,
            expert_up,
            expert_down,
            shared_gate,
            shared_up,
            shared_down,
        ),
    )


def body(*arrays):
    ep_size, tp_size = lax.axis_size("ep"), lax.axis_size("tp")
    mixer_input, query_one, key_one = arrays[0], arrays[2], arrays[4]
    head_gain, expert_input, routes = arrays[8], arrays[10], arrays[12]
    expert_gate, shared_gate = arrays[14], arrays[17]
    rows, width = mixer_input.shape
    tokens, top_count = routes.shape
    local_experts = expert_gate.shape[0]
    capacity = max(2, 5 * tokens * top_count // (4 * local_experts * ep_size))
    fits = (
        tp_size == 4
        and ep_size % 2 == 0
        and ep_size >= 4
        and local_experts == 1
        and top_count == 2
        and key_one.shape[1] == HEAD
        and query_one.shape[1] == 2 * HEAD
        and head_gain.shape[0] == 128
        and tokens == 128
        and rows % (16 * tp_size) == 0
        and rows % 128 == 0
        and width % 512 == 0
        and expert_input.shape[1] == width
        and capacity % 8 == 0
    )
    if fits:
        sizes = Sizes(
            ep_size,
            tp_size,
            rows,
            width,
            tokens,
            expert_gate.shape[2],
            shared_gate.shape[1],
            capacity,
            head_gain.shape[0],
        )
        if sizes.vmem_bytes() + 8 * 2**20 <= VMEM_LIMIT:
            return fused_body(sizes, *arrays)
    return general_body(*arrays)


def solution(mesh):
    in_specs = (
        P("ep", None),
        P(),
        P(None, "tp"),
        P(None, "tp"),
        P(None, "tp"),
        P(None, "tp"),
        P(None, "tp"),
        P("tp"),
        P(),
        P("tp", None),
        P(("ep", "tp"), None),
        P(),
        P(("ep", "tp"), None),
        P(("ep", "tp"), None),
        P("ep", None, "tp"),
        P("ep", None, "tp"),
        P("ep", "tp", None),
        P(None, "tp"),
        P(None, "tp"),
        P("tp", None),
    )
    out_specs = (P(("ep", "tp"), None), P(("ep", "tp"), None))
    return jax.shard_map(body, mesh=mesh, in_specs=in_specs, out_specs=out_specs, check_vma=False)
```

```python
import functools
import math

import jax
import jax.numpy as jnp
from jax import lax
from jax.experimental import pallas as pl
from jax.experimental.pallas import tpu as pltpu
from jax.sharding import PartitionSpec as P

HEAD = 64


EPS = 1e-06
NEG = -1e30


def normalize(activations, scaling):
    values = activations.astype(jnp.float32)
    factor = lax.rsqrt(jnp.mean(values * values, axis=-1, keepdims=True) + EPS)
    return (values * factor * scaling).astype(jnp.bfloat16)


def attention_kernel(
    shape, rank_ref, lambdas_ref, queries_ref, keys_ref, gain_ref, out_ref, maxima, totals, weighted
):
    rows, chunk, local_kv, group, value_dim = shape
    rank = rank_ref[0]
    maxima[...] = jnp.full(maxima.shape, NEG, jnp.float32)
    totals[...] = jnp.zeros(totals.shape, jnp.float32)
    weighted[...] = jnp.zeros(weighted.shape, jnp.float32)
    heads = local_kv * group
    key_cols = local_kv * HEAD
    chunks = rows // chunk
    scale = HEAD**-0.5 * math.log2(math.e)

    def block(index, masked):
        start = pl.multiple_of(index * rows, rows)
        for kv in range(local_kv):
            value_start = 2 * key_cols + kv * value_dim
            for part in range(chunks):
                span = (part + 1) * chunk if masked else rows
                values = keys_ref[pl.ds(start, span), value_start : value_start + value_dim]
                for which in range(2):
                    first = which * key_cols + kv * HEAD
                    keys = keys_ref[pl.ds(start, span), first : first + HEAD]
                    for g in range(group):
                        head = kv * group + g
                        col = (which * heads + head) * HEAD
                        queries = queries_ref[part * chunk : (part + 1) * chunk, col : col + HEAD]
                        scores = lax.dot_general(
                            queries,
                            keys,
                            (((1,), (1,)), ((), ())),
                            preferred_element_type=jnp.float32,
                        )
                        if masked:
                            row = part * chunk + lax.broadcasted_iota(jnp.int32, scores.shape, 0)
                            col_pos = lax.broadcasted_iota(jnp.int32, scores.shape, 1)
                            scores = jnp.where(col_pos <= row, scores, NEG)
                        slot = (which * heads + head) * chunks + part
                        earlier = maxima[slot]
                        latest = jnp.maximum(earlier, jnp.max(scores, axis=1, keepdims=True))
                        shrink = jnp.exp2((earlier - latest) * scale)
                        weights = jnp.exp2((scores - latest[:, :1]) * scale)
                        totals[slot] = totals[slot] * shrink + jnp.sum(
                            weights, axis=1, keepdims=True
                        )
                        weighted[slot] = weighted[slot] * shrink[:, :1] + jnp.dot(
                            weights.astype(jnp.bfloat16),
                            values,
                            preferred_element_type=jnp.float32,
                        )
                        maxima[slot] = latest

    def earlier_block(index, carry):
        block(index, False)
        return carry

    lax.fori_loop(0, rank, earlier_block, 0)
    block(rank, True)
    for head in range(heads):
        for part in range(chunks):
            one = head * chunks + part
            two = (heads + head) * chunks + part
            combined = (
                weighted[one] / totals[one][:, :1]
                - lambdas_ref[head] * (weighted[two] / totals[two][:, :1])
            )
            factor = lax.rsqrt(jnp.mean(combined * combined, axis=1, keepdims=True) + EPS)
            out_ref[
                part * chunk : (part + 1) * chunk, head * value_dim : (head + 1) * value_dim
            ] = (combined * factor * gain_ref[...]).astype(jnp.bfloat16)


def attention(queries, keys, rank, lambdas, head_gain, local_kv, group):
    rows = queries.shape[0]
    value_dim = head_gain.shape[0]
    heads = local_kv * group
    chunk = min(128, rows)
    slots = 2 * heads * (rows // chunk)
    vmem = pl.BlockSpec(memory_space=pltpu.VMEM)
    smem = pl.BlockSpec(memory_space=pltpu.SMEM)
    scores = heads * 2 * rows * keys.shape[0]
    return pl.pallas_call(
        functools.partial(attention_kernel, (rows, chunk, local_kv, group, value_dim)),
        out_shape=jax.ShapeDtypeStruct((rows, heads * value_dim), jnp.bfloat16),
        in_specs=[smem, smem, vmem, vmem, vmem],
        out_specs=vmem,
        scratch_shapes=[
            pltpu.VMEM((slots, chunk, 128), jnp.float32),
            pltpu.VMEM((slots, chunk, 128), jnp.float32),
            pltpu.VMEM((slots, chunk, value_dim), jnp.float32),
        ],
        compiler_params=pltpu.CompilerParams(vmem_limit_bytes=48 * 1024 * 1024),
        cost_estimate=pl.CostEstimate(
            flops=8 * scores * HEAD, bytes_accessed=keys.size * 2, transcendentals=scores
        ),
        name="attention",
    )(rank.reshape(1), lambdas, queries, keys, head_gain.reshape(1, value_dim))


def swap(rows, axis, size, distance):
    return lax.ppermute(rows, axis, [(i, i ^ distance) for i in range(size)])


def gather_near(block, axis, size, ahead=None):
    places = {0: block}
    distance = size // 2
    while distance:
        for place in sorted(places):
            moved = swap(places[place], axis, size, distance)
            if ahead is not None:
                moved, ahead = lax.optimization_barrier((moved, ahead))
            places[place ^ distance] = moved
        ahead = None
        distance //= 2
    return [places[place] for place in range(size)]


def scatter_near(partials, axis, size):
    sums = dict(enumerate(partials))
    distance = 1
    while distance < size:
        kept = [place for place in sorted(sums) if not place & distance]
        moved = {
            place: swap(sums[place ^ distance].astype(jnp.bfloat16), axis, size, distance)
            for place in kept
        }
        sums = {
            place: sums[place].astype(jnp.float32) + moved[place].astype(jnp.float32)
            for place in kept
        }
        distance *= 2
    return sums[0]


def general_body(
    mixer_input,
    mixer_gain,
    query_one,
    query_two,
    key_one,
    key_two,
    value_weight,
    lambdas,
    head_gain,
    output_weight,
    expert_input,
    expert_gain,
    routes,
    route_weight,
    expert_gate,
    expert_up,
    expert_down,
    shared_gate,
    shared_up,
    shared_down,
):
    ep_size = lax.axis_size("ep")
    tp_size = lax.axis_size("tp")
    ep_rank = lax.axis_index("ep")
    mixer_rows = mixer_input.shape[0]
    model_width = mixer_input.shape[1]
    query_cols = query_one.shape[1]
    key_cols = key_one.shape[1]
    value_dim = head_gain.shape[0]
    local_kv = key_cols // HEAD
    local_heads = query_cols // HEAD
    group_size = local_heads // local_kv
    normed = normalize(mixer_input, mixer_gain)

    def project(weights):
        return jnp.concatenate(
            [
                jnp.dot(normed, weight, preferred_element_type=jnp.float32).astype(jnp.bfloat16)
                for weight in weights
            ],
            axis=1,
        )

    key_values = project([key_one, key_two, value_weight])
    query_part = project([query_one, query_two])
    arrived = lax.all_gather(key_values, "ep", axis=0, tiled=True)
    head_rows = attention(
        query_part, arrived, ep_rank, lambdas, head_gain, local_kv, group_size
    )
    tp_rank = lax.axis_index("tp")
    own_rows = mixer_rows // tp_size

    def mixer_place(place):
        rows = lax.dynamic_slice_in_dim(head_rows, (tp_rank ^ place) * own_rows, own_rows, 0)
        return jnp.dot(rows, output_weight, preferred_element_type=jnp.float32).astype(
            jnp.bfloat16
        )

    mixer_sum = scatter_near(
        [mixer_place(place) for place in range(tp_size)], "tp", tp_size
    ).astype(jnp.bfloat16)

    token_rows = expert_input.shape[0]
    normed_experts = normalize(expert_input, expert_gain)
    experts_local = expert_gate.shape[0]
    expert_count = experts_local * ep_size
    top_count = routes.shape[1]
    capacity = max(2, 5 * token_rows * top_count // (4 * expert_count))
    slot_count = expert_count * capacity
    flat_routes = routes.reshape(-1)
    onehot = (flat_routes[:, None] == jnp.arange(expert_count, dtype=jnp.int32)[None, :]).astype(
        jnp.int32
    )
    slot_place = jnp.sum((jnp.cumsum(onehot, axis=0) - onehot) * onehot, axis=1)
    slot_ids = (flat_routes * capacity + slot_place).reshape(token_rows, top_count)
    slot_match = jnp.arange(slot_count, dtype=jnp.int32)[:, None, None] == slot_ids[None, :, :]
    select = jnp.any(slot_match, axis=2).astype(jnp.bfloat16)
    outgoing = jnp.dot(select, normed_experts, preferred_element_type=jnp.float32).astype(
        jnp.bfloat16
    )
    pair_rows = experts_local * capacity
    outgoing = outgoing.reshape(ep_size, pair_rows, model_width)
    outgoing, key_values = lax.optimization_barrier((outgoing, key_values))
    received = lax.all_to_all(outgoing, "ep", split_axis=0, concat_axis=0, tiled=True)
    received = received.reshape(ep_size, experts_local, capacity, model_width)
    if experts_local == 1:
        received = received.reshape(ep_size * capacity, model_width)

    def shared_expert(rows):
        gated = jnp.dot(rows, shared_gate, preferred_element_type=jnp.float32)
        lifted = jnp.dot(rows, shared_up, preferred_element_type=jnp.float32)
        hidden = (jax.nn.silu(gated) * lifted).astype(jnp.bfloat16)
        return jnp.dot(hidden, shared_down, preferred_element_type=jnp.float32).astype(
            jnp.bfloat16
        )

    def routed_expert(rows):
        if experts_local == 1:
            gated = jnp.dot(rows, expert_gate[0], preferred_element_type=jnp.float32)
            lifted = jnp.dot(rows, expert_up[0], preferred_element_type=jnp.float32)
            hidden = (jax.nn.silu(gated) * lifted).astype(jnp.bfloat16)
            return jnp.dot(hidden, expert_down[0], preferred_element_type=jnp.float32).astype(
                jnp.bfloat16
            )
        gated = jnp.einsum("secd,edf->secf", rows, expert_gate, preferred_element_type=jnp.float32)
        lifted = jnp.einsum("secd,edf->secf", rows, expert_up, preferred_element_type=jnp.float32)
        hidden = (jax.nn.silu(gated) * lifted).astype(jnp.bfloat16)
        return jnp.einsum(
            "secf,efd->secd", hidden, expert_down, preferred_element_type=jnp.float32
        ).astype(jnp.bfloat16)

    shared_places = gather_near(normed_experts, "tp", tp_size)
    routed_places = gather_near(received, "tp", tp_size, head_rows)
    shared_result = scatter_near([shared_expert(rows) for rows in shared_places], "tp", tp_size)
    routed_result = scatter_near(
        [routed_expert(rows) for rows in routed_places], "tp", tp_size
    ).astype(jnp.bfloat16)
    returned = lax.all_to_all(
        routed_result.reshape(ep_size, pair_rows, model_width),
        "ep",
        split_axis=0,
        concat_axis=0,
        tiled=True,
    )
    returned = returned.reshape(slot_count, model_width)
    spread = jnp.sum(
        jnp.where(
            jnp.arange(slot_count, dtype=jnp.int32)[None, None, :] == slot_ids[:, :, None],
            route_weight[:, :, None],
            0.0,
        ),
        axis=1,
    )
    upper = lax.reduce_precision(spread, 8, 7)
    lower = lax.reduce_precision(spread - upper, 8, 7)
    routed_total = jnp.dot(
        upper.astype(jnp.bfloat16), returned, preferred_element_type=jnp.float32
    ) + jnp.dot(lower.astype(jnp.bfloat16), returned, preferred_element_type=jnp.float32)
    expert_output = (routed_total + shared_result).astype(jnp.bfloat16)
    return (mixer_sum, expert_output)


def chunk_order(half):
    early = half // 2
    order = [("n", 0)] + [("f", d) for d in range(early)]
    order += [("n", d) for d in range(1, half)]
    return order + [("f", d) for d in range(early, half)]


def padded(rows):
    return -(-rows // 16) * 16


class Sizes:
    def __init__(self, ep, tp, rows, width, tokens, hidden, shared, capacity, value_dim):
        self.ep, self.tp, self.rows, self.width = ep, tp, rows, width
        self.tokens, self.hidden, self.shared = tokens, hidden, shared
        self.cap, self.stride = capacity, padded(capacity)
        self.value_dim = value_dim
        self.half = ep // 2
        self.own = rows // tp
        self.tile = min(512, width)

    def names(self):
        half, ep = self.half, self.ep
        crossing = [("n", d) for d in range(2, half)] + [("f", d) for d in range(half)]
        groups = (
            [("XY", 0), ("INFO", 0), ("XC", 0), ("XC", 1)]
            + [("FAR", d) for d in range(half)]
            + [("NEAR", d, 0) for d in range(1, half)]
            + [("NEAR", 1, 1)]
            + [("FY",) + name for name in crossing]
            + [("RET", d) for d in range(half)]
            + [("NRET", d, c) for d in range(1, half) for c in range(2)]
            + [("SC", 0), ("SC", 1), ("AY", 0), ("AY", 1), ("KVF", 0), ("OC", 0), ("OY", 0)]
            + [("KVN", d) for d in range(1, half)]
            + [("KVC", d) for d in range(1, half)]
        )
        table = {name: number for number, name in enumerate(groups)}
        first = len(groups)
        table["RC"], table["PC"], table["QY"] = first, first + ep, first + 2 * ep
        return table, first + 3 * ep

    def scratch(self):
        bf, f32 = jnp.bfloat16, jnp.float32
        ep, half, width, stride = self.ep, self.half, self.width, self.stride
        tokens, rows, hidden, shared = self.tokens, self.rows, self.hidden, self.shared
        vd = self.value_dim
        return dict(
            mx=((rows, width), bf),
            wq=((width, 4 * HEAD), bf),
            wk=((2 * HEAD, width), bf),
            x=((tokens, width), bf),
            info=((8, tokens), f32),
            ids=((2, tokens), jnp.int32),
            gates=((2, tokens), f32),
            wv=((width, vd), bf),
            wo=((2 * vd, width), bf),
            wg=((width, hidden), bf),
            wu=((width, hidden), bf),
            wd=((hidden, width), bf),
            sg=((width, shared), bf),
            su=((width, shared), bf),
            sd=((shared, width), bf),
            xb=((2, 2, tokens, width), bf),
            other=((8, tokens), f32),
            outf=((half, stride, width), bf),
            outn=((half, 2, stride, width), bf),
            r=((ep, 2, 2, stride, width), bf),
            p=((ep, 2, 2, stride, width), bf),
            pr=((ep, 2, stride, width), bf),
            q=((ep, 2, stride, width), bf),
            qr=((ep, stride, width), bf),
            fb=((ep, stride, width), bf),
            tn=((2, half, stride, width), bf),
            tf=((half, stride, width), bf),
            s=((2, 2, tokens, width), bf),
            sr=((2, tokens, width), bf),
            ao=((tokens, width), bf),
            ar=((tokens, width), bf),
            acc=((tokens, width), f32),
            wown=((2, tokens, half * stride), bf),
            wfar=((half, 2, tokens, stride), bf),
            woth=((2, tokens, half * stride), bf),
            nm=((rows, width), bf),
            qs=((2, 2, rows, 2 * HEAD), bf),
            kv=((ep, rows, 2 * HEAD + vd), bf),
            sc=((2, ep, rows, rows), f32),
            stat=((2, rows, 128), f32),
            tot=((2, rows, 128), f32),
            pv=((2, rows, vd), f32),
            hr=((rows, 2 * vd), bf),
            o=((2, 2, self.own, width), bf),
            orx=((2, self.own, width), bf),
            oq=((2, self.own, width), bf),
            oy=((self.own, width), bf),
        )

    def vmem_bytes(self):
        total = 0
        for shape, dtype in self.scratch().values():
            size = jnp.dtype(dtype).itemsize
            for extent in shape[:-1]:
                size *= extent
            total += size * (-(-shape[-1] // 128) * 128)
        return total


def step_plan(half):
    order = chunk_order(half)
    place = {name: number for number, name in enumerate(order)}
    plan = {number: [] for number in range(2 * half + 1)}
    early = half // 2
    for d in range(early):
        plan[place[("f", d)]] += [("crossed", "f", d)]
    plan[early] += [("core_sum", "n", 0), ("relay_kv",)]
    first = place[("n", 1)]
    plan[first] += [("crossed", "n", 2)] * (half > 2) + [("arrive_near",)]
    for d in range(3, half):
        plan[place[("n", d)] - 1] += [("crossed", "n", d)]
    for d in range(early):
        plan[first + d] += [("core_sum", "f", d)]
    for d in range(1, half):
        plan[place[("n", d)] + 2] += [("core_sum", "n", d)]
    for d in range(early, half):
        plan[place[("f", d)] - 1] += [("arrive_cross", "f", d)]
    for d in range(early):
        plan[first + d + 2] += [("side_sum", d)]
    for d in range(early, half):
        at = plan[place[("f", d)]]
        if d == half - 1:
            at += [("core_sum", "f", d - 1), ("kv_arrivals",), ("head", 0)]
        at += [("crossed", "f", d)]
    last = plan[2 * half]
    last += [("core_sum", "f", half - 1), ("side_sum", early), ("other_rows", 0), ("head", 1)]
    last += [("project_out",)] + [("side_sum", d) for d in range(early + 1, half)]
    last += [("mix_sum",), ("other_rows", 1), ("own_rows",)]
    return plan


class Later:
    def __init__(self, start):
        self.start = start


def fused_kernel(sizes, keys, *refs):
    lam, xgain, mgain, hgain = refs[:4]
    (h_x, h_ids, h_gates, h_mx, h_q1, h_q2, h_k1, h_k2, h_v) = refs[4:13]
    (h_wo, h_g, h_u, h_d, h_sg, h_su, h_sd) = refs[13:20]
    mix_out, exp_out = refs[20:22]
    b = dict(zip(keys, refs[22 : 22 + len(keys)]))
    send_sem, recv_sem, load_sem = refs[22 + len(keys) :]
    x, info = b["x"], b["info"]
    half, ep, width, stride, cap = sizes.half, sizes.ep, sizes.width, sizes.stride, sizes.cap
    tokens, rows, tile, vd = sizes.tokens, sizes.rows, sizes.tile, sizes.value_dim
    f32, bf = jnp.float32, jnp.bfloat16
    table, _ = sizes.names()
    order = chunk_order(half)
    place = {name: number for number, name in enumerate(order)}

    me = lax.axis_index("ep")
    tp = lax.axis_index("tp")
    side = me // half
    spot = me % half
    row_of = tp // 2
    core = tp % 2
    tiles = width // tile

    lines = half // 2
    line, lane_x = spot // 2, spot % 2

    def shifted(which, d, turn):
        moved = (line + lines + turn * (d // 2)) % lines
        return which * half + moved * 2 + (lane_x + d % 2) % 2

    near_to = [shifted(side, d, 1) for d in range(half)]
    near_by = [shifted(side, d, -1) for d in range(half)]
    far_to = [shifted(1 - side, d, 1) for d in range(half)]
    far_by = [shifted(1 - side, d, -1) for d in range(half)]
    early = half // 2

    def near(d):
        return (near_to[d], tp)

    def near_from(d):
        return (near_by[d], tp)

    def far(d):
        return (far_to[d], tp)

    def far_from(d):
        return (far_by[d], tp)

    partner_y = (me, (1 - row_of) * 2 + core)
    partner_c = (me, row_of * 2 + 1 - core)

    def remote(number, source, target, device):
        return pltpu.make_async_remote_copy(
            src_ref=source,
            dst_ref=target,
            send_sem=send_sem.at[number],
            recv_sem=recv_sem.at[number],
            device_id=device,
            device_id_type=pl.DeviceIdType.MESH,
        )

    copies = {}

    def made(name):
        source, target, device = copies[name]
        return remote(table[name], source(), target(), device)

    def copy(name, source, target, device):
        copies[name] = (source, target, device)
        return Later(lambda: made(name).start())

    def dot(left, right):
        return jnp.dot(left, right, preferred_element_type=f32)

    crossing = [("n", d) for d in range(2, half)] + [("f", d) for d in range(half)]
    for kind, d in crossing:
        position = place[(kind, d)]
        copies[("FY", kind, d)] = (
            lambda position=position: b["r"].at[position, 0, 0, pl.ds(0, cap)],
            lambda position=position: b["r"].at[position, 0, 1, pl.ds(0, cap)],
            partner_y,
        )
    for d in range(half):
        copies[("RET", d)] = (
            lambda d=d: b["fb"].at[place[("f", d)], pl.ds(0, cap)],
            lambda d=d: b["tf"].at[d, pl.ds(0, cap)],
            far_from(d),
        )
    for d in range(1, half):
        for c in range(2):
            cols = pl.ds(c * width // 2, width // 2)
            copies[("NRET", d, c)] = (
                lambda d=d, cols=cols: b["q"].at[place[("n", d)], :, pl.ds(0, cap), cols],
                lambda d=d, cols=cols: b["tn"].at[:, d, pl.ds(0, cap), cols],
                near_from(d),
            )

    loads = {}
    pairs = dict(
        x=(h_x, b["x"]),
        ids=(h_ids, b["ids"]),
        gates=(h_gates, b["gates"]),
        mx=(h_mx, b["mx"]),
        q1=(h_q1, b["wq"].at[:, : 2 * HEAD]),
        q2=(h_q2, b["wq"].at[:, 2 * HEAD :]),
        k1=(h_k1, b["wk"].at[:HEAD]),
        k2=(h_k2, b["wk"].at[HEAD:]),
        v=(h_v, b["wv"]),
        sg=(h_sg, b["sg"]),
        su=(h_su, b["su"]),
        sd=(h_sd, b["sd"]),
        wg=(h_g.at[0], b["wg"]),
        wu=(h_u.at[0], b["wu"]),
        wd=(h_d.at[0], b["wd"]),
        wo=(h_wo, b["wo"]),
    )
    for number, (name, (source, target)) in enumerate(pairs.items()):
        loads[name] = pltpu.make_async_copy(source, target, load_sem.at[number])
        loads[name].start()

    barrier = pltpu.get_barrier_semaphore()
    peers = [near(d) for d in range(1, half)] + [far(d) for d in range(half)]
    peers += [partner_y, partner_c]
    for device in peers:
        pl.semaphore_signal(
            barrier, inc=1, device_id=device, device_id_type=pl.DeviceIdType.MESH
        )

    def norm_rows(source, target, count, gain):
        step = min(32, count)

        @pl.loop(0, count // step)
        def _(index):
            at = pl.ds(pl.multiple_of(index * step, step), step)
            values = source[at, :].astype(f32)
            factor = lax.rsqrt(jnp.mean(values * values, axis=-1, keepdims=True) + EPS)
            target[at, :] = (values * factor * gain[...]).astype(bf)

    loads["x"].wait()
    norm_rows(x, b["xb"].at[0, 0], tokens, xgain)
    loads["ids"].wait()
    loads["gates"].wait()
    info[...] = jnp.zeros((8, tokens), f32)
    info[0:2, :] = b["ids"][...].astype(f32)
    info[2:4, :] = b["gates"][...]

    earlier = (
        lax.broadcasted_iota(jnp.int32, (tokens, tokens), 0)
        < lax.broadcasted_iota(jnp.int32, (tokens, tokens), 1)
    ).astype(bf)
    padded_ep = -(-ep // 8) * 8
    relative = lax.broadcasted_iota(jnp.int32, (padded_ep, tokens), 0)
    expert = jnp.zeros((padded_ep, tokens), f32) - 1.0
    for k, target in enumerate(near_to + far_to):
        expert = jnp.where(relative == k, target.astype(f32), expert)

    def routing(info_ref):
        first = info_ref[0:1, :] == expert
        second = info_ref[1:2, :] == expert
        named = jnp.where(first | second, 1.0, 0.0)
        position = dot(named.astype(bf), earlier)
        position = jnp.where(named > 0.0, position, -1.0)
        weight = jnp.where(first, info_ref[2:3, :], 0.0) + jnp.where(second, info_ref[3:4, :], 0.0)
        return position, weight

    slot = lax.broadcasted_iota(jnp.int32, (stride, tokens), 0).astype(f32)

    def chosen(position, which):
        return slot == position[which : which + 1, :]

    def select(position, which):
        return jnp.concatenate(
            [jnp.where(chosen(position, k), 1.0, 0.0) for k in which], axis=0
        ).astype(bf)

    def spread(position, weight, which):
        stacked = jnp.concatenate(
            [jnp.where(chosen(position, k), weight[k : k + 1, :], 0.0) for k in which], axis=0
        )
        turned = stacked.T
        upper = turned.astype(bf)
        return upper, (turned - upper.astype(f32)).astype(bf)

    own_place, own_weight = routing(info)
    near_set = list(range(half))
    far_set = list(range(half, 2 * half))
    direct_set = [0, 1]
    select_near = select(own_place, near_set)
    select_far = select(own_place, far_set)

    pl.semaphore_wait(barrier, len(peers))
    copy(("XY", 0), lambda: b["xb"].at[0, 0], lambda: b["xb"].at[1, 0], partner_y).start()
    copy(("INFO", 0), lambda: info, lambda: b["other"], partner_y).start()
    copy(("XC", 0), lambda: b["xb"].at[0, 0], lambda: b["xb"].at[0, 1], partner_c).start()

    def pick(select_rows, source, store):
        for n in range(tiles):
            cols = slice(n * tile, (n + 1) * tile)
            picked = dot(select_rows, source[:, cols]).astype(bf)
            for d in range(select_rows.shape[0] // stride):
                store(d, cols, picked[d * stride : (d + 1) * stride, :])

    def store_near(a):
        def store(d, cols, value):
            b["outn"][d, a, :, cols] = value

        return store

    def store_far(d, cols, value):
        b["outf"][d, :, cols] = value

    pick(select_near, b["xb"].at[0, 0], store_near(0))

    def core_forward(position):
        return remote(
            table["RC"] + position, b["r"].at[position, 0], b["r"].at[position, 1], partner_c
        )

    def arrive_cross(kind, d):
        made(("FAR", d) if kind == "f" else ("NEAR", d, 0)).wait_recv()
        made(("FY", kind, d)).start()

    def crossed(kind, d):
        made(("FY", kind, d)).wait_recv()
        core_forward(place[(kind, d)]).start()

    def arrive_near():
        for a in range(2):
            made(("NEAR", 1, a)).wait_recv()
        core_forward(place[("n", 1)]).start()

    def relay_kv():
        @pl.when(side == 1)
        def _():
            slot_of = b["kv"].at[far_by[0]]
            remote(table[("KVF", 0)], slot_of, slot_of, far(0)).wait_recv()

        for d in range(1, half):
            copy(("KVC", d), lambda: b["kv"].at[far_by[0]], lambda: b["kv"].at[far_by[0]], near(d))

            @pl.when(side == 1)
            def _(d=d):
                made(("KVC", d)).start()

    def other_spread():
        upper, lower = spread(other_place, other_weight, near_set)
        b["woth"][0] = upper
        b["woth"][1] = lower

    def start_near(a):
        for d in (range(1, half) if a == 0 else (1,)):
            copy(
                ("NEAR", d, a),
                lambda d=d: b["outn"].at[d, a, pl.ds(0, cap)],
                lambda d=d: b["r"].at[place[("n", d)], 0, a, pl.ds(0, cap)],
                near(d),
            ).start()

    start_near(0)
    pick(select_far, b["xb"].at[0, 0], store_far)

    def start_far(d):
        copy(
            ("FAR", d),
            lambda: b["outf"].at[d, pl.ds(0, cap)],
            lambda: b["r"].at[place[("f", d)], 0, 0, pl.ds(0, cap)],
            far(d),
        ).start()

    for d in range(early):
        start_far(d)

    loads["mx"].wait()
    norm_rows(b["mx"], b["nm"], rows, mgain)
    for name in ("q1", "q2", "k1", "k2", "v"):
        loads[name].wait()
    lane = lax.broadcasted_iota(jnp.int32, (rows, 2 * HEAD), 1)
    b["kv"][me, :, : 2 * HEAD] = lax.dot_general(
        b["nm"][...], b["wk"][...], (((1,), (1,)), ((), ())), preferred_element_type=f32
    ).astype(bf)
    b["kv"][me, :, 2 * HEAD :] = dot(b["nm"][...], b["wv"][...]).astype(bf)

    copy(("KVF", 0), lambda: b["kv"].at[me], lambda: b["kv"].at[me], far(0))

    @pl.when(side == 0)
    def _():
        made(("KVF", 0)).start()

    for d in range(1, half):
        copy(("KVN", d), lambda: b["kv"].at[me], lambda: b["kv"].at[me], near(d))

        @pl.when(near_to[d] > me)
        def _(d=d):
            made(("KVN", d)).start()

    for m in range(2):
        queries = dot(b["nm"][...], b["wq"][:, m * 2 * HEAD : (m + 1) * 2 * HEAD])
        turned = pltpu.roll(queries, HEAD, 1)
        keep = (lane < HEAD) if m == 0 else (lane >= HEAD)
        for g in range(2):
            source = queries if g == m else turned
            b["qs"][m, g] = jnp.where(keep, source, 0.0).astype(bf)

    def shared_expert(a):
        both = b["xb"][a].reshape(2 * tokens, width)
        gated = dot(both, b["sg"][...])
        lifted = dot(both, b["su"][...])
        hidden = (jax.nn.silu(gated) * lifted).astype(bf)
        for n in range(tiles):
            cols = slice(n * tile, (n + 1) * tile)
            part = dot(hidden, b["sd"][:, cols]).astype(bf)
            b["s"][a, 0, :, cols] = part[:tokens]
            b["s"][a, 1, :, cols] = part[tokens:]

    for name in ("sg", "su", "sd"):
        loads[name].wait()
    made(("XC", 0)).wait_recv()
    shared_expert(0)
    copy(("SC", 0), lambda: b["s"].at[0, 1], lambda: b["sr"].at[0], partner_c).start()

    upper, lower = spread(own_place, own_weight, near_set)
    b["wown"][0] = upper
    b["wown"][1] = lower
    for d in range(half):
        upper, lower = spread(own_place, own_weight, [half + d])
        b["wfar"][d, 0] = upper
        b["wfar"][d, 1] = lower
    for d in range(half):
        b["tf"][d, cap:, :] = jnp.zeros((stride - cap, width), bf)
        for a in range(2):
            b["tn"][a, d, cap:, :] = jnp.zeros((stride - cap, width), bf)
    made(("XY", 0)).wait_recv()
    made(("INFO", 0)).wait_recv()
    copy(("XC", 1), lambda: b["xb"].at[1, 0], lambda: b["xb"].at[1, 1], partner_c).start()
    arrive_cross("f", 0)
    other_place, other_weight = routing(b["other"])
    pick(select(other_place, direct_set), b["xb"].at[1, 0], store_near(1))
    start_near(1)
    for d in range(early, half):
        start_far(d)
    b["r"][0, 0] = b["outn"][0]

    core_forward(0).start()
    made(("XC", 1)).wait_recv()
    shared_expert(1)
    copy(("SC", 1), lambda: b["s"].at[1, 1], lambda: b["sr"].at[1], partner_c).start()
    other_spread()
    for d in range(1, early):
        arrive_cross("f", d)
    for d in range(2, half):
        arrive_cross("n", d)

    for name in ("wg", "wu", "wd"):
        loads[name].wait()

    far_places = [place[("f", d)] for d in range(half)]
    row_count = 4 * stride

    def back_copy(number):
        return remote(
            table["PC"] + number, b["p"].at[number, 1], b["pr"].at[number], partner_c
        )

    def cross_copy(number):
        return remote(
            table["QY"] + number,
            b["q"].at[number, 1, pl.ds(0, cap)],
            b["qr"].at[number, pl.ds(0, cap)],
            partner_y,
        )

    def core_sum(kind, d):
        position = place[(kind, d)]
        back_copy(position).wait_recv()
        for a in range(2):
            b["q"][position, a] = (
                b["p"][position, 0, a].astype(f32) + b["pr"][position, a].astype(f32)
            ).astype(bf)
        if kind == "f":
            cross_copy(position).start()
        elif d > 0:
            for c in range(2):
                made(("NRET", d, c)).start()
        else:
            for a in range(2):
                b["tn"][a, 0, 0:cap, :] = b["q"][position, a, 0:cap, :]

    def side_sum(d):
        position = place[("f", d)]
        cross_copy(position).wait_recv()
        b["fb"][position] = (
            b["q"][position, 0].astype(f32) + b["qr"][position].astype(f32)
        ).astype(bf)
        made(("RET", d)).start()

    def kv_arrival(name, source, d):
        block = b["kv"].at[source]
        remote(table[(name, d)], block, block, near(d)).wait_recv()

    def kv_arrivals():
        for d in range(1, half):

            @pl.when(near_by[d] < me)
            def _(d=d):
                kv_arrival("KVN", near_by[d], d)

            @pl.when(side == 1)
            def _(d=d):
                kv_arrival("KVC", far_by[d], d)

    scale = HEAD**-0.5 * math.log2(math.e)
    row_place = me * rows + lax.broadcasted_iota(jnp.int32, (rows, rows), 0)
    col_place = lax.broadcasted_iota(jnp.int32, (rows, rows), 1)
    halves = [slice(c * 128, (c + 1) * 128) for c in range(rows // 128)]

    def head(g):
        b["stat"][...] = jnp.full((2, rows, 128), NEG, f32)
        b["tot"][...] = jnp.zeros((2, rows, 128), f32)
        b["pv"][...] = jnp.zeros((2, rows, vd), f32)

        def score(j, carry):
            keys_j = b["kv"][j, :, 0 : 2 * HEAD]
            for m in range(2):
                scores = lax.dot_general(
                    b["qs"][m, g], keys_j, (((1,), (1,)), ((), ())), preferred_element_type=f32
                )
                scores = jnp.where(j * rows + col_place <= row_place, scores, NEG)
                b["sc"][m, j] = scores
                most = b["stat"][m]
                for cols in halves:
                    most = jnp.maximum(most, scores[:, cols])
                b["stat"][m] = most
            return carry

        lax.fori_loop(0, me + 1, score, 0)
        for m in range(2):
            most = jnp.max(b["stat"][m], axis=1, keepdims=True)
            b["stat"][m] = jnp.broadcast_to(most, (rows, 128))

        def weigh(j, carry):
            values = b["kv"][j, :, 2 * HEAD :]
            for m in range(2):
                most = b["stat"][m]
                total = b["tot"][m]
                parts = []
                for cols in halves:
                    weights = jnp.exp2((b["sc"][m, j, :, cols] - most) * scale)
                    total = total + weights
                    parts.append(weights.astype(bf))
                b["tot"][m] = total
                b["pv"][m] += dot(jnp.concatenate(parts, axis=1), values)
            return carry

        lax.fori_loop(0, me + 1, weigh, 0)
        sums = [jnp.sum(b["tot"][m], axis=1, keepdims=True) for m in range(2)]
        combined = b["pv"][0] / sums[0] - lam[g] * (b["pv"][1] / sums[1])
        factor = lax.rsqrt(jnp.mean(combined * combined, axis=1, keepdims=True) + EPS)
        b["hr"][:, g * vd : (g + 1) * vd] = (combined * factor * hgain[...]).astype(bf)

    def project_out():
        loads["wo"].wait()
        own = sizes.own
        for n in range(tiles):
            cols = slice(n * tile, (n + 1) * tile)
            part = dot(b["hr"][...], b["wo"][:, cols]).astype(bf)
            b["o"][:, :, :, cols] = part.reshape(2, 2, own, tile)
        made(("OC", 0)).start()

    def other_rows(c):
        for d in range(1, half):
            made(("NRET", d, c)).wait_recv()
        if c == 0:
            for a in range(2):
                made(("SC", a)).wait_recv()
        for n in range(c * tiles // 2, (c + 1) * tiles // 2):
            cols = slice(n * tile, (n + 1) * tile)
            back = b["tn"][1, :, :, cols].reshape(half * stride, tile)
            total = dot(b["woth"][0], back) + dot(b["woth"][1], back)
            total = total + b["s"][1, 0, :, cols].astype(f32) + b["sr"][1, :, cols].astype(f32)
            b["ao"][:, cols] = total.astype(bf)
        made(("AY", c)).start()

    def mix_sum():
        made(("OC", 0)).wait_recv()
        for a in range(2):
            b["oq"][a] = (b["o"][a, core].astype(f32) + b["orx"][a].astype(f32)).astype(bf)
        made(("OY", 0)).start()

    def own_rows():
        for n in range(tiles):
            cols = slice(n * tile, (n + 1) * tile)
            back = b["tn"][0, :, :, cols].reshape(half * stride, tile)
            total = dot(b["wown"][0], back) + dot(b["wown"][1], back)
            b["acc"][:, cols] = (
                total + b["s"][0, 0, :, cols].astype(f32) + b["sr"][0, :, cols].astype(f32)
            )

    copies[("OC", 0)] = (lambda: b["o"].at[:, 1 - core], lambda: b["orx"], partner_c)
    for c in range(2):
        cols = pl.ds(c * width // 2, width // 2)
        copies[("AY", c)] = (
            lambda cols=cols: b["ao"].at[:, cols],
            lambda cols=cols: b["ar"].at[:, cols],
            partner_y,
        )
    copies[("OY", 0)] = (lambda: b["oq"].at[1 - row_of], lambda: b["oy"], partner_y)
    schedule = step_plan(half)
    actions = dict(
        arrive_cross=arrive_cross,
        crossed=crossed,
        arrive_near=arrive_near,
        core_sum=core_sum,
        side_sum=side_sum,
        kv_arrivals=kv_arrivals,
        head=head,
        relay_kv=relay_kv,
        project_out=project_out,
        mix_sum=mix_sum,
        other_rows=other_rows,
        own_rows=own_rows,
    )

    def step_body(step, carry):
        for when in sorted(schedule):

            @pl.when(step == when)
            def _(when=when):
                for name, *values in schedule[when]:
                    actions[name](*values)

        @pl.when(step < ep)
        def _():
            core_forward(step).wait_recv()
            arrived = b["r"][step].reshape(row_count, width)
            gated = dot(arrived, b["wg"][...])
            lifted = dot(arrived, b["wu"][...])
            hidden = (jax.nn.silu(gated) * lifted).astype(bf)
            for n in range(tiles):
                cols = slice(n * tile, (n + 1) * tile)
                part = dot(hidden, b["wd"][:, cols]).astype(bf)
                b["p"][step, :, :, :, cols] = part.reshape(2, 2, stride, tile)
            back_copy(step).start()

        return carry

    lax.fori_loop(0, max(schedule) + 1, step_body, 0)

    made(("OY", 0)).wait_recv()
    mix_out[...] = (b["oq"][row_of].astype(f32) + b["oy"][...].astype(f32)).astype(bf)

    for d in range(half):
        made(("RET", d)).wait_recv()
        for n in range(tiles):
            cols = slice(n * tile, (n + 1) * tile)
            back = b["tf"][d, :, cols]
            b["acc"][:, cols] += dot(b["wfar"][d, 0], back) + dot(b["wfar"][d, 1], back)
    for c in range(2):
        made(("AY", c)).wait_recv()
        cols = slice(c * width // 2, (c + 1) * width // 2)
        exp_out[:, cols] = (b["acc"][:, cols] + b["ar"][:, cols].astype(f32)).astype(bf)

    conditional = {("KVF", 0): side == 0}
    for d in range(1, half):
        conditional[("KVN", d)] = near_to[d] > me
        conditional[("KVC", d)] = side == 1
    for name in copies:
        if name in conditional:

            @pl.when(conditional[name])
            def _(name=name):
                made(name).wait_send()

        else:
            made(name).wait_send()
    for position in range(ep):
        core_forward(position).wait_send()
        back_copy(position).wait_send()
        if position in far_places:
            cross_copy(position).wait_send()


def fused(sizes, args):
    scratch = sizes.scratch()
    keys = list(scratch)
    _, count = sizes.names()
    vmem = pl.BlockSpec(memory_space=pltpu.VMEM)
    smem = pl.BlockSpec(memory_space=pltpu.SMEM)
    hbm = pl.BlockSpec(memory_space=pltpu.HBM)
    return pl.pallas_call(
        functools.partial(fused_kernel, sizes, keys),
        out_shape=(
            jax.ShapeDtypeStruct((sizes.own, sizes.width), jnp.bfloat16),
            jax.ShapeDtypeStruct((sizes.tokens, sizes.width), jnp.bfloat16),
        ),
        in_specs=[smem] + [vmem] * 3 + [hbm] * 16,
        out_specs=(vmem, vmem),
        scratch_shapes=[pltpu.VMEM(shape, dtype) for shape, dtype in scratch.values()]
        + [
            pltpu.SemaphoreType.DMA((count,)),
            pltpu.SemaphoreType.DMA((count,)),
            pltpu.SemaphoreType.DMA((16,)),
        ],
        compiler_params=pltpu.CompilerParams(
            collective_id=0, has_side_effects=True, vmem_limit_bytes=VMEM_LIMIT
        ),
        name="layer",
    )(*args)


VMEM_LIMIT = 67043328


def fused_body(sizes, *arrays):
    (
        mixer_input,
        mixer_gain,
        query_one,
        query_two,
        key_one,
        key_two,
        value_weight,
        lambdas,
        head_gain,
        output_weight,
        expert_input,
        expert_gain,
        routes,
        route_weight,
        expert_gate,
        expert_up,
        expert_down,
        shared_gate,
        shared_up,
        shared_down,
    ) = arrays
    return fused(
        sizes,
        (
            lambdas,
            expert_gain.reshape(1, -1),
            mixer_gain.reshape(1, -1),
            head_gain.reshape(1, -1),
            expert_input,
            routes.T,
            route_weight.T,
            mixer_input,
            query_one,
            query_two,
            key_one.T,
            key_two.T,
            value_weight,
            output_weight,
            expert_gate,
            expert_up,
            expert_down,
            shared_gate,
            shared_up,
            shared_down,
        ),
    )


def body(*arrays):
    ep_size, tp_size = lax.axis_size("ep"), lax.axis_size("tp")
    mixer_input, query_one, key_one = arrays[0], arrays[2], arrays[4]
    head_gain, expert_input, routes = arrays[8], arrays[10], arrays[12]
    expert_gate, shared_gate = arrays[14], arrays[17]
    rows, width = mixer_input.shape
    tokens, top_count = routes.shape
    local_experts = expert_gate.shape[0]
    capacity = max(2, 5 * tokens * top_count // (4 * local_experts * ep_size))
    fits = (
        tp_size == 4
        and ep_size % 2 == 0
        and ep_size >= 4
        and local_experts == 1
        and top_count == 2
        and key_one.shape[1] == HEAD
        and query_one.shape[1] == 2 * HEAD
        and head_gain.shape[0] == 128
        and tokens == 128
        and rows % (16 * tp_size) == 0
        and rows % 128 == 0
        and width % 512 == 0
        and expert_input.shape[1] == width
        and capacity % 8 == 0
    )
    if fits:
        sizes = Sizes(
            ep_size,
            tp_size,
            rows,
            width,
            tokens,
            expert_gate.shape[2],
            shared_gate.shape[1],
            capacity,
            head_gain.shape[0],
        )
        if sizes.vmem_bytes() + 8 * 2**20 <= VMEM_LIMIT:
            return fused_body(sizes, *arrays)
    return general_body(*arrays)


def solution(mesh):
    in_specs = (
        P("ep", None),
        P(),
        P(None, "tp"),
        P(None, "tp"),
        P(None, "tp"),
        P(None, "tp"),
        P(None, "tp"),
        P("tp"),
        P(),
        P("tp", None),
        P(("ep", "tp"), None),
        P(),
        P(("ep", "tp"), None),
        P(("ep", "tp"), None),
        P("ep", None, "tp"),
        P("ep", None, "tp"),
        P("ep", "tp", None),
        P(None, "tp"),
        P(None, "tp"),
        P("tp", None),
    )
    out_specs = (P(("ep", "tp"), None), P(("ep", "tp"), None))
    return jax.shard_map(body, mesh=mesh, in_specs=in_specs, out_specs=out_specs, check_vma=False)
```

```python
import functools
import math

import jax
import jax.numpy as jnp
from jax import lax
from jax.experimental import pallas as pl
from jax.experimental.pallas import tpu as pltpu
from jax.sharding import PartitionSpec as P

HEAD = 64


EPS = 1e-06
NEG = -1e30


def normalize(activations, scaling):
    values = activations.astype(jnp.float32)
    factor = lax.rsqrt(jnp.mean(values * values, axis=-1, keepdims=True) + EPS)
    return (values * factor * scaling).astype(jnp.bfloat16)


def attention_kernel(
    shape, rank_ref, lambdas_ref, queries_ref, keys_ref, gain_ref, out_ref, maxima, totals, weighted
):
    rows, chunk, local_kv, group, value_dim = shape
    rank = rank_ref[0]
    maxima[...] = jnp.full(maxima.shape, NEG, jnp.float32)
    totals[...] = jnp.zeros(totals.shape, jnp.float32)
    weighted[...] = jnp.zeros(weighted.shape, jnp.float32)
    heads = local_kv * group
    key_cols = local_kv * HEAD
    chunks = rows // chunk
    scale = HEAD**-0.5 * math.log2(math.e)

    def block(index, masked):
        start = pl.multiple_of(index * rows, rows)
        for kv in range(local_kv):
            value_start = 2 * key_cols + kv * value_dim
            for part in range(chunks):
                span = (part + 1) * chunk if masked else rows
                values = keys_ref[pl.ds(start, span), value_start : value_start + value_dim]
                for which in range(2):
                    first = which * key_cols + kv * HEAD
                    keys = keys_ref[pl.ds(start, span), first : first + HEAD]
                    for g in range(group):
                        head = kv * group + g
                        col = (which * heads + head) * HEAD
                        queries = queries_ref[part * chunk : (part + 1) * chunk, col : col + HEAD]
                        scores = lax.dot_general(
                            queries,
                            keys,
                            (((1,), (1,)), ((), ())),
                            preferred_element_type=jnp.float32,
                        )
                        if masked:
                            row = part * chunk + lax.broadcasted_iota(jnp.int32, scores.shape, 0)
                            col_pos = lax.broadcasted_iota(jnp.int32, scores.shape, 1)
                            scores = jnp.where(col_pos <= row, scores, NEG)
                        slot = (which * heads + head) * chunks + part
                        earlier = maxima[slot]
                        latest = jnp.maximum(earlier, jnp.max(scores, axis=1, keepdims=True))
                        shrink = jnp.exp2((earlier - latest) * scale)
                        weights = jnp.exp2((scores - latest[:, :1]) * scale)
                        totals[slot] = totals[slot] * shrink + jnp.sum(
                            weights, axis=1, keepdims=True
                        )
                        weighted[slot] = weighted[slot] * shrink[:, :1] + jnp.dot(
                            weights.astype(jnp.bfloat16),
                            values,
                            preferred_element_type=jnp.float32,
                        )
                        maxima[slot] = latest

    def earlier_block(index, carry):
        block(index, False)
        return carry

    lax.fori_loop(0, rank, earlier_block, 0)
    block(rank, True)
    for head in range(heads):
        for part in range(chunks):
            one = head * chunks + part
            two = (heads + head) * chunks + part
            combined = (
                weighted[one] / totals[one][:, :1]
                - lambdas_ref[head] * (weighted[two] / totals[two][:, :1])
            )
            factor = lax.rsqrt(jnp.mean(combined * combined, axis=1, keepdims=True) + EPS)
            out_ref[
                part * chunk : (part + 1) * chunk, head * value_dim : (head + 1) * value_dim
            ] = (combined * factor * gain_ref[...]).astype(jnp.bfloat16)


def attention(queries, keys, rank, lambdas, head_gain, local_kv, group):
    rows = queries.shape[0]
    value_dim = head_gain.shape[0]
    heads = local_kv * group
    chunk = min(128, rows)
    slots = 2 * heads * (rows // chunk)
    vmem = pl.BlockSpec(memory_space=pltpu.VMEM)
    smem = pl.BlockSpec(memory_space=pltpu.SMEM)
    scores = heads * 2 * rows * keys.shape[0]
    return pl.pallas_call(
        functools.partial(attention_kernel, (rows, chunk, local_kv, group, value_dim)),
        out_shape=jax.ShapeDtypeStruct((rows, heads * value_dim), jnp.bfloat16),
        in_specs=[smem, smem, vmem, vmem, vmem],
        out_specs=vmem,
        scratch_shapes=[
            pltpu.VMEM((slots, chunk, 128), jnp.float32),
            pltpu.VMEM((slots, chunk, 128), jnp.float32),
            pltpu.VMEM((slots, chunk, value_dim), jnp.float32),
        ],
        compiler_params=pltpu.CompilerParams(vmem_limit_bytes=48 * 1024 * 1024),
        cost_estimate=pl.CostEstimate(
            flops=8 * scores * HEAD, bytes_accessed=keys.size * 2, transcendentals=scores
        ),
        name="attention",
    )(rank.reshape(1), lambdas, queries, keys, head_gain.reshape(1, value_dim))


def swap(rows, axis, size, distance):
    return lax.ppermute(rows, axis, [(i, i ^ distance) for i in range(size)])


def gather_near(block, axis, size, ahead=None):
    places = {0: block}
    distance = size // 2
    while distance:
        for place in sorted(places):
            moved = swap(places[place], axis, size, distance)
            if ahead is not None:
                moved, ahead = lax.optimization_barrier((moved, ahead))
            places[place ^ distance] = moved
        ahead = None
        distance //= 2
    return [places[place] for place in range(size)]


def scatter_near(partials, axis, size):
    sums = dict(enumerate(partials))
    distance = 1
    while distance < size:
        kept = [place for place in sorted(sums) if not place & distance]
        moved = {
            place: swap(sums[place ^ distance].astype(jnp.bfloat16), axis, size, distance)
            for place in kept
        }
        sums = {
            place: sums[place].astype(jnp.float32) + moved[place].astype(jnp.float32)
            for place in kept
        }
        distance *= 2
    return sums[0]


def general_body(
    mixer_input,
    mixer_gain,
    query_one,
    query_two,
    key_one,
    key_two,
    value_weight,
    lambdas,
    head_gain,
    output_weight,
    expert_input,
    expert_gain,
    routes,
    route_weight,
    expert_gate,
    expert_up,
    expert_down,
    shared_gate,
    shared_up,
    shared_down,
):
    ep_size = lax.axis_size("ep")
    tp_size = lax.axis_size("tp")
    ep_rank = lax.axis_index("ep")
    mixer_rows = mixer_input.shape[0]
    model_width = mixer_input.shape[1]
    query_cols = query_one.shape[1]
    key_cols = key_one.shape[1]
    value_dim = head_gain.shape[0]
    local_kv = key_cols // HEAD
    local_heads = query_cols // HEAD
    group_size = local_heads // local_kv
    normed = normalize(mixer_input, mixer_gain)

    def project(weights):
        return jnp.concatenate(
            [
                jnp.dot(normed, weight, preferred_element_type=jnp.float32).astype(jnp.bfloat16)
                for weight in weights
            ],
            axis=1,
        )

    key_values = project([key_one, key_two, value_weight])
    query_part = project([query_one, query_two])
    arrived = lax.all_gather(key_values, "ep", axis=0, tiled=True)
    head_rows = attention(
        query_part, arrived, ep_rank, lambdas, head_gain, local_kv, group_size
    )
    tp_rank = lax.axis_index("tp")
    own_rows = mixer_rows // tp_size

    def mixer_place(place):
        rows = lax.dynamic_slice_in_dim(head_rows, (tp_rank ^ place) * own_rows, own_rows, 0)
        return jnp.dot(rows, output_weight, preferred_element_type=jnp.float32).astype(
            jnp.bfloat16
        )

    mixer_sum = scatter_near(
        [mixer_place(place) for place in range(tp_size)], "tp", tp_size
    ).astype(jnp.bfloat16)

    token_rows = expert_input.shape[0]
    normed_experts = normalize(expert_input, expert_gain)
    experts_local = expert_gate.shape[0]
    expert_count = experts_local * ep_size
    top_count = routes.shape[1]
    capacity = max(2, 5 * token_rows * top_count // (4 * expert_count))
    slot_count = expert_count * capacity
    flat_routes = routes.reshape(-1)
    onehot = (flat_routes[:, None] == jnp.arange(expert_count, dtype=jnp.int32)[None, :]).astype(
        jnp.int32
    )
    slot_place = jnp.sum((jnp.cumsum(onehot, axis=0) - onehot) * onehot, axis=1)
    slot_ids = (flat_routes * capacity + slot_place).reshape(token_rows, top_count)
    slot_match = jnp.arange(slot_count, dtype=jnp.int32)[:, None, None] == slot_ids[None, :, :]
    select = jnp.any(slot_match, axis=2).astype(jnp.bfloat16)
    outgoing = jnp.dot(select, normed_experts, preferred_element_type=jnp.float32).astype(
        jnp.bfloat16
    )
    pair_rows = experts_local * capacity
    outgoing = outgoing.reshape(ep_size, pair_rows, model_width)
    outgoing, key_values = lax.optimization_barrier((outgoing, key_values))
    received = lax.all_to_all(outgoing, "ep", split_axis=0, concat_axis=0, tiled=True)
    received = received.reshape(ep_size, experts_local, capacity, model_width)
    if experts_local == 1:
        received = received.reshape(ep_size * capacity, model_width)

    def shared_expert(rows):
        gated = jnp.dot(rows, shared_gate, preferred_element_type=jnp.float32)
        lifted = jnp.dot(rows, shared_up, preferred_element_type=jnp.float32)
        hidden = (jax.nn.silu(gated) * lifted).astype(jnp.bfloat16)
        return jnp.dot(hidden, shared_down, preferred_element_type=jnp.float32).astype(
            jnp.bfloat16
        )

    def routed_expert(rows):
        if experts_local == 1:
            gated = jnp.dot(rows, expert_gate[0], preferred_element_type=jnp.float32)
            lifted = jnp.dot(rows, expert_up[0], preferred_element_type=jnp.float32)
            hidden = (jax.nn.silu(gated) * lifted).astype(jnp.bfloat16)
            return jnp.dot(hidden, expert_down[0], preferred_element_type=jnp.float32).astype(
                jnp.bfloat16
            )
        gated = jnp.einsum("secd,edf->secf", rows, expert_gate, preferred_element_type=jnp.float32)
        lifted = jnp.einsum("secd,edf->secf", rows, expert_up, preferred_element_type=jnp.float32)
        hidden = (jax.nn.silu(gated) * lifted).astype(jnp.bfloat16)
        return jnp.einsum(
            "secf,efd->secd", hidden, expert_down, preferred_element_type=jnp.float32
        ).astype(jnp.bfloat16)

    shared_places = gather_near(normed_experts, "tp", tp_size)
    routed_places = gather_near(received, "tp", tp_size, head_rows)
    shared_result = scatter_near([shared_expert(rows) for rows in shared_places], "tp", tp_size)
    routed_result = scatter_near(
        [routed_expert(rows) for rows in routed_places], "tp", tp_size
    ).astype(jnp.bfloat16)
    returned = lax.all_to_all(
        routed_result.reshape(ep_size, pair_rows, model_width),
        "ep",
        split_axis=0,
        concat_axis=0,
        tiled=True,
    )
    returned = returned.reshape(slot_count, model_width)
    spread = jnp.sum(
        jnp.where(
            jnp.arange(slot_count, dtype=jnp.int32)[None, None, :] == slot_ids[:, :, None],
            route_weight[:, :, None],
            0.0,
        ),
        axis=1,
    )
    upper = lax.reduce_precision(spread, 8, 7)
    lower = lax.reduce_precision(spread - upper, 8, 7)
    routed_total = jnp.dot(
        upper.astype(jnp.bfloat16), returned, preferred_element_type=jnp.float32
    ) + jnp.dot(lower.astype(jnp.bfloat16), returned, preferred_element_type=jnp.float32)
    expert_output = (routed_total + shared_result).astype(jnp.bfloat16)
    return (mixer_sum, expert_output)


def chunk_order(half):
    early = half // 2
    order = [("n", 0)] + [("f", d) for d in range(early)]
    order += [("n", d) for d in range(1, half)]
    return order + [("f", d) for d in range(early, half)]


def padded(rows):
    return -(-rows // 16) * 16


class Sizes:
    def __init__(self, ep, tp, rows, width, tokens, hidden, shared, capacity, value_dim):
        self.ep, self.tp, self.rows, self.width = ep, tp, rows, width
        self.tokens, self.hidden, self.shared = tokens, hidden, shared
        self.cap, self.stride = capacity, padded(capacity)
        self.value_dim = value_dim
        self.half = ep // 2
        self.own = rows // tp
        self.tile = min(512, width)

    def names(self):
        half, ep = self.half, self.ep
        crossing = [("n", d) for d in range(2, half)] + [("f", d) for d in range(half)]
        groups = (
            [("XY", 0), ("INFO", 0), ("XC", 0), ("XC", 1)]
            + [("FAR", d) for d in range(half)]
            + [("NEAR", d, 0) for d in range(1, half)]
            + [("NEAR", 1, 1)]
            + [("FY",) + name for name in crossing]
            + [("RET", d) for d in range(half)]
            + [("NRET", d, c) for d in range(1, half) for c in range(2)]
            + [("SC", 0), ("SC", 1), ("AY", 0), ("AY", 1), ("KVF", 0), ("OC", 0), ("OY", 0)]
            + [("KVN", d) for d in range(1, half)]
            + [("KVC", d) for d in range(1, half)]
        )
        table = {name: number for number, name in enumerate(groups)}
        first = len(groups)
        table["RC"], table["PC"], table["QY"] = first, first + ep, first + 2 * ep
        return table, first + 3 * ep

    def scratch(self):
        bf, f32 = jnp.bfloat16, jnp.float32
        ep, half, width, stride = self.ep, self.half, self.width, self.stride
        tokens, rows, hidden, shared = self.tokens, self.rows, self.hidden, self.shared
        vd = self.value_dim
        return dict(
            mx=((rows, width), bf),
            wq=((width, 4 * HEAD), bf),
            wk=((2 * HEAD, width), bf),
            x=((tokens, width), bf),
            info=((8, tokens), f32),
            ids=((2, tokens), jnp.int32),
            gates=((2, tokens), f32),
            wv=((width, vd), bf),
            wo=((2 * vd, width), bf),
            wg=((width, hidden), bf),
            wu=((width, hidden), bf),
            wd=((hidden, width), bf),
            sg=((width, shared), bf),
            su=((width, shared), bf),
            sd=((shared, width), bf),
            xb=((2, 2, tokens, width), bf),
            other=((8, tokens), f32),
            outf=((half, stride, width), bf),
            outn=((half, 2, stride, width), bf),
            r=((ep, 2, 2, stride, width), bf),
            p=((ep, 2, 2, stride, width), bf),
            pr=((ep, 2, stride, width), bf),
            q=((ep, 2, stride, width), bf),
            qr=((ep, stride, width), bf),
            fb=((ep, stride, width), bf),
            tn=((2, half, stride, width), bf),
            tf=((half, stride, width), bf),
            s=((2, 2, tokens, width), bf),
            sr=((2, tokens, width), bf),
            ao=((tokens, width), bf),
            ar=((tokens, width), bf),
            acc=((tokens, width), f32),
            wown=((2, tokens, half * stride), bf),
            wfar=((half, 2, tokens, stride), bf),
            woth=((2, tokens, half * stride), bf),
            nm=((rows, width), bf),
            qs=((2, 2, rows, 2 * HEAD), bf),
            kv=((ep, rows, 2 * HEAD + vd), bf),
            sc=((2, ep, rows, rows), f32),
            stat=((2, rows, 128), f32),
            tot=((2, rows, 128), f32),
            pv=((2, rows, vd), f32),
            hr=((rows, 2 * vd), bf),
            o=((2, 2, self.own, width), bf),
            orx=((2, self.own, width), bf),
            oq=((2, self.own, width), bf),
            oy=((self.own, width), bf),
        )

    def vmem_bytes(self):
        total = 0
        for shape, dtype in self.scratch().values():
            size = jnp.dtype(dtype).itemsize
            for extent in shape[:-1]:
                size *= extent
            total += size * (-(-shape[-1] // 128) * 128)
        return total


def step_plan(half):
    order = chunk_order(half)
    place = {name: number for number, name in enumerate(order)}
    plan = {number: [] for number in range(2 * half + 1)}
    early = half // 2
    plan[early] += [("relay_kv",)]
    for d in range(early):
        plan[place[("f", d)]] += [("crossed", "f", d)]
    plan[early] += [("core_sum", "n", 0)]
    first = place[("n", 1)]
    plan[first] += [("crossed", "n", 2)] * (half > 2) + [("arrive_near",)]
    for d in range(3, half):
        plan[place[("n", d)] - 1] += [("crossed", "n", d)]
    for d in range(early):
        plan[first + d] += [("core_sum", "f", d)]
    for d in range(1, half):
        plan[place[("n", d)] + 2] += [("core_sum", "n", d)]
    for d in range(early, half):
        plan[place[("f", d)] - 1] += [("arrive_cross", "f", d)]
    for d in range(early):
        plan[first + d + 2] += [("side_sum", d)]
    for d in range(early, half):
        at = plan[place[("f", d)]]
        if d == half - 1:
            at += [("core_sum", "f", d - 1), ("kv_arrivals",), ("head", 0)]
        at += [("crossed", "f", d)]
    last = plan[2 * half]
    last += [("core_sum", "f", half - 1), ("side_sum", early), ("other_rows", 0), ("head", 1)]
    last += [("project_out",)] + [("side_sum", d) for d in range(early + 1, half)]
    last += [("mix_sum",), ("other_rows", 1), ("own_rows",)]
    return plan


class Later:
    def __init__(self, start):
        self.start = start


def fused_kernel(sizes, keys, *refs):
    lam, xgain, mgain, hgain = refs[:4]
    (h_x, h_ids, h_gates, h_mx, h_q1, h_q2, h_k1, h_k2, h_v) = refs[4:13]
    (h_wo, h_g, h_u, h_d, h_sg, h_su, h_sd) = refs[13:20]
    mix_out, exp_out = refs[20:22]
    b = dict(zip(keys, refs[22 : 22 + len(keys)]))
    send_sem, recv_sem, load_sem = refs[22 + len(keys) :]
    x, info = b["x"], b["info"]
    half, ep, width, stride, cap = sizes.half, sizes.ep, sizes.width, sizes.stride, sizes.cap
    tokens, rows, tile, vd = sizes.tokens, sizes.rows, sizes.tile, sizes.value_dim
    f32, bf = jnp.float32, jnp.bfloat16
    table, _ = sizes.names()
    order = chunk_order(half)
    place = {name: number for number, name in enumerate(order)}

    me = lax.axis_index("ep")
    tp = lax.axis_index("tp")
    side = me // half
    spot = me % half
    row_of = tp // 2
    core = tp % 2
    tiles = width // tile

    lines = half // 2
    line, lane_x = spot // 2, spot % 2

    def shifted(which, d, turn):
        moved = (line + lines + turn * (d // 2)) % lines
        return which * half + moved * 2 + (lane_x + d % 2) % 2

    near_to = [shifted(side, d, 1) for d in range(half)]
    near_by = [shifted(side, d, -1) for d in range(half)]
    far_to = [shifted(1 - side, d, 1) for d in range(half)]
    far_by = [shifted(1 - side, d, -1) for d in range(half)]
    early = half // 2

    def near(d):
        return (near_to[d], tp)

    def near_from(d):
        return (near_by[d], tp)

    def far(d):
        return (far_to[d], tp)

    def far_from(d):
        return (far_by[d], tp)

    partner_y = (me, (1 - row_of) * 2 + core)
    partner_c = (me, row_of * 2 + 1 - core)

    def remote(number, source, target, device):
        return pltpu.make_async_remote_copy(
            src_ref=source,
            dst_ref=target,
            send_sem=send_sem.at[number],
            recv_sem=recv_sem.at[number],
            device_id=device,
            device_id_type=pl.DeviceIdType.MESH,
        )

    copies = {}

    def made(name):
        source, target, device = copies[name]
        return remote(table[name], source(), target(), device)

    def copy(name, source, target, device):
        copies[name] = (source, target, device)
        return Later(lambda: made(name).start())

    def dot(left, right):
        return jnp.dot(left, right, preferred_element_type=f32)

    crossing = [("n", d) for d in range(2, half)] + [("f", d) for d in range(half)]
    for kind, d in crossing:
        position = place[(kind, d)]
        copies[("FY", kind, d)] = (
            lambda position=position: b["r"].at[position, 0, 0, pl.ds(0, cap)],
            lambda position=position: b["r"].at[position, 0, 1, pl.ds(0, cap)],
            partner_y,
        )
    for d in range(half):
        copies[("RET", d)] = (
            lambda d=d: b["fb"].at[place[("f", d)], pl.ds(0, cap)],
            lambda d=d: b["tf"].at[d, pl.ds(0, cap)],
            far_from(d),
        )
    for d in range(1, half):
        for c in range(2):
            cols = pl.ds(c * width // 2, width // 2)
            copies[("NRET", d, c)] = (
                lambda d=d, cols=cols: b["q"].at[place[("n", d)], :, pl.ds(0, cap), cols],
                lambda d=d, cols=cols: b["tn"].at[:, d, pl.ds(0, cap), cols],
                near_from(d),
            )

    loads = {}
    pairs = dict(
        x=(h_x, b["x"]),
        ids=(h_ids, b["ids"]),
        gates=(h_gates, b["gates"]),
        mx=(h_mx, b["mx"]),
        q1=(h_q1, b["wq"].at[:, : 2 * HEAD]),
        q2=(h_q2, b["wq"].at[:, 2 * HEAD :]),
        k1=(h_k1, b["wk"].at[:HEAD]),
        k2=(h_k2, b["wk"].at[HEAD:]),
        v=(h_v, b["wv"]),
        sg=(h_sg, b["sg"]),
        su=(h_su, b["su"]),
        sd=(h_sd, b["sd"]),
        wg=(h_g.at[0], b["wg"]),
        wu=(h_u.at[0], b["wu"]),
        wd=(h_d.at[0], b["wd"]),
        wo=(h_wo, b["wo"]),
    )
    for number, (name, (source, target)) in enumerate(pairs.items()):
        loads[name] = pltpu.make_async_copy(source, target, load_sem.at[number])
        loads[name].start()

    barrier = pltpu.get_barrier_semaphore()
    peers = [near(d) for d in range(1, half)] + [far(d) for d in range(half)]
    peers += [partner_y, partner_c]
    for device in peers:
        pl.semaphore_signal(
            barrier, inc=1, device_id=device, device_id_type=pl.DeviceIdType.MESH
        )

    def norm_rows(source, target, count, gain):
        step = min(32, count)

        @pl.loop(0, count // step)
        def _(index):
            at = pl.ds(pl.multiple_of(index * step, step), step)
            values = source[at, :].astype(f32)
            factor = lax.rsqrt(jnp.mean(values * values, axis=-1, keepdims=True) + EPS)
            target[at, :] = (values * factor * gain[...]).astype(bf)

    loads["x"].wait()
    norm_rows(x, b["xb"].at[0, 0], tokens, xgain)
    loads["ids"].wait()
    loads["gates"].wait()
    info[...] = jnp.zeros((8, tokens), f32)
    info[0:2, :] = b["ids"][...].astype(f32)
    info[2:4, :] = b["gates"][...]

    earlier = (
        lax.broadcasted_iota(jnp.int32, (tokens, tokens), 0)
        < lax.broadcasted_iota(jnp.int32, (tokens, tokens), 1)
    ).astype(bf)
    padded_ep = -(-ep // 8) * 8
    relative = lax.broadcasted_iota(jnp.int32, (padded_ep, tokens), 0)
    expert = jnp.zeros((padded_ep, tokens), f32) - 1.0
    for k, target in enumerate(near_to + far_to):
        expert = jnp.where(relative == k, target.astype(f32), expert)

    def routing(info_ref):
        first = info_ref[0:1, :] == expert
        second = info_ref[1:2, :] == expert
        named = jnp.where(first | second, 1.0, 0.0)
        position = dot(named.astype(bf), earlier)
        position = jnp.where(named > 0.0, position, -1.0)
        weight = jnp.where(first, info_ref[2:3, :], 0.0) + jnp.where(second, info_ref[3:4, :], 0.0)
        return position, weight

    slot = lax.broadcasted_iota(jnp.int32, (stride, tokens), 0).astype(f32)

    def chosen(position, which):
        return slot == position[which : which + 1, :]

    def select(position, which):
        return jnp.concatenate(
            [jnp.where(chosen(position, k), 1.0, 0.0) for k in which], axis=0
        ).astype(bf)

    def spread(position, weight, which):
        stacked = jnp.concatenate(
            [jnp.where(chosen(position, k), weight[k : k + 1, :], 0.0) for k in which], axis=0
        )
        turned = stacked.T
        upper = turned.astype(bf)
        return upper, (turned - upper.astype(f32)).astype(bf)

    own_place, own_weight = routing(info)
    near_set = list(range(half))
    far_set = list(range(half, 2 * half))
    direct_set = [0, 1]
    select_near = select(own_place, near_set)
    select_far = select(own_place, far_set)

    pl.semaphore_wait(barrier, len(peers))
    copy(("XY", 0), lambda: b["xb"].at[0, 0], lambda: b["xb"].at[1, 0], partner_y).start()
    copy(("INFO", 0), lambda: info, lambda: b["other"], partner_y).start()
    copy(("XC", 0), lambda: b["xb"].at[0, 0], lambda: b["xb"].at[0, 1], partner_c).start()

    def pick(select_rows, source, store):
        for n in range(tiles):
            cols = slice(n * tile, (n + 1) * tile)
            picked = dot(select_rows, source[:, cols]).astype(bf)
            for d in range(select_rows.shape[0] // stride):
                store(d, cols, picked[d * stride : (d + 1) * stride, :])

    def store_near(a):
        def store(d, cols, value):
            b["outn"][d, a, :, cols] = value

        return store

    def store_far(d, cols, value):
        b["outf"][d, :, cols] = value

    pick(select_near, b["xb"].at[0, 0], store_near(0))

    def core_forward(position):
        return remote(
            table["RC"] + position, b["r"].at[position, 0], b["r"].at[position, 1], partner_c
        )

    def arrive_cross(kind, d):
        made(("FAR", d) if kind == "f" else ("NEAR", d, 0)).wait_recv()
        made(("FY", kind, d)).start()

    def crossed(kind, d):
        made(("FY", kind, d)).wait_recv()
        core_forward(place[(kind, d)]).start()

    def arrive_near():
        for a in range(2):
            made(("NEAR", 1, a)).wait_recv()
        core_forward(place[("n", 1)]).start()

    def relay_kv():
        @pl.when(side == 1)
        def _():
            slot_of = b["kv"].at[far_by[0]]
            remote(table[("KVF", 0)], slot_of, slot_of, far(0)).wait_recv()

        for d in range(1, half):
            copy(("KVC", d), lambda: b["kv"].at[far_by[0]], lambda: b["kv"].at[far_by[0]], near(d))

            @pl.when(side == 1)
            def _(d=d):
                made(("KVC", d)).start()

    def other_spread():
        upper, lower = spread(other_place, other_weight, near_set)
        b["woth"][0] = upper
        b["woth"][1] = lower

    def start_near(a):
        for d in (range(1, half) if a == 0 else (1,)):
            copy(
                ("NEAR", d, a),
                lambda d=d: b["outn"].at[d, a, pl.ds(0, cap)],
                lambda d=d: b["r"].at[place[("n", d)], 0, a, pl.ds(0, cap)],
                near(d),
            ).start()

    start_near(0)
    pick(select_far, b["xb"].at[0, 0], store_far)

    def start_far(d):
        copy(
            ("FAR", d),
            lambda: b["outf"].at[d, pl.ds(0, cap)],
            lambda: b["r"].at[place[("f", d)], 0, 0, pl.ds(0, cap)],
            far(d),
        ).start()

    for d in range(early):
        start_far(d)

    loads["mx"].wait()
    norm_rows(b["mx"], b["nm"], rows, mgain)
    for name in ("q1", "q2", "k1", "k2", "v"):
        loads[name].wait()
    lane = lax.broadcasted_iota(jnp.int32, (rows, 2 * HEAD), 1)
    b["kv"][me, :, : 2 * HEAD] = lax.dot_general(
        b["nm"][...], b["wk"][...], (((1,), (1,)), ((), ())), preferred_element_type=f32
    ).astype(bf)
    b["kv"][me, :, 2 * HEAD :] = dot(b["nm"][...], b["wv"][...]).astype(bf)

    copy(("KVF", 0), lambda: b["kv"].at[me], lambda: b["kv"].at[me], far(0))

    @pl.when(side == 0)
    def _():
        made(("KVF", 0)).start()

    for d in range(1, half):
        copy(("KVN", d), lambda: b["kv"].at[me], lambda: b["kv"].at[me], near(d))

        @pl.when(near_to[d] > me)
        def _(d=d):
            made(("KVN", d)).start()

    for m in range(2):
        queries = dot(b["nm"][...], b["wq"][:, m * 2 * HEAD : (m + 1) * 2 * HEAD])
        turned = pltpu.roll(queries, HEAD, 1)
        keep = (lane < HEAD) if m == 0 else (lane >= HEAD)
        for g in range(2):
            source = queries if g == m else turned
            b["qs"][m, g] = jnp.where(keep, source, 0.0).astype(bf)

    def shared_expert(a):
        both = b["xb"][a].reshape(2 * tokens, width)
        gated = dot(both, b["sg"][...])
        lifted = dot(both, b["su"][...])
        hidden = (jax.nn.silu(gated) * lifted).astype(bf)
        for n in range(tiles):
            cols = slice(n * tile, (n + 1) * tile)
            part = dot(hidden, b["sd"][:, cols]).astype(bf)
            b["s"][a, 0, :, cols] = part[:tokens]
            b["s"][a, 1, :, cols] = part[tokens:]

    for name in ("sg", "su", "sd"):
        loads[name].wait()
    made(("XC", 0)).wait_recv()
    shared_expert(0)
    copy(("SC", 0), lambda: b["s"].at[0, 1], lambda: b["sr"].at[0], partner_c).start()

    upper, lower = spread(own_place, own_weight, near_set)
    b["wown"][0] = upper
    b["wown"][1] = lower
    for d in range(half):
        upper, lower = spread(own_place, own_weight, [half + d])
        b["wfar"][d, 0] = upper
        b["wfar"][d, 1] = lower
    for d in range(half):
        b["tf"][d, cap:, :] = jnp.zeros((stride - cap, width), bf)
        for a in range(2):
            b["tn"][a, d, cap:, :] = jnp.zeros((stride - cap, width), bf)
    made(("XY", 0)).wait_recv()
    made(("INFO", 0)).wait_recv()
    copy(("XC", 1), lambda: b["xb"].at[1, 0], lambda: b["xb"].at[1, 1], partner_c).start()
    arrive_cross("f", 0)
    other_place, other_weight = routing(b["other"])
    pick(select(other_place, direct_set), b["xb"].at[1, 0], store_near(1))
    start_near(1)
    for d in range(early, half):
        start_far(d)
    b["r"][0, 0] = b["outn"][0]

    core_forward(0).start()
    made(("XC", 1)).wait_recv()
    shared_expert(1)
    copy(("SC", 1), lambda: b["s"].at[1, 1], lambda: b["sr"].at[1], partner_c).start()
    other_spread()
    for d in range(1, early):
        arrive_cross("f", d)
    for d in range(2, half):
        arrive_cross("n", d)

    for name in ("wg", "wu", "wd"):
        loads[name].wait()

    far_places = [place[("f", d)] for d in range(half)]
    row_count = 4 * stride

    def back_copy(number):
        return remote(
            table["PC"] + number, b["p"].at[number, 1], b["pr"].at[number], partner_c
        )

    def cross_copy(number):
        return remote(
            table["QY"] + number,
            b["q"].at[number, 1, pl.ds(0, cap)],
            b["qr"].at[number, pl.ds(0, cap)],
            partner_y,
        )

    def core_sum(kind, d):
        position = place[(kind, d)]
        back_copy(position).wait_recv()
        for a in range(2):
            b["q"][position, a] = (
                b["p"][position, 0, a].astype(f32) + b["pr"][position, a].astype(f32)
            ).astype(bf)
        if kind == "f":
            cross_copy(position).start()
        elif d > 0:
            for c in range(2):
                made(("NRET", d, c)).start()
        else:
            for a in range(2):
                b["tn"][a, 0, 0:cap, :] = b["q"][position, a, 0:cap, :]

    def side_sum(d):
        position = place[("f", d)]
        cross_copy(position).wait_recv()
        b["fb"][position] = (
            b["q"][position, 0].astype(f32) + b["qr"][position].astype(f32)
        ).astype(bf)
        made(("RET", d)).start()

    def kv_arrival(name, source, d):
        block = b["kv"].at[source]
        remote(table[(name, d)], block, block, near(d)).wait_recv()

    def kv_arrivals():
        for d in range(1, half):

            @pl.when(near_by[d] < me)
            def _(d=d):
                kv_arrival("KVN", near_by[d], d)

            @pl.when(side == 1)
            def _(d=d):
                kv_arrival("KVC", far_by[d], d)

    scale = HEAD**-0.5 * math.log2(math.e)
    row_place = me * rows + lax.broadcasted_iota(jnp.int32, (rows, rows), 0)
    col_place = lax.broadcasted_iota(jnp.int32, (rows, rows), 1)
    halves = [slice(c * 128, (c + 1) * 128) for c in range(rows // 128)]

    def head(g):
        b["stat"][...] = jnp.full((2, rows, 128), NEG, f32)
        b["tot"][...] = jnp.zeros((2, rows, 128), f32)
        b["pv"][...] = jnp.zeros((2, rows, vd), f32)

        def score(j, carry):
            keys_j = b["kv"][j, :, 0 : 2 * HEAD]
            for m in range(2):
                scores = lax.dot_general(
                    b["qs"][m, g], keys_j, (((1,), (1,)), ((), ())), preferred_element_type=f32
                )
                scores = jnp.where(j * rows + col_place <= row_place, scores, NEG)
                b["sc"][m, j] = scores
                most = b["stat"][m]
                for cols in halves:
                    most = jnp.maximum(most, scores[:, cols])
                b["stat"][m] = most
            return carry

        lax.fori_loop(0, me + 1, score, 0)
        for m in range(2):
            most = jnp.max(b["stat"][m], axis=1, keepdims=True)
            b["stat"][m] = jnp.broadcast_to(most, (rows, 128))

        def weigh(j, carry):
            values = b["kv"][j, :, 2 * HEAD :]
            for m in range(2):
                most = b["stat"][m]
                total = b["tot"][m]
                parts = []
                for cols in halves:
                    weights = jnp.exp2((b["sc"][m, j, :, cols] - most) * scale)
                    total = total + weights
                    parts.append(weights.astype(bf))
                b["tot"][m] = total
                b["pv"][m] += dot(jnp.concatenate(parts, axis=1), values)
            return carry

        lax.fori_loop(0, me + 1, weigh, 0)
        sums = [jnp.sum(b["tot"][m], axis=1, keepdims=True) for m in range(2)]
        combined = b["pv"][0] / sums[0] - lam[g] * (b["pv"][1] / sums[1])
        factor = lax.rsqrt(jnp.mean(combined * combined, axis=1, keepdims=True) + EPS)
        b["hr"][:, g * vd : (g + 1) * vd] = (combined * factor * hgain[...]).astype(bf)

    def project_out():
        loads["wo"].wait()
        own = sizes.own
        for n in range(tiles):
            cols = slice(n * tile, (n + 1) * tile)
            part = dot(b["hr"][...], b["wo"][:, cols]).astype(bf)
            b["o"][:, :, :, cols] = part.reshape(2, 2, own, tile)
        made(("OC", 0)).start()

    def other_rows(c):
        for d in range(1, half):
            made(("NRET", d, c)).wait_recv()
        if c == 0:
            for a in range(2):
                made(("SC", a)).wait_recv()
        for n in range(c * tiles // 2, (c + 1) * tiles // 2):
            cols = slice(n * tile, (n + 1) * tile)
            back = b["tn"][1, :, :, cols].reshape(half * stride, tile)
            total = dot(b["woth"][0], back) + dot(b["woth"][1], back)
            total = total + b["s"][1, 0, :, cols].astype(f32) + b["sr"][1, :, cols].astype(f32)
            b["ao"][:, cols] = total.astype(bf)
        made(("AY", c)).start()

    def mix_sum():
        made(("OC", 0)).wait_recv()
        for a in range(2):
            b["oq"][a] = (b["o"][a, core].astype(f32) + b["orx"][a].astype(f32)).astype(bf)
        made(("OY", 0)).start()

    def own_rows():
        for n in range(tiles):
            cols = slice(n * tile, (n + 1) * tile)
            back = b["tn"][0, :, :, cols].reshape(half * stride, tile)
            total = dot(b["wown"][0], back) + dot(b["wown"][1], back)
            b["acc"][:, cols] = (
                total + b["s"][0, 0, :, cols].astype(f32) + b["sr"][0, :, cols].astype(f32)
            )

    copies[("OC", 0)] = (lambda: b["o"].at[:, 1 - core], lambda: b["orx"], partner_c)
    for c in range(2):
        cols = pl.ds(c * width // 2, width // 2)
        copies[("AY", c)] = (
            lambda cols=cols: b["ao"].at[:, cols],
            lambda cols=cols: b["ar"].at[:, cols],
            partner_y,
        )
    copies[("OY", 0)] = (lambda: b["oq"].at[1 - row_of], lambda: b["oy"], partner_y)
    schedule = step_plan(half)
    actions = dict(
        arrive_cross=arrive_cross,
        crossed=crossed,
        arrive_near=arrive_near,
        core_sum=core_sum,
        side_sum=side_sum,
        kv_arrivals=kv_arrivals,
        head=head,
        relay_kv=relay_kv,
        project_out=project_out,
        mix_sum=mix_sum,
        other_rows=other_rows,
        own_rows=own_rows,
    )

    def step_body(step, carry):
        for when in sorted(schedule):

            @pl.when(step == when)
            def _(when=when):
                for name, *values in schedule[when]:
                    actions[name](*values)

        @pl.when(step < ep)
        def _():
            core_forward(step).wait_recv()
            arrived = b["r"][step].reshape(row_count, width)
            gated = dot(arrived, b["wg"][...])
            lifted = dot(arrived, b["wu"][...])
            hidden = (jax.nn.silu(gated) * lifted).astype(bf)
            for n in range(tiles):
                cols = slice(n * tile, (n + 1) * tile)
                part = dot(hidden, b["wd"][:, cols]).astype(bf)
                b["p"][step, :, :, :, cols] = part.reshape(2, 2, stride, tile)
            back_copy(step).start()

        return carry

    lax.fori_loop(0, max(schedule) + 1, step_body, 0)

    made(("OY", 0)).wait_recv()
    mix_out[...] = (b["oq"][row_of].astype(f32) + b["oy"][...].astype(f32)).astype(bf)

    for d in range(half):
        made(("RET", d)).wait_recv()
        for n in range(tiles):
            cols = slice(n * tile, (n + 1) * tile)
            back = b["tf"][d, :, cols]
            b["acc"][:, cols] += dot(b["wfar"][d, 0], back) + dot(b["wfar"][d, 1], back)
    for c in range(2):
        made(("AY", c)).wait_recv()
        cols = slice(c * width // 2, (c + 1) * width // 2)
        exp_out[:, cols] = (b["acc"][:, cols] + b["ar"][:, cols].astype(f32)).astype(bf)

    conditional = {("KVF", 0): side == 0}
    for d in range(1, half):
        conditional[("KVN", d)] = near_to[d] > me
        conditional[("KVC", d)] = side == 1
    for name in copies:
        if name in conditional:

            @pl.when(conditional[name])
            def _(name=name):
                made(name).wait_send()

        else:
            made(name).wait_send()
    for position in range(ep):
        core_forward(position).wait_send()
        back_copy(position).wait_send()
        if position in far_places:
            cross_copy(position).wait_send()


def fused(sizes, args):
    scratch = sizes.scratch()
    keys = list(scratch)
    _, count = sizes.names()
    vmem = pl.BlockSpec(memory_space=pltpu.VMEM)
    smem = pl.BlockSpec(memory_space=pltpu.SMEM)
    hbm = pl.BlockSpec(memory_space=pltpu.HBM)
    return pl.pallas_call(
        functools.partial(fused_kernel, sizes, keys),
        out_shape=(
            jax.ShapeDtypeStruct((sizes.own, sizes.width), jnp.bfloat16),
            jax.ShapeDtypeStruct((sizes.tokens, sizes.width), jnp.bfloat16),
        ),
        in_specs=[smem] + [vmem] * 3 + [hbm] * 16,
        out_specs=(vmem, vmem),
        scratch_shapes=[pltpu.VMEM(shape, dtype) for shape, dtype in scratch.values()]
        + [
            pltpu.SemaphoreType.DMA((count,)),
            pltpu.SemaphoreType.DMA((count,)),
            pltpu.SemaphoreType.DMA((16,)),
        ],
        compiler_params=pltpu.CompilerParams(
            collective_id=0, has_side_effects=True, vmem_limit_bytes=VMEM_LIMIT
        ),
        name="layer",
    )(*args)


VMEM_LIMIT = 67043328


def fused_body(sizes, *arrays):
    (
        mixer_input,
        mixer_gain,
        query_one,
        query_two,
        key_one,
        key_two,
        value_weight,
        lambdas,
        head_gain,
        output_weight,
        expert_input,
        expert_gain,
        routes,
        route_weight,
        expert_gate,
        expert_up,
        expert_down,
        shared_gate,
        shared_up,
        shared_down,
    ) = arrays
    return fused(
        sizes,
        (
            lambdas,
            expert_gain.reshape(1, -1),
            mixer_gain.reshape(1, -1),
            head_gain.reshape(1, -1),
            expert_input,
            routes.T,
            route_weight.T,
            mixer_input,
            query_one,
            query_two,
            key_one.T,
            key_two.T,
            value_weight,
            output_weight,
            expert_gate,
            expert_up,
            expert_down,
            shared_gate,
            shared_up,
            shared_down,
        ),
    )


def body(*arrays):
    ep_size, tp_size = lax.axis_size("ep"), lax.axis_size("tp")
    mixer_input, query_one, key_one = arrays[0], arrays[2], arrays[4]
    head_gain, expert_input, routes = arrays[8], arrays[10], arrays[12]
    expert_gate, shared_gate = arrays[14], arrays[17]
    rows, width = mixer_input.shape
    tokens, top_count = routes.shape
    local_experts = expert_gate.shape[0]
    capacity = max(2, 5 * tokens * top_count // (4 * local_experts * ep_size))
    fits = (
        tp_size == 4
        and ep_size % 2 == 0
        and ep_size >= 4
        and local_experts == 1
        and top_count == 2
        and key_one.shape[1] == HEAD
        and query_one.shape[1] == 2 * HEAD
        and head_gain.shape[0] == 128
        and tokens == 128
        and rows % (16 * tp_size) == 0
        and rows % 128 == 0
        and width % 512 == 0
        and expert_input.shape[1] == width
        and capacity % 8 == 0
    )
    if fits:
        sizes = Sizes(
            ep_size,
            tp_size,
            rows,
            width,
            tokens,
            expert_gate.shape[2],
            shared_gate.shape[1],
            capacity,
            head_gain.shape[0],
        )
        if sizes.vmem_bytes() + 8 * 2**20 <= VMEM_LIMIT:
            return fused_body(sizes, *arrays)
    return general_body(*arrays)


def solution(mesh):
    in_specs = (
        P("ep", None),
        P(),
        P(None, "tp"),
        P(None, "tp"),
        P(None, "tp"),
        P(None, "tp"),
        P(None, "tp"),
        P("tp"),
        P(),
        P("tp", None),
        P(("ep", "tp"), None),
        P(),
        P(("ep", "tp"), None),
        P(("ep", "tp"), None),
        P("ep", None, "tp"),
        P("ep", None, "tp"),
        P("ep", "tp", None),
        P(None, "tp"),
        P(None, "tp"),
        P("tp", None),
    )
    out_specs = (P(("ep", "tp"), None), P(("ep", "tp"), None))
    return jax.shard_map(body, mesh=mesh, in_specs=in_specs, out_specs=out_specs, check_vma=False)
```
